256 devices in a mesh: ep: 32 (over z, x), tp: 8 (over y, core).
Axes of the slice: x: 4, y: 4, z: 8, core: 2. Of those that a mesh axis runs over, the one named last changes fastest.
Arguments:
- tokens: bfloat16 [512, 1024], P('ep'), may hold values from -6 to 6
- norm_gain: float32 [1024], replicated, may hold values from 0.1 to 1.9
- routing: int32 [512, 2], P('ep'), may hold values from 0 to 31, all different within a row; in each aligned block of 16 rows (0 to 15, 16 to 31, ...) at most 8 rows name the same one
- route_weight: float32 [512, 2], P('ep'), may hold values from 0.1 to 1
- w_gate: bfloat16 [32, 1024, 3584], P('ep', None, 'tp'), may hold values from -0.1875 to 0.1875
- w_up: bfloat16 [32, 1024, 3584], P('ep', None, 'tp'), may hold values from -0.1875 to 0.1875
- w_down: bfloat16 [32, 3584, 1024], P('ep', 'tp'), may hold values from -0.09375 to 0.09375
Outputs:
- mixed: bfloat16 [512, 1024], P('ep', 'tp')
The draws below stay inside these ranges and needn't reach their ends.
Inputs may be any that keep to these rules, and one draw needn't show every extreme that they name: `routing`: each row names 2 different experts of 0 to 31; among the 16 tokens of one index of ep no expert is named more than 8 times, and in some draws' blocks exactly 8 times.
All inputs are finite; a program needn't handle non-finite values.
Results may differ from the reference program's by a relative error of at most 0.0022.
Values may be sent and summed in bfloat16 or wider, within the bound.
A program may use at most 64 MiB of HBM per device.

```python
import math
import jax
import jax.numpy as jnp
import numpy as np
from jax import lax

D = 1024
FF = 3584
TOP = 2
TOK_DEV = 16
CAP = 8
EXPERTS = 32
TOKENS = 512


def level_of(rng, shape, cuts, low, top_value):
    factor_of, own = 1.0, jax.random.fold_in(rng, 6)
    for position, shards_of in cuts:
        draws = jnp.exp(jax.random.uniform(jax.random.fold_in(own, position), (shards_of,), jnp.float32, low / len(cuts), top_value / len(cuts)))
        factor_of = factor_of * jnp.repeat(draws, shape[position] // shards_of).reshape([-1 if axis == position else 1 for axis in range(len(shape))])
    return factor_of


def shared_out(rng, own, number, rows, number_of, top, limit, lean):
    ranking = jax.random.permutation(rng, number_of)
    heavy_load, usual = portions_of(number_of, rows * top, limit, lean, True), portions_of(number_of, rows * top, limit, lean, False)
    places = jnp.arange(number_of)

    def named(sizes, rotation):
        used = int((sizes > 0).sum())
        fixed = max(1, used // 4)
        shifted = fixed + (places - fixed + rotation * (used - fixed)) % max(1, number_of - fixed)
        return jnp.zeros((number_of,), jnp.int32).at[ranking[jnp.where(places < fixed, places, shifted)]].set(jnp.asarray(sizes, jnp.int32))

    sizes = jnp.where(number % 4 == 0, named(heavy_load, number // 4), named(usual, number - number // 4 - 1))
    mixed = jax.random.permutation(jax.random.fold_in(own, 3), number_of)
    donor, taker = mixed[0:number_of // 2 * 2:2], mixed[1:number_of // 2 * 2:2]
    room = jnp.minimum(sizes[donor] - 1, limit - sizes[taker]) // 2
    room = jnp.where((donor == ranking[0]) | (taker == ranking[0]) | (sizes[taker] == 0), 0, jnp.maximum(room, 0))
    shifted = jax.random.randint(jax.random.fold_in(own, 4), (number_of // 2,), 0, 1 << 20) % (room + 1)
    sizes = sizes.at[donor].add(-shifted).at[taker].add(shifted)
    labels = jnp.searchsorted(jnp.cumsum(sizes), jnp.arange(rows * top), side="right").astype(jnp.int32)
    listing = labels.reshape(top, rows).T
    listing = listing[jax.random.permutation(jax.random.fold_in(own, 1), rows)]
    rotation = jax.random.randint(jax.random.fold_in(own, 2), (rows, 1), 0, top)
    return jnp.take_along_axis(listing, (jnp.arange(top)[None, :] + rotation) % top, axis=1)


def portions_of(count, total, most, slope, full):
    loads = [(1 << 20) // math.isqrt(grade ** slope) + 1 for grade in range(1, count + 1)]
    largest = most if full else min(most, max(-(-total // count), total * loads[0] // sum(loads)))
    least = 1 if total - largest >= count - 1 else 0
    counts, rest = [largest] + [least] * (count - 1), total - largest - least * (count - 1)
    while rest > 0:
        movable = [i for i in range(1, count) if counts[i] < largest] or [i for i in range(1, count) if counts[i] < most]
        whole, left = sum([loads[i] for i in movable]), rest
        for i in movable:
            extra = min(most - counts[i], max(1, left * loads[i] // whole), rest)
            counts[i] = counts[i] + extra
            rest = rest - extra
    return np.array(counts)


def scatter_about(own_key, dims, scale, reach, shards=(), kind=jnp.bfloat16):
    level = level_of(own_key, dims, shards, -0.22, 0.18) if shards else 1.0
    array = jax.random.normal(own_key, dims, jnp.float32) * scale * level
    return jnp.minimum(jnp.maximum(array, -reach), reach).astype(kind)


def setup_inputs(seed: int = 0) -> dict:
    seeds = jax.random.split(jax.random.key(seed), 8)
    tokens = scatter_about(seeds[0], (TOKENS, D), 1.0, 6.0, ((0, 32),))
    norm_gain = jnp.clip(1.0 + 0.18 * jax.random.normal(seeds[1], (D,), jnp.float32), 0.1, 1.9)
    routing_keys = jax.random.split(jax.random.fold_in(seeds[2], 1), TOKENS // TOK_DEV)
    routing_turns = jax.random.permutation(jax.random.fold_in(seeds[2], 3), TOKENS // TOK_DEV)
    routing = jax.vmap(lambda own, number: shared_out(jax.random.fold_in(seeds[2], 2), own, number, TOK_DEV, EXPERTS, TOP, CAP, 2))(routing_keys, routing_turns).reshape((TOKENS, TOP))
    route_weight = jnp.clip(0.1 + 0.9 * jax.random.uniform(seeds[3], (TOKENS, TOP), jnp.float32) ** level_of(seeds[3], (TOKENS, TOP), ((0, 32),), -0.2, 0.2), 0.1, 1.0)
    w_gate = scatter_about(seeds[4], (EXPERTS, D, FF), D ** -0.5, 0.1875, ((0, 32), (2, 8)))
    w_up = scatter_about(seeds[5], (EXPERTS, D, FF), D ** -0.5, 0.1875, ((0, 32), (2, 8)))
    w_down = scatter_about(seeds[6], (EXPERTS, FF, D), FF ** -0.5, 0.09375, ((0, 32), (1, 8)))
    return {"tokens": tokens, "norm_gain": norm_gain, "routing": routing, "route_weight": route_weight, "w_gate": w_gate, "w_up": w_up, "w_down": w_down}


norm_eps = 1e-06

def reference(tokens, norm_gain, routing, route_weight, w_gate, w_up, w_down):
    values = tokens.astype(jnp.float32)
    scale = lax.rsqrt(lax.optimization_barrier(jnp.mean(values * values, axis=-1, keepdims=True)) + norm_eps)
    normed = (values * scale * norm_gain).astype(jnp.bfloat16)
    top_count = routing.shape[1]
    flat_ids = routing.reshape(-1).astype(jnp.int32)
    token_rows = jnp.repeat(normed, top_count, axis=0)

    def one_slot(pair):
        token_row, expert_id = pair
        gate_act = jnp.dot(token_row[None, :], w_gate[expert_id], preferred_element_type=jnp.float32)
        up_act = jnp.dot(token_row[None, :], w_up[expert_id], preferred_element_type=jnp.float32)
        hidden = (jax.nn.silu(gate_act) * up_act).astype(jnp.bfloat16)
        return jnp.dot(hidden, w_down[expert_id], preferred_element_type=jnp.float32)[0]
    expert_out = lax.map(one_slot, (token_rows, flat_ids))
    expert_out = expert_out.reshape(routing.shape[0], top_count, -1)
    mixed = lax.optimization_barrier(jnp.sum(expert_out * route_weight[:, :, None], axis=1))
    return mixed.astype(jnp.bfloat16)
```

```python
import functools

import jax
import jax.numpy as jnp
from jax import lax
from jax.experimental import pallas as pl
from jax.experimental.pallas import tpu as pltpu
from jax.sharding import PartitionSpec as P

CAP = 8
MESH = pl.DeviceIdType.MESH

norm_eps = 1e-06


def kernel(groups, shares, tokens_hbm, gain_hbm, routing_hbm, route_weight_hbm, gate_hbm, up_hbm, down_hbm, mixed,
           tokens, gain, routing, route_weight, gate, up, down,
           outgoing, incoming, partial, reduced, back, arrived,
           load_sem, swap_send, swap_recv, out_sem, in_sem, part_send, part_recv, back_send, back_recv):
    ep, tp = lax.axis_index("ep"), lax.axis_index("tp")
    width = tokens.shape[1]
    part = mixed.shape[1]
    half = groups // 2
    rows = half * CAP
    planes = shares // 2
    share = gate_hbm.shape[1]
    y, core = tp // 2, lax.rem(tp, 2)
    place, parity = ep // 2, lax.rem(ep, 2)
    own = (core == parity).astype(jnp.int32)
    shift = half // 4
    tile = 2 * part

    def group(q):
        return 2 * lax.rem(place + q, half) + core

    pairs = ((tokens_hbm, tokens), (gain_hbm, gain), (routing_hbm, routing), (route_weight_hbm, route_weight),
             (gate_hbm.at[0], gate.at[0:share]), (up_hbm.at[0], up.at[0:share]), (down_hbm.at[0], down.at[0:share]))
    loads = [pltpu.make_async_copy(source, target, load_sem.at[i]) for i, (source, target) in enumerate(pairs)]
    for i in (2, 3, 0, 1, 4, 5, 6):
        loads[i].start()

    far_first = sorted(range(half), key=lambda q: -min(q, half - q))
    barrier = pltpu.get_barrier_semaphore()
    for q in far_first:
        def greet(q=q):
            pl.semaphore_signal(barrier, inc=1, device_id=(group(q), 2 * y + parity), device_id_type=MESH)
        if q == 0:
            pl.when(core != parity)(greet)
        else:
            greet()
    for d in range(1, planes):
        pl.semaphore_signal(barrier, inc=1, device_id=(ep, 2 * lax.rem(y + d, planes) + core), device_id_type=MESH)
    pl.semaphore_signal(barrier, inc=1, device_id=(ep, 2 * y + 1 - core), device_id_type=MESH)

    count = tokens.shape[0]
    earlier = lax.broadcasted_iota(jnp.int32, (count, count), 0) < lax.broadcasted_iota(jnp.int32, (count, count), 1)
    earlier = jnp.where(earlier, 1.0, 0.0).astype(jnp.bfloat16)

    def slots_of(lines, expert_of):
        line = lax.broadcasted_iota(jnp.int32, (lines, count), 0)
        expert = expert_of(line // CAP)
        member = jnp.zeros((lines, count), jnp.float32)
        weight = jnp.zeros((lines, count), jnp.float32)
        for k in range(routing.shape[0]):
            named = routing[k:k + 1, :] == expert
            member = jnp.where(named, 1.0, member)
            weight = jnp.where(named, route_weight[k:k + 1, :], weight)
        before = jnp.dot(member.astype(jnp.bfloat16), earlier, preferred_element_type=jnp.float32)
        placed = jnp.where(before == lax.rem(line, CAP).astype(jnp.float32), member, 0.0)
        return placed, weight

    loads[2].wait()
    loads[3].wait()
    placed, _ = slots_of(rows, lambda q: group(q))
    loads[0].wait()
    loads[1].wait()
    values = tokens[...].astype(jnp.float32)
    scale = lax.rsqrt(jnp.mean(values * values, axis=-1, keepdims=True) + norm_eps)
    normed = (values * scale * gain[...]).astype(jnp.bfloat16)
    sent = jnp.dot(placed.astype(jnp.bfloat16), normed, preferred_element_type=jnp.float32)
    outgoing[...] = sent.reshape(half, CAP, width).astype(jnp.bfloat16)
    for i in (4, 5, 6):
        loads[i].wait()

    pl.semaphore_wait(barrier, half + planes - own)

    for q in far_first:
        at = (2 * half - q - shift) % half

        def dispatch(q=q, at=at):
            pltpu.make_async_remote_copy(
                src_ref=outgoing.at[q], dst_ref=incoming.at[at], send_sem=out_sem, recv_sem=in_sem,
                device_id=(group(q), 2 * y + parity), device_id_type=MESH).start()

        def keep(q=q, at=at):
            incoming[at] = outgoing[q]
        if q == 0:
            pl.when(core != parity)(dispatch)
            pl.when(core == parity)(keep)
        else:
            dispatch()

    swaps = [pltpu.make_async_remote_copy(
        src_ref=ref.at[0:share], dst_ref=ref.at[share:2 * share], send_sem=swap_send.at[i], recv_sem=swap_recv.at[i],
        device_id=(ep, 2 * y + 1 - core), device_id_type=MESH) for i, ref in enumerate((gate, up, down))]
    for swap in swaps:
        swap.start()

    picked, weight = slots_of(groups * CAP, lambda q: q)
    weight = jnp.transpose(weight * picked)

    for swap in swaps:
        swap.wait_recv()

    def wait_for(ref, sem, most):
        less, full = ref.at[pl.ds(0, most - 1)], ref.at[pl.ds(0, most)]
        pl.when(core == parity)(lambda: pltpu.make_async_copy(less, less, sem).wait())
        pl.when(core != parity)(lambda: pltpu.make_async_copy(full, full, sem).wait())
    wait_for(incoming, in_sem, half)

    x = incoming[...].astype(jnp.float32).reshape(rows, width).astype(jnp.bfloat16)
    last = (((1,), (1,)), ((), ()))
    gate_act = lax.dot_general(x, gate[...], last, preferred_element_type=jnp.float32)
    up_act = lax.dot_general(x, up[...], last, preferred_element_type=jnp.float32)
    hidden = (gate_act / (1.0 + jnp.exp(-gate_act)) * up_act).astype(jnp.bfloat16)

    chunks = 2
    piece = rows // chunks
    order = sorted(range(1, planes), key=lambda d: -min(d, planes - d))

    def columns(d):
        return pl.ds(pl.multiple_of(lax.rem(y + d, planes) * tile, tile), tile)

    def give(d, k):
        some = pl.ds(k * piece, piece)
        return pltpu.make_async_remote_copy(
            src_ref=partial.at[d - 1, some], dst_ref=reduced.at[d - 1, some],
            send_sem=part_send.at[d - 1, k], recv_sem=part_recv.at[d - 1, k],
            device_id=(ep, 2 * lax.rem(y + d, planes) + core), device_id_type=MESH)
    for d in order:
        partial[d - 1] = jnp.dot(hidden, down[:, columns(d)], preferred_element_type=jnp.float32)
        give(d, 0).start()
    for k in range(1, chunks):
        for d in order:
            give(d, k).start()
    total = jnp.dot(hidden, down[:, columns(0)], preferred_element_type=jnp.float32)

    def home(q):
        return lax.rem(q + shift, half)

    for k in range(chunks):
        mine = total[k * piece:(k + 1) * piece]
        for d in range(1, planes):
            give(d, k).wait_recv()
        for d in range(1, planes):
            mine = mine + reduced[d - 1, k * piece:(k + 1) * piece]
        first = k * (half // chunks)
        upto = first + half // chunks
        for side in range(2):
            back[side, first:upto] = mine[:, side * part:(side + 1) * part].reshape(half // chunks, CAP, part)
        distance = {at: min((at + shift) % half, half - (at + shift) % half) for at in range(first, upto)}
        for at in sorted(distance, key=lambda at: -distance[at]):
            for side in range(2):
                def send(at=at, side=side):
                    pltpu.make_async_remote_copy(
                        src_ref=back.at[side, at], dst_ref=arrived.at[ep], send_sem=back_send, recv_sem=back_recv,
                        device_id=(group(at + shift), 2 * y + side), device_id_type=MESH).start()

                def hold(at=at, side=side):
                    arrived[ep] = back[side, at]
                if distance[at] == 0:
                    here = jnp.logical_and(core == parity, core == side)
                    pl.when(here)(hold)
                    pl.when(jnp.logical_not(here))(send)
                else:
                    send()

    wait_for(arrived, back_recv, groups)
    out = jnp.dot(weight, arrived[...].reshape(groups * CAP, part), precision=lax.Precision.HIGHEST,
                  preferred_element_type=jnp.float32)
    mixed[...] = out.astype(mixed.dtype)
    wait_for(outgoing, out_sem, half)
    for swap in swaps:
        swap.wait_send()
    for k in range(chunks):
        for d in range(1, planes):
            give(d, k).wait_send()
    wait_for(arrived, back_send, groups)


def solution(mesh):
    groups, shares = mesh.shape["ep"], mesh.shape["tp"]

    def local(tokens, norm_gain, routing, route_weight, w_gate, w_up, w_down):
        count, width = tokens.shape
        part = width // shares
        half, planes = groups // 2, shares // 2
        rows = half * CAP
        share = w_down.shape[1]
        vmem = pl.BlockSpec(memory_space=pltpu.VMEM)
        hbm = pl.BlockSpec(memory_space=pltpu.HBM)
        return pl.pallas_call(
            functools.partial(kernel, groups, shares),
            out_shape=jax.ShapeDtypeStruct((count, part), jnp.bfloat16),
            in_specs=[hbm] * 7,
            out_specs=vmem,
            scratch_shapes=[
                pltpu.VMEM((count, width), tokens.dtype),
                pltpu.VMEM((1, width), norm_gain.dtype),
                pltpu.VMEM(routing.shape[::-1], routing.dtype),
                pltpu.VMEM(route_weight.shape[::-1], route_weight.dtype),
                pltpu.VMEM((2 * share, width), jnp.bfloat16),
                pltpu.VMEM((2 * share, width), jnp.bfloat16),
                pltpu.VMEM((2 * share, width), jnp.bfloat16),
                pltpu.VMEM((half, CAP, width), jnp.bfloat16),
                pltpu.VMEM((half, CAP, width), jnp.bfloat16),
                pltpu.VMEM((planes - 1, rows, 2 * part), jnp.float32),
                pltpu.VMEM((planes - 1, rows, 2 * part), jnp.float32),
                pltpu.VMEM((2, half, CAP, part), jnp.float32),
                pltpu.VMEM((groups, CAP, part), jnp.float32),
                pltpu.SemaphoreType.DMA((7,)),
                pltpu.SemaphoreType.DMA((3,)),
                pltpu.SemaphoreType.DMA((3,)),
                pltpu.SemaphoreType.DMA,
                pltpu.SemaphoreType.DMA,
                pltpu.SemaphoreType.DMA((planes - 1, 2)),
                pltpu.SemaphoreType.DMA((planes - 1, 2)),
                pltpu.SemaphoreType.DMA,
                pltpu.SemaphoreType.DMA,
            ],
            compiler_params=pltpu.CompilerParams(collective_id=0, has_side_effects=True,
                                                 vmem_limit_bytes=67043328),
            name="experts",
        )(tokens, norm_gain.reshape(1, width), routing.T, route_weight.T,
          jnp.swapaxes(w_gate, 1, 2), jnp.swapaxes(w_up, 1, 2), w_down)

    in_specs = (
        P("ep", None),
        P(),
        P("ep", None),
        P("ep", None),
        P("ep", None, "tp"),
        P("ep", None, "tp"),
        P("ep", "tp", None),
    )
    return jax.shard_map(local, mesh=mesh, in_specs=in_specs, out_specs=P("ep", "tp"), check_vma=False)
```

```python
import functools

import jax
import jax.numpy as jnp
from jax import lax
from jax.experimental import pallas as pl
from jax.experimental.pallas import tpu as pltpu
from jax.sharding import PartitionSpec as P

CAP = 8
XS = 4
CHUNKS = ((0, 3), (3, 5), (5, 8))
MESH = pl.DeviceIdType.MESH

norm_eps = 1e-06


def kernel(groups, shares, tokens_hbm, gain_hbm, routing_hbm, route_weight_hbm, gate_hbm, up_hbm, down_hbm, mixed,
           tokens, gain, routing, route_weight, gate, up, down,
           row_tokens, row_routing, outgoing, incoming, partial, reduced, back, arrived,
           load_sem, row_send, row_recv, swap_send, swap_recv, out_sem, in_sem,
           part_send, part_recv, back_send, back_recv):
    ep, tp = lax.axis_index("ep"), lax.axis_index("tp")
    count, width = tokens.shape
    part = mixed.shape[1]
    zs = groups // XS
    planes = shares // 2
    share = gate_hbm.shape[1]
    tile = 2 * part
    z, x = ep // XS, lax.rem(ep, XS)
    y, core = tp // 2, lax.rem(tp, 2)
    parity = lax.rem(x, 2)
    same = core == parity

    offset = [(p + 1) // 2 if p % 2 else (zs - p // 2) % zs for p in range(zs)]
    position = {r: p for p, r in enumerate(offset)}

    def device(dz, to_x, dy, to_core):
        return (XS * lax.rem(z + dz, zs) + to_x, 2 * lax.rem(y + dy, planes) + to_core)

    def signal(target):
        pl.semaphore_signal(barrier, inc=1, device_id=target, device_id_type=MESH)

    def remote(src, dst, send, recv, target):
        return pltpu.make_async_remote_copy(src_ref=src, dst_ref=dst, send_sem=send, recv_sem=recv,
                                            device_id=target, device_id_type=MESH)

    far_first = sorted(range(1, zs), key=lambda q: -min(q, zs - q))
    barrier = pltpu.get_barrier_semaphore()
    for q in far_first:
        signal(device(q, x, 0, core))
    row_mate = [device(0, lax.rem(x + lax.rem(core + parity, 2) + 2 * v, XS), 0, parity) for v in range(2)]
    signal(row_mate[1])
    pl.when(jnp.logical_not(same))(lambda: signal(row_mate[0]))
    for d in (2, 1, 3):
        signal(device(0, x, d, core))
    partner = device(0, x, 0, 1 - core)
    signal(partner)

    pairs = ((tokens_hbm, tokens), (gain_hbm, gain), (routing_hbm, routing), (route_weight_hbm, route_weight),
             (gate_hbm.at[0], gate.at[0:share]), (up_hbm.at[0], up.at[0:share]), (down_hbm.at[0], down.at[0:share]))
    loads = [pltpu.make_async_copy(source, target, load_sem.at[i]) for i, (source, target) in enumerate(pairs)]
    for i in (0, 2, 1, 3, 4, 5, 6):
        loads[i].start()

    loads[0].wait()
    loads[2].wait()
    pl.semaphore_wait(barrier, zs - 1 + planes - 1 + 1 + 2 - same.astype(jnp.int32))

    def to_mate(v):
        remote(tokens, row_tokens.at[x // 2], row_send.at[0], row_recv.at[0], row_mate[v]).start()
        remote(routing, row_routing.at[x // 2], row_send.at[1], row_recv.at[1], row_mate[v]).start()
    to_mate(1)
    pl.when(jnp.logical_not(same))(lambda: to_mate(0))

    @pl.when(same)
    def _():
        row_tokens[x // 2] = tokens[...]
        row_routing[x // 2] = routing[...]

    loads[1].wait()
    loads[3].wait()
    for i in (4, 5, 6):
        loads[i].wait()
    swaps = [remote(ref.at[0:share], ref.at[share:2 * share], swap_send.at[i], swap_recv.at[i], partner)
             for i, ref in enumerate((gate, up, down))]
    for swap in swaps:
        swap.start()

    def wait_bytes(ref, number, sem):
        some = ref.at[pl.ds(0, number)]
        pltpu.make_async_copy(some, some, sem).wait()

    def wait_rows(sems):
        for ref, sem in zip((row_tokens, row_routing), sems):
            pl.when(same)(lambda ref=ref, sem=sem: wait_bytes(ref, 1, sem))
            pl.when(jnp.logical_not(same))(lambda ref=ref, sem=sem: wait_bytes(ref, 2, sem))
    wait_rows((row_recv.at[0], row_recv.at[1]))

    earlier = lax.broadcasted_iota(jnp.int32, (count, count), 0) < lax.broadcasted_iota(jnp.int32, (count, count), 1)
    earlier = jnp.where(earlier, 1.0, 0.0).astype(jnp.bfloat16)

    def slots_of(lines, expert_of, chosen, weights=None):
        line = lax.broadcasted_iota(jnp.int32, (lines, count), 0)
        expert = expert_of(line // CAP)
        member = jnp.zeros((lines, count), jnp.float32)
        weight = jnp.zeros((lines, count), jnp.float32)
        for k in range(chosen.shape[0]):
            named = chosen[k:k + 1, :] == expert
            member = jnp.where(named, 1.0, member)
            if weights is not None:
                weight = jnp.where(named, weights[k:k + 1, :], weight)
        before = jnp.dot(member.astype(jnp.bfloat16), earlier, preferred_element_type=jnp.float32)
        placed = jnp.where(before == lax.rem(line, CAP).astype(jnp.float32), member, 0.0)
        return placed, weight

    for u in range(2):
        placed, _ = slots_of(zs * CAP, lambda q: XS * lax.rem(z + q, zs) + x, row_routing[u])
        values = row_tokens[u].astype(jnp.float32)
        scale = lax.rsqrt(jnp.mean(values * values, axis=-1, keepdims=True) + norm_eps)
        normed = (values * scale * gain[...]).astype(jnp.bfloat16)
        sent = jnp.dot(placed.astype(jnp.bfloat16), normed, preferred_element_type=jnp.float32)
        outgoing[:, u] = sent.reshape(zs, CAP, width).astype(jnp.bfloat16)

    chunk_of = {p: k for k, (first, upto) in enumerate(CHUNKS) for p in range(first, upto)}
    for q in far_first:
        p = position[(zs - q) % zs]
        remote(outgoing.at[q], incoming.at[p], out_sem, in_sem.at[chunk_of[p]], device(q, x, 0, core)).start()
    incoming[0] = outgoing[0]

    def expert_at(place):
        p = place // XS
        away = jnp.where(lax.rem(p, 2) == 1, (p + 1) // 2, zs - p // 2)
        return XS * lax.rem(z - away + zs, zs) + lax.rem(place, XS)
    picked, weight = slots_of(groups * CAP, expert_at, routing[...], route_weight[...])
    weight = jnp.transpose(weight * picked)

    for swap in swaps:
        swap.wait_recv()

    def columns(d):
        return pl.ds(pl.multiple_of(lax.rem(y + d, planes) * tile, tile), tile)

    def give(d, k):
        first, upto = CHUNKS[k]
        some = pl.ds(first * 2 * CAP, (upto - first) * 2 * CAP)
        return remote(partial.at[d - 1, some], reduced.at[d - 1, some], part_send.at[d - 1, k], part_recv.at[d - 1, k],
                      device(0, x, d, core))

    last = (((1,), (1,)), ((), ()))
    totals = []
    for k, (first, upto) in enumerate(CHUNKS):
        wait_bytes(incoming, upto - max(first, 1), in_sem.at[k])
        rows = (upto - first) * 2 * CAP
        here = slice(first * 2 * CAP, upto * 2 * CAP)
        a = incoming[first:upto].astype(jnp.float32).reshape(rows, width).astype(jnp.bfloat16)
        gate_act = lax.dot_general(a, gate[...], last, preferred_element_type=jnp.float32)
        up_act = lax.dot_general(a, up[...], last, preferred_element_type=jnp.float32)
        hidden = (gate_act / (1.0 + jnp.exp(-gate_act)) * up_act).astype(jnp.bfloat16)
        for d in (2, 1, 3):
            partial[d - 1, here] = jnp.dot(hidden, down[:, columns(d)], preferred_element_type=jnp.float32)
            give(d, k).start()
        totals.append(jnp.dot(hidden, down[:, columns(0)], preferred_element_type=jnp.float32))

    for k, (first, upto) in enumerate(CHUNKS):
        here = slice(first * 2 * CAP, upto * 2 * CAP)
        mine = totals[k]
        for d in (1, 3, 2):
            give(d, k).wait_recv()
            mine = mine + reduced[d - 1, here]
        for side in range(2):
            back[side, first:upto] = mine[:, side * part:(side + 1) * part].reshape(upto - first, 2, CAP, part)
        for p in reversed(range(first, upto)):
            for u in range(2):
                to_x = core + 2 * u
                for side in range(2):
                    def send(p=p, u=u, side=side, to_x=to_x, k=k):
                        remote(back.at[side, p, u], arrived.at[p * XS + x], back_send, back_recv.at[k],
                               device(offset[p], to_x, 0, side)).start()

                    def hold(p=p, u=u, side=side):
                        arrived[p * XS + x] = back[side, p, u]
                    if p == 0:
                        mine_too = jnp.logical_and(to_x == x, core == side)
                        pl.when(mine_too)(hold)
                        pl.when(jnp.logical_not(mine_too))(send)
                    else:
                        send()

    def wait_blocks(number, own_too, sem):
        if own_too:
            pl.when(same)(lambda: wait_bytes(arrived, number - 1, sem))
            pl.when(jnp.logical_not(same))(lambda: wait_bytes(arrived, number, sem))
        else:
            wait_bytes(arrived, number, sem)

    flat = XS * CAP
    out = jnp.zeros((count, part), jnp.float32)
    for k, (first, upto) in enumerate(CHUNKS):
        wait_blocks((upto - first) * XS, first == 0, back_recv.at[k])
        out = out + jnp.dot(weight[:, first * flat:upto * flat], arrived[first * XS:upto * XS].reshape((upto - first) * flat, part),
                            precision=lax.Precision.HIGHEST, preferred_element_type=jnp.float32)
    mixed[...] = out.astype(mixed.dtype)

    wait_rows((row_send.at[0], row_send.at[1]))
    wait_bytes(outgoing, zs - 1, out_sem)
    for swap in swaps:
        swap.wait_send()
    for k in range(len(CHUNKS)):
        for d in range(1, planes):
            give(d, k).wait_send()
    wait_blocks(groups, True, back_send)


def solution(mesh):
    groups, shares = mesh.shape["ep"], mesh.shape["tp"]

    def local(tokens, norm_gain, routing, route_weight, w_gate, w_up, w_down):
        count, width = tokens.shape
        part = width // shares
        zs, planes = groups // XS, shares // 2
        rows = zs * 2 * CAP
        share = w_down.shape[1]
        chunks = len(CHUNKS)
        vmem = pl.BlockSpec(memory_space=pltpu.VMEM)
        hbm = pl.BlockSpec(memory_space=pltpu.HBM)
        dma = pltpu.SemaphoreType.DMA
        return pl.pallas_call(
            functools.partial(kernel, groups, shares),
            out_shape=jax.ShapeDtypeStruct((count, part), jnp.bfloat16),
            in_specs=[hbm] * 7,
            out_specs=vmem,
            scratch_shapes=[
                pltpu.VMEM((count, width), tokens.dtype),
                pltpu.VMEM((1, width), norm_gain.dtype),
                pltpu.VMEM(routing.shape[::-1], routing.dtype),
                pltpu.VMEM(route_weight.shape[::-1], route_weight.dtype),
                pltpu.VMEM((2 * share, width), jnp.bfloat16),
                pltpu.VMEM((2 * share, width), jnp.bfloat16),
                pltpu.VMEM((2 * share, width), jnp.bfloat16),
                pltpu.VMEM((2, count, width), tokens.dtype),
                pltpu.VMEM((2, *routing.shape[::-1]), routing.dtype),
                pltpu.VMEM((zs, 2, CAP, width), jnp.bfloat16),
                pltpu.VMEM((zs, 2, CAP, width), jnp.bfloat16),
                pltpu.VMEM((planes - 1, rows, 2 * part), jnp.float32),
                pltpu.VMEM((planes - 1, rows, 2 * part), jnp.float32),
                pltpu.VMEM((2, zs, 2, CAP, part), jnp.float32),
                pltpu.VMEM((groups, CAP, part), jnp.float32),
                dma((7,)), dma((2,)), dma((2,)), dma((3,)), dma((3,)), dma, dma((chunks,)),
                dma((planes - 1, chunks)), dma((planes - 1, chunks)), dma, dma((chunks,)),
            ],
            compiler_params=pltpu.CompilerParams(collective_id=0, has_side_effects=True,
                                                 vmem_limit_bytes=67043328),
            name="experts",
        )(tokens, norm_gain.reshape(1, width), routing.T, route_weight.T,
          jnp.swapaxes(w_gate, 1, 2), jnp.swapaxes(w_up, 1, 2), w_down)

    in_specs = (
        P("ep", None),
        P(),
        P("ep", None),
        P("ep", None),
        P("ep", None, "tp"),
        P("ep", None, "tp"),
        P("ep", "tp", None),
    )
    return jax.shard_map(local, mesh=mesh, in_specs=in_specs, out_specs=P("ep", "tp"), check_vma=False)
```

```python
import functools

import jax
import jax.numpy as jnp
from jax import lax
from jax.experimental import pallas as pl
from jax.experimental.pallas import tpu as pltpu
from jax.sharding import PartitionSpec as P

CAP = 8
CHUNKS = ((0, 16),)
PIECES = (((12, 16), (8, 12), (4, 8), (0, 4)),)
STEPS = ('c0', 'r0', 'r1', 'r2', 'r3')
MESH = pl.DeviceIdType.MESH

norm_eps = 1e-06


def kernel(groups, shares, tokens_hbm, gain_hbm, routing_hbm, route_weight_hbm, gate_hbm, up_hbm, down_hbm, mixed,
           tokens, gain, routing, route_weight, gate, up, down, gate_across, up_across,
           outgoing, incoming, partial, reduced, back, arrived,
           load_sem, swap_send, swap_recv, out_sem, in_sem, part_send, part_recv, back_send, back_recv):
    ep, tp = lax.axis_index("ep"), lax.axis_index("tp")
    width = tokens.shape[1]
    part = mixed.shape[1]
    half = groups // 2
    rows = half * CAP
    planes = shares // 2
    share = gate_hbm.shape[1]
    y, core = tp // 2, lax.rem(tp, 2)
    place, parity = ep // 2, lax.rem(ep, 2)
    own = (core == parity).astype(jnp.int32)
    offset = sorted(range(half), key=lambda q: min(q, half - q))
    position = {q: p for p, q in enumerate(offset)}
    chunk_of = {p: k for k, (first, upto) in enumerate(CHUNKS) for p in range(first, upto)}
    tile = 2 * part

    def group(q):
        return 2 * lax.rem(place + q, half) + core

    pairs = ((tokens_hbm, tokens), (gain_hbm, gain), (routing_hbm, routing), (route_weight_hbm, route_weight),
             (gate_hbm.at[0], gate.at[0:share]), (up_hbm.at[0], up.at[0:share]), (down_hbm.at[0], down.at[0:share]))
    loads = [pltpu.make_async_copy(source, target, load_sem.at[i]) for i, (source, target) in enumerate(pairs)]
    for i in (2, 3, 0, 1, 4, 5, 6):
        loads[i].start()

    far_first = sorted(range(half), key=lambda q: -min(q, half - q))
    barrier = pltpu.get_barrier_semaphore()
    for q in far_first:
        def greet(q=q):
            pl.semaphore_signal(barrier, inc=1, device_id=(group(q), 2 * y + parity), device_id_type=MESH)
        if q == 0:
            pl.when(core != parity)(greet)
        else:
            greet()
    for d in range(1, planes):
        pl.semaphore_signal(barrier, inc=1, device_id=(ep, 2 * lax.rem(y + d, planes) + core), device_id_type=MESH)
    pl.semaphore_signal(barrier, inc=1, device_id=(ep, 2 * y + 1 - core), device_id_type=MESH)

    count = tokens.shape[0]
    earlier = lax.broadcasted_iota(jnp.int32, (count, count), 0) < lax.broadcasted_iota(jnp.int32, (count, count), 1)
    earlier = jnp.where(earlier, 1.0, 0.0).astype(jnp.bfloat16)

    def slots_of(lines, expert_of):
        line = lax.broadcasted_iota(jnp.int32, (lines, count), 0)
        expert = expert_of(line // CAP)
        member = jnp.zeros((lines, count), jnp.float32)
        weight = jnp.zeros((lines, count), jnp.float32)
        for k in range(routing.shape[0]):
            named = routing[k:k + 1, :] == expert
            member = jnp.where(named, 1.0, member)
            weight = jnp.where(named, route_weight[k:k + 1, :], weight)
        before = jnp.dot(member.astype(jnp.bfloat16), earlier, preferred_element_type=jnp.float32)
        placed = jnp.where(before == lax.rem(line, CAP).astype(jnp.float32), member, 0.0)
        return placed, weight

    loads[2].wait()
    loads[3].wait()
    placed, _ = slots_of(rows, lambda q: group(q))
    loads[0].wait()
    loads[1].wait()
    values = tokens[...].astype(jnp.float32)
    scale = lax.rsqrt(jnp.mean(values * values, axis=-1, keepdims=True) + norm_eps)
    normed = (values * scale * gain[...]).astype(jnp.bfloat16)
    sent = jnp.dot(placed.astype(jnp.bfloat16), normed, preferred_element_type=jnp.float32)
    outgoing[...] = sent.reshape(half, CAP, width).astype(jnp.bfloat16)

    pl.semaphore_wait(barrier, half + planes - own)

    for q in far_first:
        at = position[(half - q) % half]

        def dispatch(q=q, at=at):
            pltpu.make_async_remote_copy(
                src_ref=outgoing.at[q], dst_ref=incoming.at[at], send_sem=out_sem, recv_sem=in_sem.at[chunk_of[at]],
                device_id=(group(q), 2 * y + parity), device_id_type=MESH).start()

        def keep(q=q, at=at):
            incoming[at] = outgoing[q]
        if q == 0:
            pl.when(core != parity)(dispatch)
            pl.when(core == parity)(keep)
        else:
            dispatch()

    swaps = [pltpu.make_async_remote_copy(
        src_ref=ref.at[0:share], dst_ref=ref.at[share:2 * share], send_sem=swap_send.at[i], recv_sem=swap_recv.at[i],
        device_id=(ep, 2 * y + 1 - core), device_id_type=MESH) for i, ref in enumerate((gate, up, down))]
    for i in (4, 5, 6):
        loads[i].wait()
    for swap in swaps:
        swap.start()

    picked, weight = slots_of(groups * CAP, lambda q: q)
    weight = jnp.transpose(weight * picked)

    for swap in swaps:
        swap.wait_recv()
    gate_across[...] = jnp.transpose(gate[...])
    up_across[...] = jnp.transpose(up[...])

    def wait_for(ref, sem, most):
        less, full = ref.at[pl.ds(0, most - 1)], ref.at[pl.ds(0, most)]
        pl.when(core == parity)(lambda: pltpu.make_async_copy(less, less, sem).wait())
        pl.when(core != parity)(lambda: pltpu.make_async_copy(full, full, sem).wait())

    order = sorted(range(1, planes), key=lambda d: -min(d, planes - d))
    pieces = [piece for some in PIECES for piece in some]
    totals = {}

    def columns(d):
        return pl.ds(pl.multiple_of(lax.rem(y + d, planes) * tile, tile), tile)

    def give(d, piece):
        some = pl.ds(piece[0] * CAP, (piece[1] - piece[0]) * CAP)
        sems = part_send.at[d - 1, pieces.index(piece)], part_recv.at[d - 1, pieces.index(piece)]
        return pltpu.make_async_remote_copy(
            src_ref=partial.at[d - 1, some], dst_ref=reduced.at[d - 1, some], send_sem=sems[0], recv_sem=sems[1],
            device_id=(ep, 2 * lax.rem(y + d, planes) + core), device_id_type=MESH)

    def multiply(k):
        first, upto = CHUNKS[k]
        if first == 0:
            wait_for(incoming, in_sem.at[k], upto)
        else:
            some = incoming.at[pl.ds(first, upto - first)]
            pltpu.make_async_copy(some, some, in_sem.at[k]).wait()
        x = incoming[first:upto].astype(jnp.float32).reshape((upto - first) * CAP, width).astype(jnp.bfloat16)
        gate_act = jnp.dot(x, gate_across[...], preferred_element_type=jnp.float32)
        up_act = jnp.dot(x, up_across[...], preferred_element_type=jnp.float32)
        hidden = (gate_act / (1.0 + jnp.exp(-gate_act)) * up_act).astype(jnp.bfloat16)
        for d in order:
            partial[d - 1, first * CAP:upto * CAP] = jnp.dot(hidden, down[:, columns(d)],
                                                             preferred_element_type=jnp.float32)
            give(d, PIECES[k][0]).start()
        for piece in PIECES[k][1:]:
            for d in order:
                give(d, piece).start()
        mine = jnp.dot(hidden, down[:, columns(0)], preferred_element_type=jnp.float32)
        for piece in PIECES[k]:
            totals[piece] = mine[(piece[0] - first) * CAP:(piece[1] - first) * CAP]

    def give_back(k):
        piece = pieces[k]
        first, upto = piece
        mine = totals[piece]
        for d in range(1, planes):
            give(d, piece).wait_recv()
        for d in range(1, planes):
            mine = mine + reduced[d - 1, first * CAP:upto * CAP]
        for side in range(2):
            back[side, first:upto] = mine[:, side * part:(side + 1) * part].reshape(upto - first, CAP, part)
        for at in reversed(range(first, upto)):
            for side in range(2):
                def send(at=at, side=side):
                    pltpu.make_async_remote_copy(
                        src_ref=back.at[side, at], dst_ref=arrived.at[ep], send_sem=back_send, recv_sem=back_recv,
                        device_id=(group(offset[at]), 2 * y + side), device_id_type=MESH).start()

                def hold(at=at, side=side):
                    arrived[ep] = back[side, at]
                if at == 0:
                    here = jnp.logical_and(core == parity, core == side)
                    pl.when(here)(hold)
                    pl.when(jnp.logical_not(here))(send)
                else:
                    send()

    for step in STEPS:
        (multiply if step[0] == "c" else give_back)(int(step[1:]))

    wait_for(arrived, back_recv, groups)
    out = jnp.dot(weight, arrived[...].reshape(groups * CAP, part), precision=lax.Precision.HIGHEST,
                  preferred_element_type=jnp.float32)
    mixed[...] = out.astype(mixed.dtype)
    wait_for(outgoing, out_sem, half)
    for swap in swaps:
        swap.wait_send()
    for piece in pieces:
        for d in range(1, planes):
            give(d, piece).wait_send()
    wait_for(arrived, back_send, groups)


def solution(mesh):
    groups, shares = mesh.shape["ep"], mesh.shape["tp"]

    def local(tokens, norm_gain, routing, route_weight, w_gate, w_up, w_down):
        count, width = tokens.shape
        part = width // shares
        half, planes = groups // 2, shares // 2
        rows = half * CAP
        share = w_down.shape[1]
        pieces = sum(map(len, PIECES))
        vmem = pl.BlockSpec(memory_space=pltpu.VMEM)
        hbm = pl.BlockSpec(memory_space=pltpu.HBM)
        return pl.pallas_call(
            functools.partial(kernel, groups, shares),
            out_shape=pltpu.VMEM((count, part), jnp.bfloat16),
            in_specs=[hbm] * 7,
            out_specs=vmem,
            scratch_shapes=[
                pltpu.VMEM((count, width), tokens.dtype),
                pltpu.VMEM((1, width), norm_gain.dtype),
                pltpu.VMEM(routing.shape[::-1], routing.dtype),
                pltpu.VMEM(route_weight.shape[::-1], route_weight.dtype),
                pltpu.VMEM((2 * share, width), jnp.bfloat16),
                pltpu.VMEM((2 * share, width), jnp.bfloat16),
                pltpu.VMEM((2 * share, width), jnp.bfloat16),
                pltpu.VMEM((width, 2 * share), jnp.bfloat16),
                pltpu.VMEM((width, 2 * share), jnp.bfloat16),
                pltpu.VMEM((half, CAP, width), jnp.bfloat16),
                pltpu.VMEM((half, CAP, width), jnp.bfloat16),
                pltpu.VMEM((planes - 1, rows, 2 * part), jnp.float32),
                pltpu.VMEM((planes - 1, rows, 2 * part), jnp.float32),
                pltpu.VMEM((2, half, CAP, part), jnp.float32),
                pltpu.VMEM((groups, CAP, part), jnp.float32),
                pltpu.SemaphoreType.DMA((7,)),
                pltpu.SemaphoreType.DMA((3,)),
                pltpu.SemaphoreType.DMA((3,)),
                pltpu.SemaphoreType.DMA,
                pltpu.SemaphoreType.DMA((len(CHUNKS),)),
                pltpu.SemaphoreType.DMA((planes - 1, pieces)),
                pltpu.SemaphoreType.DMA((planes - 1, pieces)),
                pltpu.SemaphoreType.DMA,
                pltpu.SemaphoreType.DMA,
            ],
            compiler_params=pltpu.CompilerParams(collective_id=0, has_side_effects=True,
                                                 vmem_limit_bytes=67043328 - 16384),
            name="experts",
        )(tokens, norm_gain.reshape(1, width), routing.T, route_weight.T,
          jnp.swapaxes(w_gate, 1, 2), jnp.swapaxes(w_up, 1, 2), w_down)

    in_specs = (
        P("ep", None),
        P(),
        P("ep", None),
        P("ep", None),
        P("ep", None, "tp"),
        P("ep", None, "tp"),
        P("ep", "tp", None),
    )
    return jax.shard_map(local, mesh=mesh, in_specs=in_specs, out_specs=P("ep", "tp"), check_vma=False)
```

```python
import functools

import jax
import jax.numpy as jnp
from jax import lax
from jax.experimental import pallas as pl
from jax.experimental.pallas import tpu as pltpu
from jax.sharding import PartitionSpec as P

CAP = 8
CHUNKS = ((0, 16),)
PIECES = (((12, 16), (8, 12), (4, 8), (0, 4)),)
STEPS = ('c0', 'r0', 'r1', 'r2', 'r3')
STEPS_16 = 32767.0
LEAST = 2e-34
MESH = pl.DeviceIdType.MESH

norm_eps = 1e-06


def kernel(groups, shares, tokens_hbm, gain_hbm, routing_hbm, route_weight_hbm, gate_hbm, up_hbm, down_hbm, mixed,
           tokens, gain, routing, route_weight, gate, up, down, gate_across, up_across,
           outgoing, incoming, partial, reduced, peak, their_peak, back, arrived,
           load_sem, swap_send, swap_recv, out_sem, in_sem, part_send, part_recv, peak_send, peak_recv, back_send, back_recv):
    ep, tp = lax.axis_index("ep"), lax.axis_index("tp")
    width = tokens.shape[1]
    part = mixed.shape[1]
    half = groups // 2
    rows = half * CAP
    planes = shares // 2
    share = gate_hbm.shape[1]
    y, core = tp // 2, lax.rem(tp, 2)
    place, parity = ep // 2, lax.rem(ep, 2)
    own = (core == parity).astype(jnp.int32)
    offset = sorted(range(half), key=lambda q: min(q, half - q))
    position = {q: p for p, q in enumerate(offset)}
    chunk_of = {p: k for k, (first, upto) in enumerate(CHUNKS) for p in range(first, upto)}
    tile = 2 * part

    def group(q):
        return 2 * lax.rem(place + q, half) + core

    pairs = ((tokens_hbm, tokens), (gain_hbm, gain), (routing_hbm, routing), (route_weight_hbm, route_weight),
             (gate_hbm.at[0], gate.at[0:share]), (up_hbm.at[0], up.at[0:share]), (down_hbm.at[0], down.at[0:share]))
    loads = [pltpu.make_async_copy(source, target, load_sem.at[i]) for i, (source, target) in enumerate(pairs)]
    for i in (2, 3, 0, 1, 4, 5, 6):
        loads[i].start()

    far_first = sorted(range(half), key=lambda q: -min(q, half - q))
    barrier = pltpu.get_barrier_semaphore()
    for q in far_first:
        def greet(q=q):
            pl.semaphore_signal(barrier, inc=1, device_id=(group(q), 2 * y + parity), device_id_type=MESH)
        if q == 0:
            pl.when(core != parity)(greet)
        else:
            greet()
    for d in range(1, planes):
        pl.semaphore_signal(barrier, inc=1, device_id=(ep, 2 * lax.rem(y + d, planes) + core), device_id_type=MESH)
    pl.semaphore_signal(barrier, inc=1, device_id=(ep, 2 * y + 1 - core), device_id_type=MESH)

    count = tokens.shape[0]
    earlier = lax.broadcasted_iota(jnp.int32, (count, count), 0) < lax.broadcasted_iota(jnp.int32, (count, count), 1)
    earlier = jnp.where(earlier, 1.0, 0.0).astype(jnp.bfloat16)

    def slots_of(lines, expert_of):
        line = lax.broadcasted_iota(jnp.int32, (lines, count), 0)
        expert = expert_of(line // CAP)
        member = jnp.zeros((lines, count), jnp.float32)
        weight = jnp.zeros((lines, count), jnp.float32)
        for k in range(routing.shape[0]):
            named = routing[k:k + 1, :] == expert
            member = jnp.where(named, 1.0, member)
            weight = jnp.where(named, route_weight[k:k + 1, :], weight)
        before = jnp.dot(member.astype(jnp.bfloat16), earlier, preferred_element_type=jnp.float32)
        placed = jnp.where(before == lax.rem(line, CAP).astype(jnp.float32), member, 0.0)
        return placed, weight

    loads[2].wait()
    loads[3].wait()
    placed, _ = slots_of(rows, lambda q: group(q))
    loads[0].wait()
    loads[1].wait()
    values = tokens[...].astype(jnp.float32)
    scale = lax.rsqrt(jnp.mean(values * values, axis=-1, keepdims=True) + norm_eps)
    normed = (values * scale * gain[...]).astype(jnp.bfloat16)
    sent = jnp.dot(placed.astype(jnp.bfloat16), normed, preferred_element_type=jnp.float32)
    outgoing[...] = sent.reshape(half, CAP, width).astype(jnp.bfloat16)

    pl.semaphore_wait(barrier, half + planes - own)

    for q in far_first:
        at = position[(half - q) % half]

        def dispatch(q=q, at=at):
            pltpu.make_async_remote_copy(
                src_ref=outgoing.at[q], dst_ref=incoming.at[at], send_sem=out_sem, recv_sem=in_sem.at[chunk_of[at]],
                device_id=(group(q), 2 * y + parity), device_id_type=MESH).start()

        def keep(q=q, at=at):
            incoming[at] = outgoing[q]
        if q == 0:
            pl.when(core != parity)(dispatch)
            pl.when(core == parity)(keep)
        else:
            dispatch()

    swaps = [pltpu.make_async_remote_copy(
        src_ref=ref.at[0:share], dst_ref=ref.at[share:2 * share], send_sem=swap_send.at[i], recv_sem=swap_recv.at[i],
        device_id=(ep, 2 * y + 1 - core), device_id_type=MESH) for i, ref in enumerate((gate, up, down))]
    for i in (4, 5, 6):
        loads[i].wait()
    for swap in swaps:
        swap.start()

    picked, weight = slots_of(groups * CAP, lambda q: q)
    weight = jnp.transpose(weight * picked)

    for swap in swaps:
        swap.wait_recv()
    gate_across[...] = jnp.transpose(gate[...])
    up_across[...] = jnp.transpose(up[...])

    def wait_for(ref, sem, most):
        less, full = ref.at[pl.ds(0, most - 1)], ref.at[pl.ds(0, most)]
        pl.when(core == parity)(lambda: pltpu.make_async_copy(less, less, sem).wait())
        pl.when(core != parity)(lambda: pltpu.make_async_copy(full, full, sem).wait())

    order = sorted(range(1, planes), key=lambda d: -min(d, planes - d))
    pieces = [piece for some in PIECES for piece in some]
    totals = {}

    def columns(d):
        return pl.ds(pl.multiple_of(lax.rem(y + d, planes) * tile, tile), tile)

    def give(d, piece):
        some = pl.ds(piece[0] * CAP, (piece[1] - piece[0]) * CAP)
        sems = part_send.at[d - 1, pieces.index(piece)], part_recv.at[d - 1, pieces.index(piece)]
        return pltpu.make_async_remote_copy(
            src_ref=partial.at[d - 1, some], dst_ref=reduced.at[d - 1, some], send_sem=sems[0], recv_sem=sems[1],
            device_id=(ep, 2 * lax.rem(y + d, planes) + core), device_id_type=MESH)

    def give_peak(d):
        return pltpu.make_async_remote_copy(
            src_ref=peak.at[d - 1], dst_ref=their_peak.at[d - 1], send_sem=peak_send.at[d - 1],
            recv_sem=peak_recv.at[d - 1], device_id=(ep, 2 * lax.rem(y + d, planes) + core), device_id_type=MESH)

    def multiply(k):
        first, upto = CHUNKS[k]
        if first == 0:
            wait_for(incoming, in_sem.at[k], upto)
        else:
            some = incoming.at[pl.ds(first, upto - first)]
            pltpu.make_async_copy(some, some, in_sem.at[k]).wait()
        x = incoming[first:upto].astype(jnp.float32).reshape((upto - first) * CAP, width).astype(jnp.bfloat16)
        gate_act = jnp.dot(x, gate_across[...], preferred_element_type=jnp.float32)
        up_act = jnp.dot(x, up_across[...], preferred_element_type=jnp.float32)
        hidden = (gate_act / (1.0 + jnp.exp(-gate_act)) * up_act).astype(jnp.bfloat16)
        for d in order:
            block = jnp.dot(hidden, down[:, columns(d)], preferred_element_type=jnp.float32)
            sides = [block[:, side * part:(side + 1) * part].reshape(upto - first, CAP, part) for side in range(2)]
            most = jnp.maximum(jnp.max(jnp.maximum(jnp.abs(sides[0]), jnp.abs(sides[1])), axis=0), LEAST)
            peak[d - 1] = most
            give_peak(d).start()
            for side in range(2):
                coded = jnp.round(sides[side] * (STEPS_16 / most)).reshape((upto - first) * CAP, part)
                partial[d - 1, first * CAP:upto * CAP, side * part:(side + 1) * part] = (
                    coded.astype(jnp.int32).astype(jnp.int16))
            give(d, PIECES[k][0]).start()
        for piece in PIECES[k][1:]:
            for d in order:
                give(d, piece).start()
        mine = jnp.dot(hidden, down[:, columns(0)], preferred_element_type=jnp.float32)
        for piece in PIECES[k]:
            totals[piece] = mine[(piece[0] - first) * CAP:(piece[1] - first) * CAP]

    def give_back(k):
        piece = pieces[k]
        first, upto = piece
        mine = totals[piece]
        for d in range(1, planes):
            if k == 0:
                give_peak(d).wait_recv()
            give(d, piece).wait_recv()
        for side in range(2):
            columns_here = slice(side * part, (side + 1) * part)
            total = mine[:, columns_here].reshape(upto - first, CAP, part)
            for d in range(1, planes):
                coded = reduced[d - 1, first * CAP:upto * CAP, columns_here].astype(jnp.int32).astype(jnp.float32)
                total = total + coded.reshape(upto - first, CAP, part) * (their_peak[d - 1] * (1.0 / STEPS_16))
            back[side, first:upto] = total
        for at in reversed(range(first, upto)):
            for side in range(2):
                def send(at=at, side=side):
                    pltpu.make_async_remote_copy(
                        src_ref=back.at[side, at], dst_ref=arrived.at[ep], send_sem=back_send, recv_sem=back_recv,
                        device_id=(group(offset[at]), 2 * y + side), device_id_type=MESH).start()

                def hold(at=at, side=side):
                    arrived[ep] = back[side, at]
                if at == 0:
                    here = jnp.logical_and(core == parity, core == side)
                    pl.when(here)(hold)
                    pl.when(jnp.logical_not(here))(send)
                else:
                    send()

    for step in STEPS:
        (multiply if step[0] == "c" else give_back)(int(step[1:]))

    wait_for(arrived, back_recv, groups)
    out = jnp.dot(weight, arrived[...].reshape(groups * CAP, part), precision=lax.Precision.HIGHEST,
                  preferred_element_type=jnp.float32)
    mixed[...] = out.astype(mixed.dtype)
    wait_for(outgoing, out_sem, half)
    for swap in swaps:
        swap.wait_send()
    for d in range(1, planes):
        give_peak(d).wait_send()
    for piece in pieces:
        for d in range(1, planes):
            give(d, piece).wait_send()
    wait_for(arrived, back_send, groups)


def solution(mesh):
    groups, shares = mesh.shape["ep"], mesh.shape["tp"]

    def local(tokens, norm_gain, routing, route_weight, w_gate, w_up, w_down):
        count, width = tokens.shape
        part = width // shares
        half, planes = groups // 2, shares // 2
        rows = half * CAP
        share = w_down.shape[1]
        pieces = sum(map(len, PIECES))
        vmem = pl.BlockSpec(memory_space=pltpu.VMEM)
        hbm = pl.BlockSpec(memory_space=pltpu.HBM)
        return pl.pallas_call(
            functools.partial(kernel, groups, shares),
            out_shape=pltpu.VMEM((count, part), jnp.bfloat16),
            in_specs=[hbm] * 7,
            out_specs=vmem,
            scratch_shapes=[
                pltpu.VMEM((count, width), tokens.dtype),
                pltpu.VMEM((1, width), norm_gain.dtype),
                pltpu.VMEM(routing.shape[::-1], routing.dtype),
                pltpu.VMEM(route_weight.shape[::-1], route_weight.dtype),
                pltpu.VMEM((2 * share, width), jnp.bfloat16),
                pltpu.VMEM((2 * share, width), jnp.bfloat16),
                pltpu.VMEM((2 * share, width), jnp.bfloat16),
                pltpu.VMEM((width, 2 * share), jnp.bfloat16),
                pltpu.VMEM((width, 2 * share), jnp.bfloat16),
                pltpu.VMEM((half, CAP, width), jnp.bfloat16),
                pltpu.VMEM((half, CAP, width), jnp.bfloat16),
                pltpu.VMEM((planes - 1, rows, 2 * part), jnp.int16),
                pltpu.VMEM((planes - 1, rows, 2 * part), jnp.int16),
                pltpu.VMEM((planes - 1, CAP, part), jnp.float32),
                pltpu.VMEM((planes - 1, CAP, part), jnp.float32),
                pltpu.VMEM((2, half, CAP, part), jnp.float32),
                pltpu.VMEM((groups, CAP, part), jnp.float32),
                pltpu.SemaphoreType.DMA((7,)),
                pltpu.SemaphoreType.DMA((3,)),
                pltpu.SemaphoreType.DMA((3,)),
                pltpu.SemaphoreType.DMA,
                pltpu.SemaphoreType.DMA((len(CHUNKS),)),
                pltpu.SemaphoreType.DMA((planes - 1, pieces)),
                pltpu.SemaphoreType.DMA((planes - 1, pieces)),
                pltpu.SemaphoreType.DMA((planes - 1,)),
                pltpu.SemaphoreType.DMA((planes - 1,)),
                pltpu.SemaphoreType.DMA,
                pltpu.SemaphoreType.DMA,
            ],
            compiler_params=pltpu.CompilerParams(collective_id=0, has_side_effects=True,
                                                 vmem_limit_bytes=67043328 - 16384),
            name="experts",
        )(tokens, norm_gain.reshape(1, width), routing.T, route_weight.T,
          jnp.swapaxes(w_gate, 1, 2), jnp.swapaxes(w_up, 1, 2), w_down)

    in_specs = (
        P("ep", None),
        P(),
        P("ep", None),
        P("ep", None),
        P("ep", None, "tp"),
        P("ep", None, "tp"),
        P("ep", "tp", None),
    )
    return jax.shard_map(local, mesh=mesh, in_specs=in_specs, out_specs=P("ep", "tp"), check_vma=False)
```

```python
import functools

import jax
import jax.numpy as jnp
from jax import lax
from jax.experimental import pallas as pl
from jax.experimental.pallas import tpu as pltpu
from jax.sharding import PartitionSpec as P

CAP = 8
XS = 4
CHUNKS = ((0, 16),)
PIECES = (((12, 16), (8, 12), (4, 8), (0, 4)),)
STEPS = ('c0', 'r0', 'r1', 'r2', 'r3')
STEPS_16 = 32767.0
LEAST = 2e-34
MESH = pl.DeviceIdType.MESH

norm_eps = 1e-06


def tables(zs, xs):
    steps = [(dz, dx) for dz in range(zs) for dx in range(xs)]
    inverse = {(dz, dx): ((zs - dz) % zs, (xs - dx) % xs) for dz, dx in steps}
    hops = lambda step: min(step[0], zs - step[0]) + min(step[1], xs - step[1])
    alone = sorted((step for step in steps if inverse[step] == step), key=hops)
    paired = sorted((step for step in steps if step < inverse[step]), key=hops)
    near, far = [], []
    for some, single, double in ((near, alone[:2], paired[:len(paired) // 2]), (far, alone[2:], paired[len(paired) // 2:])):
        some.append(single[0])
        for step in double:
            some += [step, inverse[step]]
        some.append(single[1])
    return near, far, [near.index(inverse[step]) for step in near]


def kernel(groups, shares, tokens_hbm, gain_hbm, routing_hbm, route_weight_hbm, gate_hbm, up_hbm, down_hbm, mixed,
           tokens, gain, routing, route_weight, gate, up, down, gate_across, up_across,
           outgoing, incoming, partial, reduced, peak, their_peak, back, arrived,
           load_sem, swap_send, swap_recv, out_sem, in_sem, part_send, part_recv, peak_send, peak_recv, back_send, back_recv):
    ep, tp = lax.axis_index("ep"), lax.axis_index("tp")
    width = tokens.shape[1]
    part = mixed.shape[1]
    half = groups // 2
    rows = half * CAP
    planes = shares // 2
    share = gate_hbm.shape[1]
    y, core = tp // 2, lax.rem(tp, 2)
    near, far, back_at = tables(groups // XS, XS)

    def group(p):
        dz, dx = (n + (f - n) * core for n, f in zip(near[p], far[p]))
        return XS * lax.rem(ep // XS + dz, groups // XS) + lax.rem(lax.rem(ep, XS) + dx, XS)

    chunk_of = {p: k for k, (first, upto) in enumerate(CHUNKS) for p in range(first, upto)}
    tile = 2 * part

    barrier = pltpu.get_barrier_semaphore()
    for p in reversed(range(half)):
        def greet(p=p):
            pl.semaphore_signal(barrier, inc=1, device_id=(group(p), tp), device_id_type=MESH)
        if p == 0:
            pl.when(core == 1)(greet)
        else:
            greet()
    for d in range(1, planes):
        pl.semaphore_signal(barrier, inc=1, device_id=(ep, 2 * lax.rem(y + d, planes) + core), device_id_type=MESH)
    pl.semaphore_signal(barrier, inc=1, device_id=(ep, 2 * y + 1 - core), device_id_type=MESH)

    pairs = ((tokens_hbm, tokens), (gain_hbm, gain), (routing_hbm, routing), (route_weight_hbm, route_weight),
             (gate_hbm.at[0], gate.at[0:share]), (up_hbm.at[0], up.at[0:share]), (down_hbm.at[0], down.at[0:share]))
    loads = [pltpu.make_async_copy(source, target, load_sem.at[i]) for i, (source, target) in enumerate(pairs)]
    for i in (2, 3, 0, 1, 4, 5, 6):
        loads[i].start()

    count = tokens.shape[0]
    earlier = lax.broadcasted_iota(jnp.int32, (count, count), 0) < lax.broadcasted_iota(jnp.int32, (count, count), 1)
    earlier = jnp.where(earlier, 1.0, 0.0).astype(jnp.bfloat16)

    def slots_of(lines, expert_of):
        line = lax.broadcasted_iota(jnp.int32, (lines, count), 0)
        expert = expert_of(line // CAP)
        member = jnp.zeros((lines, count), jnp.float32)
        weight = jnp.zeros((lines, count), jnp.float32)
        for k in range(routing.shape[0]):
            named = routing[k:k + 1, :] == expert
            member = jnp.where(named, 1.0, member)
            weight = jnp.where(named, route_weight[k:k + 1, :], weight)
        before = jnp.dot(member.astype(jnp.bfloat16), earlier, preferred_element_type=jnp.float32)
        placed = jnp.where(before == lax.rem(line, CAP).astype(jnp.float32), member, 0.0)
        return placed, weight

    loads[2].wait()
    loads[3].wait()

    def named_at(line):
        expert = jnp.zeros_like(line)
        for p in range(half):
            expert = jnp.where(line == p, group(p), expert)
        return expert
    placed, _ = slots_of(rows, named_at)
    loads[0].wait()
    loads[1].wait()
    values = tokens[...].astype(jnp.float32)
    scale = lax.rsqrt(jnp.mean(values * values, axis=-1, keepdims=True) + norm_eps)
    normed = (values * scale * gain[...]).astype(jnp.bfloat16)
    sent = jnp.dot(placed.astype(jnp.bfloat16), normed, preferred_element_type=jnp.float32)
    outgoing[...] = sent.reshape(half, CAP, width).astype(jnp.bfloat16)

    pl.semaphore_wait(barrier, half + planes - 1 + core)

    for p in reversed(range(half)):
        def dispatch(p=p):
            pltpu.make_async_remote_copy(
                src_ref=outgoing.at[p], dst_ref=incoming.at[back_at[p]], send_sem=out_sem,
                recv_sem=in_sem.at[chunk_of[back_at[p]]], device_id=(group(p), tp), device_id_type=MESH).start()

        def keep(p=p):
            incoming[p] = outgoing[p]
        if p == 0:
            pl.when(core == 1)(dispatch)
            pl.when(core == 0)(keep)
        else:
            dispatch()

    swaps = [pltpu.make_async_remote_copy(
        src_ref=ref.at[0:share], dst_ref=ref.at[share:2 * share], send_sem=swap_send.at[i], recv_sem=swap_recv.at[i],
        device_id=(ep, 2 * y + 1 - core), device_id_type=MESH) for i, ref in enumerate((gate, up, down))]
    for i in (4, 5, 6):
        loads[i].wait()
    for swap in swaps:
        swap.start()

    picked, weight = slots_of(groups * CAP, lambda q: q)
    weight = jnp.transpose(weight * picked)

    for swap in swaps:
        swap.wait_recv()
    gate_across[...] = jnp.transpose(gate[...])
    up_across[...] = jnp.transpose(up[...])

    def wait_for(ref, sem, most):
        less, full = ref.at[pl.ds(0, most - 1)], ref.at[pl.ds(0, most)]
        pl.when(core == 0)(lambda: pltpu.make_async_copy(less, less, sem).wait())
        pl.when(core == 1)(lambda: pltpu.make_async_copy(full, full, sem).wait())

    order = sorted(range(1, planes), key=lambda d: -min(d, planes - d))
    pieces = [piece for some in PIECES for piece in some]
    totals = {}

    def columns(d):
        return pl.ds(pl.multiple_of(lax.rem(y + d, planes) * tile, tile), tile)

    def give(d, piece):
        some = pl.ds(piece[0] * CAP, (piece[1] - piece[0]) * CAP)
        sems = part_send.at[d - 1, pieces.index(piece)], part_recv.at[d - 1, pieces.index(piece)]
        return pltpu.make_async_remote_copy(
            src_ref=partial.at[d - 1, some], dst_ref=reduced.at[d - 1, some], send_sem=sems[0], recv_sem=sems[1],
            device_id=(ep, 2 * lax.rem(y + d, planes) + core), device_id_type=MESH)

    def give_peak(d):
        return pltpu.make_async_remote_copy(
            src_ref=peak.at[d - 1], dst_ref=their_peak.at[d - 1], send_sem=peak_send.at[d - 1],
            recv_sem=peak_recv.at[d - 1], device_id=(ep, 2 * lax.rem(y + d, planes) + core), device_id_type=MESH)

    def multiply(k):
        first, upto = CHUNKS[k]
        if first == 0:
            wait_for(incoming, in_sem.at[k], upto)
        else:
            some = incoming.at[pl.ds(first, upto - first)]
            pltpu.make_async_copy(some, some, in_sem.at[k]).wait()
        x = incoming[first:upto].astype(jnp.float32).reshape((upto - first) * CAP, width).astype(jnp.bfloat16)
        gate_act = jnp.dot(x, gate_across[...], preferred_element_type=jnp.float32)
        up_act = jnp.dot(x, up_across[...], preferred_element_type=jnp.float32)
        hidden = (gate_act / (1.0 + jnp.exp(-gate_act)) * up_act).astype(jnp.bfloat16)
        for d in order:
            block = jnp.dot(hidden, down[:, columns(d)], preferred_element_type=jnp.float32)
            sides = [block[:, side * part:(side + 1) * part].reshape(upto - first, CAP, part) for side in range(2)]
            most = jnp.maximum(jnp.max(jnp.maximum(jnp.abs(sides[0]), jnp.abs(sides[1])), axis=0), LEAST)
            peak[d - 1] = most
            give_peak(d).start()
            for side in range(2):
                coded = jnp.round(sides[side] * (STEPS_16 / most)).reshape((upto - first) * CAP, part)
                partial[d - 1, first * CAP:upto * CAP, side * part:(side + 1) * part] = (
                    coded.astype(jnp.int32).astype(jnp.int16))
            give(d, PIECES[k][0]).start()
        for piece in PIECES[k][1:]:
            for d in order:
                give(d, piece).start()
        mine = jnp.dot(hidden, down[:, columns(0)], preferred_element_type=jnp.float32)
        for piece in PIECES[k]:
            totals[piece] = mine[(piece[0] - first) * CAP:(piece[1] - first) * CAP]

    def give_back(k):
        piece = pieces[k]
        first, upto = piece
        mine = totals[piece]
        for d in range(1, planes):
            if k == 0:
                give_peak(d).wait_recv()
            give(d, piece).wait_recv()
        for side in range(2):
            columns_here = slice(side * part, (side + 1) * part)
            total = mine[:, columns_here].reshape(upto - first, CAP, part)
            for d in range(1, planes):
                coded = reduced[d - 1, first * CAP:upto * CAP, columns_here].astype(jnp.int32).astype(jnp.float32)
                total = total + coded.reshape(upto - first, CAP, part) * (their_peak[d - 1] * (1.0 / STEPS_16))
            back[side, first:upto] = total
        for at in reversed(range(first, upto)):
            for side in range(2):
                def send(at=at, side=side):
                    pltpu.make_async_remote_copy(
                        src_ref=back.at[side, at], dst_ref=arrived.at[ep], send_sem=back_send, recv_sem=back_recv,
                        device_id=(group(at), 2 * y + side), device_id_type=MESH).start()

                def hold(at=at, side=side):
                    arrived[ep] = back[side, at]
                if at == 0:
                    if side == 0:
                        pl.when(core == 0)(hold)
                        pl.when(core == 1)(send)
                    else:
                        send()
                else:
                    send()

    for step in STEPS:
        (multiply if step[0] == "c" else give_back)(int(step[1:]))

    wait_for(arrived, back_recv, groups)
    out = jnp.dot(weight, arrived[...].reshape(groups * CAP, part), precision=lax.Precision.HIGHEST,
                  preferred_element_type=jnp.float32)
    mixed[...] = out.astype(mixed.dtype)
    wait_for(outgoing, out_sem, half)
    for swap in swaps:
        swap.wait_send()
    for d in range(1, planes):
        give_peak(d).wait_send()
    for piece in pieces:
        for d in range(1, planes):
            give(d, piece).wait_send()
    wait_for(arrived, back_send, groups)


def solution(mesh):
    groups, shares = mesh.shape["ep"], mesh.shape["tp"]

    def local(tokens, norm_gain, routing, route_weight, w_gate, w_up, w_down):
        count, width = tokens.shape
        part = width // shares
        half, planes = groups // 2, shares // 2
        rows = half * CAP
        share = w_down.shape[1]
        pieces = sum(map(len, PIECES))
        vmem = pl.BlockSpec(memory_space=pltpu.VMEM)
        hbm = pl.BlockSpec(memory_space=pltpu.HBM)
        return pl.pallas_call(
            functools.partial(kernel, groups, shares),
            out_shape=pltpu.VMEM((count, part), jnp.bfloat16),
            in_specs=[hbm] * 7,
            out_specs=vmem,
            scratch_shapes=[
                pltpu.VMEM((count, width), tokens.dtype),
                pltpu.VMEM((1, width), norm_gain.dtype),
                pltpu.VMEM(routing.shape[::-1], routing.dtype),
                pltpu.VMEM(route_weight.shape[::-1], route_weight.dtype),
                pltpu.VMEM((2 * share, width), jnp.bfloat16),
                pltpu.VMEM((2 * share, width), jnp.bfloat16),
                pltpu.VMEM((2 * share, width), jnp.bfloat16),
                pltpu.VMEM((width, 2 * share), jnp.bfloat16),
                pltpu.VMEM((width, 2 * share), jnp.bfloat16),
                pltpu.VMEM((half, CAP, width), jnp.bfloat16),
                pltpu.VMEM((half, CAP, width), jnp.bfloat16),
                pltpu.VMEM((planes - 1, rows, 2 * part), jnp.int16),
                pltpu.VMEM((planes - 1, rows, 2 * part), jnp.int16),
                pltpu.VMEM((planes - 1, CAP, part), jnp.float32),
                pltpu.VMEM((planes - 1, CAP, part), jnp.float32),
                pltpu.VMEM((2, half, CAP, part), jnp.float32),
                pltpu.VMEM((groups, CAP, part), jnp.float32),
                pltpu.SemaphoreType.DMA((7,)),
                pltpu.SemaphoreType.DMA((3,)),
                pltpu.SemaphoreType.DMA((3,)),
                pltpu.SemaphoreType.DMA,
                pltpu.SemaphoreType.DMA((len(CHUNKS),)),
                pltpu.SemaphoreType.DMA((planes - 1, pieces)),
                pltpu.SemaphoreType.DMA((planes - 1, pieces)),
                pltpu.SemaphoreType.DMA((planes - 1,)),
                pltpu.SemaphoreType.DMA((planes - 1,)),
                pltpu.SemaphoreType.DMA,
                pltpu.SemaphoreType.DMA,
            ],
            compiler_params=pltpu.CompilerParams(collective_id=0, has_side_effects=True,
                                                 vmem_limit_bytes=67043328 - 16384),
            name="experts",
        )(tokens, norm_gain.reshape(1, width), routing.T, route_weight.T,
          jnp.swapaxes(w_gate, 1, 2), jnp.swapaxes(w_up, 1, 2), w_down)

    in_specs = (
        P("ep", None),
        P(),
        P("ep", None),
        P("ep", None),
        P("ep", None, "tp"),
        P("ep", None, "tp"),
        P("ep", "tp", None),
    )
    return jax.shard_map(local, mesh=mesh, in_specs=in_specs, out_specs=P("ep", "tp"), check_vma=False)
```

```python
import functools

import jax
import jax.numpy as jnp
from jax import lax
from jax.experimental import pallas as pl
from jax.experimental.pallas import tpu as pltpu
from jax.sharding import PartitionSpec as P

CAP = 8
XS = 4
CHUNKS = ((0, 16),)
PIECES = (((0, 4, 1), (0, 4, 0), (4, 16, 1), (4, 16, 0)),)
STEPS = ('c0', 'r0', 'r1', 'r2', 'r3')
STEPS_16 = 32767.0
LEAST = 2e-34
MESH = pl.DeviceIdType.MESH

norm_eps = 1e-06


def kernel(groups, shares, tokens_hbm, gain_hbm, routing_hbm, route_weight_hbm, gate_hbm, up_hbm, down_hbm, mixed,
           tokens, gain, routing, route_weight, gate, up, down, gate_across, up_across,
           outgoing, incoming, partial, reduced, peak, their_peak, back, arrived,
           load_sem, swap_send, swap_recv, out_sem, in_sem, part_send, part_recv, peak_send, peak_recv, back_send, back_recv):
    ep, tp = lax.axis_index("ep"), lax.axis_index("tp")
    width = tokens.shape[1]
    part = mixed.shape[1]
    half = groups // 2
    rows = half * CAP
    planes = shares // 2
    share = gate_hbm.shape[1]
    y, core = tp // 2, lax.rem(tp, 2)
    zs = groups // XS
    z, x = ep // XS, lax.rem(ep, XS)
    lower = 1 - z // (zs // 2)
    theirs, goal = half * (1 - core), half * core

    def near(q, dx):
        return XS * lax.rem(z + q, zs // 2) + lax.rem(x + dx, XS)

    rounds = [(q, dx) for q in (0, 3, 1, 2) for dx in (2, 3, 1, 0)]

    chunk_of = {p: k for k, (first, upto) in enumerate(CHUNKS) for p in range(first, upto)}
    tile = 2 * part

    barrier = pltpu.get_barrier_semaphore()
    for q, dx in rounds:
        pl.semaphore_signal(barrier, inc=1, device_id=(theirs + near(q, dx), 2 * y + 1 - lower), device_id_type=MESH)
    for d in range(1, planes):
        pl.semaphore_signal(barrier, inc=1, device_id=(ep, 2 * lax.rem(y + d, planes) + core), device_id_type=MESH)
    pl.semaphore_signal(barrier, inc=1, device_id=(ep, 2 * y + 1 - core), device_id_type=MESH)

    pairs = ((tokens_hbm, tokens), (gain_hbm, gain), (routing_hbm, routing), (route_weight_hbm, route_weight),
             (gate_hbm.at[0], gate.at[0:share]), (up_hbm.at[0], up.at[0:share]), (down_hbm.at[0], down.at[0:share]))
    loads = [pltpu.make_async_copy(source, target, load_sem.at[i]) for i, (source, target) in enumerate(pairs)]
    for i in (2, 3, 0, 1, 4, 5, 6):
        loads[i].start()

    count = tokens.shape[0]
    earlier = lax.broadcasted_iota(jnp.int32, (count, count), 0) < lax.broadcasted_iota(jnp.int32, (count, count), 1)
    earlier = jnp.where(earlier, 1.0, 0.0).astype(jnp.bfloat16)

    def slots_of(lines, expert_of):
        line = lax.broadcasted_iota(jnp.int32, (lines, count), 0)
        expert = expert_of(line // CAP)
        member = jnp.zeros((lines, count), jnp.float32)
        weight = jnp.zeros((lines, count), jnp.float32)
        for k in range(routing.shape[0]):
            named = routing[k:k + 1, :] == expert
            member = jnp.where(named, 1.0, member)
            weight = jnp.where(named, route_weight[k:k + 1, :], weight)
        before = jnp.dot(member.astype(jnp.bfloat16), earlier, preferred_element_type=jnp.float32)
        placed = jnp.where(before == lax.rem(line, CAP).astype(jnp.float32), member, 0.0)
        return placed, weight

    loads[2].wait()
    loads[3].wait()
    placed, _ = slots_of(rows, lambda p: goal + p)
    loads[0].wait()
    loads[1].wait()
    values = tokens[...].astype(jnp.float32)
    scale = lax.rsqrt(jnp.mean(values * values, axis=-1, keepdims=True) + norm_eps)
    normed = (values * scale * gain[...]).astype(jnp.bfloat16)
    sent = jnp.dot(placed.astype(jnp.bfloat16), normed, preferred_element_type=jnp.float32)
    outgoing[...] = sent.reshape(half, CAP, width).astype(jnp.bfloat16)

    pl.semaphore_wait(barrier, half + planes)

    for q, dx in rounds:
        p = near(q, dx)
        pltpu.make_async_remote_copy(
            src_ref=outgoing.at[p], dst_ref=incoming.at[lax.rem(ep, half)], send_sem=out_sem, recv_sem=in_sem.at[0],
            device_id=(goal + p, 2 * y + lower), device_id_type=MESH).start()

    swaps = [pltpu.make_async_remote_copy(
        src_ref=ref.at[0:share], dst_ref=ref.at[share:2 * share], send_sem=swap_send.at[i], recv_sem=swap_recv.at[i],
        device_id=(ep, 2 * y + 1 - core), device_id_type=MESH) for i, ref in enumerate((gate, up, down))]
    for i in (4, 5, 6):
        loads[i].wait()
    for swap in swaps:
        swap.start()

    picked, weight = slots_of(groups * CAP, lambda q: q)
    weight = jnp.transpose(weight * picked)

    for swap in swaps:
        swap.wait_recv()
    gate_across[...] = jnp.transpose(gate[...])
    up_across[...] = jnp.transpose(up[...])

    def wait_for(ref, sem, most):
        less, full = ref.at[pl.ds(0, most - 1)], ref.at[pl.ds(0, most)]
        pl.when(core == lower)(lambda: pltpu.make_async_copy(less, less, sem).wait())
        pl.when(core != lower)(lambda: pltpu.make_async_copy(full, full, sem).wait())

    def wait_all(ref, sem):
        pltpu.make_async_copy(ref, ref, sem).wait()

    pieces = [piece for some in PIECES for piece in some]
    totals = {}
    others = range(planes - 1)

    def plane(d):
        return d + (d + planes - y) // planes

    def seen_at(d):
        return y - (y + planes - 1 - plane(d)) // planes

    def columns(to):
        return pl.ds(pl.multiple_of(to * tile, tile), tile)

    def give(d, piece):
        some, side, k = pl.ds(piece[0] * CAP, (piece[1] - piece[0]) * CAP), piece[2], pieces.index(piece)
        return pltpu.make_async_remote_copy(
            src_ref=partial.at[d, side, some], dst_ref=reduced.at[seen_at(d), side, some],
            send_sem=part_send.at[d, k], recv_sem=part_recv.at[seen_at(d), k],
            device_id=(ep, 2 * plane(d) + core), device_id_type=MESH)

    def received(d, piece):
        some, side, k = pl.ds(piece[0] * CAP, (piece[1] - piece[0]) * CAP), piece[2], pieces.index(piece)
        return pltpu.make_async_copy(reduced.at[d, side, some], reduced.at[d, side, some], part_recv.at[d, k])

    def give_peak(d):
        return pltpu.make_async_remote_copy(
            src_ref=peak.at[d], dst_ref=their_peak.at[seen_at(d)], send_sem=peak_send.at[d],
            recv_sem=peak_recv.at[seen_at(d)], device_id=(ep, 2 * plane(d) + core), device_id_type=MESH)

    def multiply(k):
        first, upto = CHUNKS[k]
        wait_all(incoming.at[pl.ds(first, upto - first)], in_sem.at[k])
        a = incoming[first:upto].astype(jnp.float32).reshape((upto - first) * CAP, width).astype(jnp.bfloat16)
        gate_act = jnp.dot(a, gate_across[...], preferred_element_type=jnp.float32)
        up_act = jnp.dot(a, up_across[...], preferred_element_type=jnp.float32)
        hidden = (gate_act / (1.0 + jnp.exp(-gate_act)) * up_act).astype(jnp.bfloat16)
        for d in others:
            block = jnp.dot(hidden, down[:, columns(plane(d))], preferred_element_type=jnp.float32)
            sides = [block[:, side * part:(side + 1) * part].reshape(upto - first, CAP, part) for side in range(2)]
            most = jnp.maximum(jnp.max(jnp.maximum(jnp.abs(sides[0]), jnp.abs(sides[1])), axis=0), LEAST)
            peak[d] = most
            give_peak(d).start()
            for side in range(2):
                coded = jnp.round(sides[side] * (STEPS_16 / most)).reshape((upto - first) * CAP, part)
                partial[d, side, first * CAP:upto * CAP] = (
                    coded.astype(jnp.int32).astype(jnp.int16))
            give(d, PIECES[k][0]).start()
        for piece in PIECES[k][1:]:
            for d in others:
                give(d, piece).start()
        mine = jnp.dot(hidden, down[:, columns(y)], preferred_element_type=jnp.float32)
        for piece in PIECES[k]:
            totals[piece] = mine[(piece[0] - first) * CAP:(piece[1] - first) * CAP]

    def give_back(k):
        piece = pieces[k]
        first, upto, side = piece
        for d in others:
            if k == 0:
                pltpu.make_async_copy(their_peak.at[d], their_peak.at[d], peak_recv.at[d]).wait()
            received(d, piece).wait()
        total = totals[piece][:, side * part:(side + 1) * part].reshape(upto - first, CAP, part)
        for d in others:
            coded = reduced[d, side, first * CAP:upto * CAP].astype(jnp.int32).astype(jnp.float32)
            total = total + coded.reshape(upto - first, CAP, part) * (their_peak[d] * (1.0 / STEPS_16))
        back[side, first:upto] = total
        for start in range(first, upto, XS):
            for dx in (2, 3, 1, 0):
                p = start + lax.rem(x + dx, XS)

                def send(p=p):
                    pltpu.make_async_remote_copy(
                        src_ref=back.at[side, p], dst_ref=arrived.at[ep], send_sem=back_send, recv_sem=back_recv,
                        device_id=(theirs + p, 2 * y + side), device_id_type=MESH).start()

                def hold(p=p):
                    arrived[ep] = back[side, p]
                if dx == 0:
                    here = jnp.logical_and(theirs + p == ep, core == side)
                    pl.when(here)(hold)
                    pl.when(jnp.logical_not(here))(send)
                else:
                    send()

    for step in STEPS:
        (multiply if step[0] == "c" else give_back)(int(step[1:]))

    wait_for(arrived, back_recv, groups)
    out = jnp.dot(weight, arrived[...].reshape(groups * CAP, part), precision=lax.Precision.HIGHEST,
                  preferred_element_type=jnp.float32)
    mixed[...] = out.astype(mixed.dtype)
    wait_all(outgoing, out_sem)
    for swap in swaps:
        swap.wait_send()
    for d in others:
        give_peak(d).wait_send()
    for piece in pieces:
        for d in others:
            give(d, piece).wait_send()
    wait_for(arrived, back_send, groups)


def solution(mesh):
    groups, shares = mesh.shape["ep"], mesh.shape["tp"]

    def local(tokens, norm_gain, routing, route_weight, w_gate, w_up, w_down):
        count, width = tokens.shape
        part = width // shares
        half, planes = groups // 2, shares // 2
        rows = half * CAP
        share = w_down.shape[1]
        pieces = sum(map(len, PIECES))
        vmem = pl.BlockSpec(memory_space=pltpu.VMEM)
        hbm = pl.BlockSpec(memory_space=pltpu.HBM)
        return pl.pallas_call(
            functools.partial(kernel, groups, shares),
            out_shape=pltpu.VMEM((count, part), jnp.bfloat16),
            in_specs=[hbm] * 7,
            out_specs=vmem,
            scratch_shapes=[
                pltpu.VMEM((count, width), tokens.dtype),
                pltpu.VMEM((1, width), norm_gain.dtype),
                pltpu.VMEM(routing.shape[::-1], routing.dtype),
                pltpu.VMEM(route_weight.shape[::-1], route_weight.dtype),
                pltpu.VMEM((2 * share, width), jnp.bfloat16),
                pltpu.VMEM((2 * share, width), jnp.bfloat16),
                pltpu.VMEM((2 * share, width), jnp.bfloat16),
                pltpu.VMEM((width, 2 * share), jnp.bfloat16),
                pltpu.VMEM((width, 2 * share), jnp.bfloat16),
                pltpu.VMEM((half, CAP, width), jnp.bfloat16),
                pltpu.VMEM((half, CAP, width), jnp.bfloat16),
                pltpu.VMEM((planes - 1, 2, rows, part), jnp.int16),
                pltpu.VMEM((planes - 1, 2, rows, part), jnp.int16),
                pltpu.VMEM((planes - 1, CAP, part), jnp.float32),
                pltpu.VMEM((planes - 1, CAP, part), jnp.float32),
                pltpu.VMEM((2, half, CAP, part), jnp.float32),
                pltpu.VMEM((groups, CAP, part), jnp.float32),
                pltpu.SemaphoreType.DMA((7,)),
                pltpu.SemaphoreType.DMA((3,)),
                pltpu.SemaphoreType.DMA((3,)),
                pltpu.SemaphoreType.DMA,
                pltpu.SemaphoreType.DMA((len(CHUNKS),)),
                pltpu.SemaphoreType.DMA((planes - 1, pieces)),
                pltpu.SemaphoreType.DMA((planes - 1, pieces)),
                pltpu.SemaphoreType.DMA((planes - 1,)),
                pltpu.SemaphoreType.DMA((planes - 1,)),
                pltpu.SemaphoreType.DMA,
                pltpu.SemaphoreType.DMA,
            ],
            compiler_params=pltpu.CompilerParams(collective_id=0, has_side_effects=True,
                                                 vmem_limit_bytes=67043328 - 16384),
            name="experts",
        )(tokens, norm_gain.reshape(1, width), routing.T, route_weight.T,
          jnp.swapaxes(w_gate, 1, 2), jnp.swapaxes(w_up, 1, 2), w_down)

    in_specs = (
        P("ep", None),
        P(),
        P("ep", None),
        P("ep", None),
        P("ep", None, "tp"),
        P("ep", None, "tp"),
        P("ep", "tp", None),
    )
    return jax.shard_map(local, mesh=mesh, in_specs=in_specs, out_specs=P("ep", "tp"), check_vma=False)
```

```python
import functools

import jax
import jax.numpy as jnp
from jax import lax
from jax.experimental import pallas as pl
from jax.experimental.pallas import tpu as pltpu
from jax.sharding import PartitionSpec as P

CAP = 8
XS = 4
CHUNKS = ((0, 16),)
PIECES = (((0, 4, 1), (0, 8, 0), (4, 12, 1), (8, 16, 0), (12, 16, 1)),)
STEPS = ('c0', 'r0', 'r1', 'r2', 'r3', 'r4')
STEPS_16 = 32767.0
LEAST = 2e-34
MESH = pl.DeviceIdType.MESH

norm_eps = 1e-06


def kernel(groups, shares, tokens_hbm, gain_hbm, routing_hbm, route_weight_hbm, gate_hbm, up_hbm, down_hbm, mixed,
           tokens, gain, routing, route_weight, gate, up, down, gate_across, up_across,
           outgoing, incoming, partial, reduced, peak, their_peak, back, arrived,
           load_sem, swap_send, swap_recv, out_sem, in_sem, part_send, part_recv, peak_send, peak_recv, back_send, back_recv):
    ep, tp = lax.axis_index("ep"), lax.axis_index("tp")
    width = tokens.shape[1]
    part = mixed.shape[1]
    half = groups // 2
    rows = half * CAP
    planes = shares // 2
    share = gate_hbm.shape[1]
    y, core = tp // 2, lax.rem(tp, 2)
    zs = groups // XS
    z, x = ep // XS, lax.rem(ep, XS)
    lower = 1 - z // (zs // 2)
    theirs, goal = half * (1 - core), half * core

    def near(q, dx):
        return XS * lax.rem(z + q, zs // 2) + lax.rem(x + dx, XS)

    rounds = [(q, dx) for dx in (2, 3, 1, 0) for q in (0, 3, 1, 2)]

    chunk_of = {p: k for k, (first, upto) in enumerate(CHUNKS) for p in range(first, upto)}
    tile = 2 * part

    barrier = pltpu.get_barrier_semaphore()
    for q, dx in rounds:
        pl.semaphore_signal(barrier, inc=1, device_id=(theirs + near(q, dx), 2 * y + 1 - lower), device_id_type=MESH)
    for d in range(1, planes):
        pl.semaphore_signal(barrier, inc=1, device_id=(ep, 2 * lax.rem(y + d, planes) + core), device_id_type=MESH)
    pl.semaphore_signal(barrier, inc=1, device_id=(ep, 2 * y + 1 - core), device_id_type=MESH)

    pairs = ((tokens_hbm, tokens), (gain_hbm, gain), (routing_hbm, routing), (route_weight_hbm, route_weight),
             (gate_hbm.at[0], gate.at[0:share]), (up_hbm.at[0], up.at[0:share]), (down_hbm.at[0], down.at[0:share]))
    loads = [pltpu.make_async_copy(source, target, load_sem.at[i]) for i, (source, target) in enumerate(pairs)]
    for i in (2, 3, 0, 1, 4, 5, 6):
        loads[i].start()

    count = tokens.shape[0]
    earlier = lax.broadcasted_iota(jnp.int32, (count, count), 0) < lax.broadcasted_iota(jnp.int32, (count, count), 1)
    earlier = jnp.where(earlier, 1.0, 0.0).astype(jnp.bfloat16)

    def slots_of(lines, expert_of):
        line = lax.broadcasted_iota(jnp.int32, (lines, count), 0)
        expert = expert_of(line // CAP)
        member = jnp.zeros((lines, count), jnp.float32)
        weight = jnp.zeros((lines, count), jnp.float32)
        for k in range(routing.shape[0]):
            named = routing[k:k + 1, :] == expert
            member = jnp.where(named, 1.0, member)
            weight = jnp.where(named, route_weight[k:k + 1, :], weight)
        before = jnp.dot(member.astype(jnp.bfloat16), earlier, preferred_element_type=jnp.float32)
        placed = jnp.where(before == lax.rem(line, CAP).astype(jnp.float32), member, 0.0)
        return placed, weight

    loads[2].wait()
    loads[3].wait()
    placed, _ = slots_of(rows, lambda p: goal + p)
    loads[0].wait()
    loads[1].wait()
    values = tokens[...].astype(jnp.float32)
    scale = lax.rsqrt(jnp.mean(values * values, axis=-1, keepdims=True) + norm_eps)
    normed = (values * scale * gain[...]).astype(jnp.bfloat16)
    sent = jnp.dot(placed.astype(jnp.bfloat16), normed, preferred_element_type=jnp.float32)
    outgoing[...] = sent.reshape(half, CAP, width).astype(jnp.bfloat16)

    pl.semaphore_wait(barrier, half + planes)

    def dispatch():
        for q, dx in rounds:
            p = near(q, dx)
            pltpu.make_async_remote_copy(
                src_ref=outgoing.at[p], dst_ref=incoming.at[lax.rem(ep, half)], send_sem=out_sem, recv_sem=in_sem.at[0],
                device_id=(goal + p, 2 * y + lower), device_id_type=MESH).start()

    pl.when(lower + 1 - core > 0)(dispatch)

    swaps = [pltpu.make_async_remote_copy(
        src_ref=ref.at[0:share], dst_ref=ref.at[share:2 * share], send_sem=swap_send.at[i], recv_sem=swap_recv.at[i],
        device_id=(ep, 2 * y + 1 - core), device_id_type=MESH) for i, ref in enumerate((gate, up, down))]
    for i in (4, 5, 6):
        loads[i].wait()
    for swap in swaps:
        swap.start()

    picked, weight = slots_of(groups * CAP, lambda q: q)
    weight = jnp.transpose(weight * picked)

    for swap in swaps:
        swap.wait_recv()
    pl.when(lower + 1 - core == 0)(dispatch)
    gate_across[...] = jnp.transpose(gate[...])
    up_across[...] = jnp.transpose(up[...])

    def wait_for(ref, sem, most):
        less, full = ref.at[pl.ds(0, most - 1)], ref.at[pl.ds(0, most)]
        pl.when(core == lower)(lambda: pltpu.make_async_copy(less, less, sem).wait())
        pl.when(core != lower)(lambda: pltpu.make_async_copy(full, full, sem).wait())

    def wait_all(ref, sem):
        pltpu.make_async_copy(ref, ref, sem).wait()

    pieces = [piece for some in PIECES for piece in some]
    totals = {}
    others = range(planes - 1)

    def plane(d):
        return d + (d + planes - y) // planes

    def seen_at(d):
        return y - (y + planes - 1 - plane(d)) // planes

    def columns(to):
        return pl.ds(pl.multiple_of(to * tile, tile), tile)

    def give(d, piece):
        some, side, k = pl.ds(piece[0] * CAP, (piece[1] - piece[0]) * CAP), piece[2], pieces.index(piece)
        return pltpu.make_async_remote_copy(
            src_ref=partial.at[d, side, some], dst_ref=reduced.at[seen_at(d), side, some],
            send_sem=part_send.at[d, k], recv_sem=part_recv.at[seen_at(d), k],
            device_id=(ep, 2 * plane(d) + core), device_id_type=MESH)

    def received(d, piece):
        some, side, k = pl.ds(piece[0] * CAP, (piece[1] - piece[0]) * CAP), piece[2], pieces.index(piece)
        return pltpu.make_async_copy(reduced.at[d, side, some], reduced.at[d, side, some], part_recv.at[d, k])

    def give_peak(d):
        return pltpu.make_async_remote_copy(
            src_ref=peak.at[d], dst_ref=their_peak.at[seen_at(d)], send_sem=peak_send.at[d],
            recv_sem=peak_recv.at[seen_at(d)], device_id=(ep, 2 * plane(d) + core), device_id_type=MESH)

    def multiply(k):
        first, upto = CHUNKS[k]
        wait_all(incoming.at[pl.ds(first, upto - first)], in_sem.at[k])
        a = incoming[first:upto].astype(jnp.float32).reshape((upto - first) * CAP, width).astype(jnp.bfloat16)
        gate_act = jnp.dot(a, gate_across[...], preferred_element_type=jnp.float32)
        up_act = jnp.dot(a, up_across[...], preferred_element_type=jnp.float32)
        hidden = (gate_act / (1.0 + jnp.exp(-gate_act)) * up_act).astype(jnp.bfloat16)
        for d in others:
            block = jnp.dot(hidden, down[:, columns(plane(d))], preferred_element_type=jnp.float32)
            sides = [block[:, side * part:(side + 1) * part].reshape(upto - first, CAP, part) for side in range(2)]
            most = jnp.maximum(jnp.max(jnp.maximum(jnp.abs(sides[0]), jnp.abs(sides[1])), axis=0), LEAST)
            peak[d] = most
            give_peak(d).start()
            for side in range(2):
                coded = jnp.round(sides[side] * (STEPS_16 / most)).reshape((upto - first) * CAP, part)
                partial[d, side, first * CAP:upto * CAP] = (
                    coded.astype(jnp.int32).astype(jnp.int16))
            give(d, PIECES[k][0]).start()
        for piece in PIECES[k][1:]:
            for d in others:
                give(d, piece).start()
        mine = jnp.dot(hidden, down[:, columns(y)], preferred_element_type=jnp.float32)
        for piece in PIECES[k]:
            totals[piece] = mine[(piece[0] - first) * CAP:(piece[1] - first) * CAP]

    def give_back(k):
        piece = pieces[k]
        first, upto, side = piece
        for d in others:
            if k == 0:
                pltpu.make_async_copy(their_peak.at[d], their_peak.at[d], peak_recv.at[d]).wait()
            received(d, piece).wait()
        total = totals[piece][:, side * part:(side + 1) * part].reshape(upto - first, CAP, part)
        for d in others:
            coded = reduced[d, side, first * CAP:upto * CAP].astype(jnp.int32).astype(jnp.float32)
            total = total + coded.reshape(upto - first, CAP, part) * (their_peak[d] * (1.0 / STEPS_16))
        back[side, first:upto] = total
        for start in range(first, upto, XS):
            for dx in (2, 3, 1, 0):
                p = start + lax.rem(x + dx, XS)

                def send(p=p):
                    pltpu.make_async_remote_copy(
                        src_ref=back.at[side, p], dst_ref=arrived.at[ep], send_sem=back_send, recv_sem=back_recv,
                        device_id=(theirs + p, 2 * y + side), device_id_type=MESH).start()

                def hold(p=p):
                    arrived[ep] = back[side, p]
                if dx == 0:
                    here = jnp.logical_and(theirs + p == ep, core == side)
                    pl.when(here)(hold)
                    pl.when(jnp.logical_not(here))(send)
                else:
                    send()

    for step in STEPS:
        (multiply if step[0] == "c" else give_back)(int(step[1:]))

    wait_for(arrived, back_recv, groups)
    out = jnp.dot(weight, arrived[...].reshape(groups * CAP, part), precision=lax.Precision.HIGHEST,
                  preferred_element_type=jnp.float32)
    mixed[...] = out.astype(mixed.dtype)
    wait_all(outgoing, out_sem)
    for swap in swaps:
        swap.wait_send()
    for d in others:
        give_peak(d).wait_send()
    for piece in pieces:
        for d in others:
            give(d, piece).wait_send()
    wait_for(arrived, back_send, groups)


def solution(mesh):
    groups, shares = mesh.shape["ep"], mesh.shape["tp"]

    def local(tokens, norm_gain, routing, route_weight, w_gate, w_up, w_down):
        count, width = tokens.shape
        part = width // shares
        half, planes = groups // 2, shares // 2
        rows = half * CAP
        share = w_down.shape[1]
        pieces = sum(map(len, PIECES))
        vmem = pl.BlockSpec(memory_space=pltpu.VMEM)
        hbm = pl.BlockSpec(memory_space=pltpu.HBM)
        return pl.pallas_call(
            functools.partial(kernel, groups, shares),
            out_shape=pltpu.VMEM((count, part), jnp.bfloat16),
            in_specs=[hbm] * 7,
            out_specs=vmem,
            scratch_shapes=[
                pltpu.VMEM((count, width), tokens.dtype),
                pltpu.VMEM((1, width), norm_gain.dtype),
                pltpu.VMEM(routing.shape[::-1], routing.dtype),
                pltpu.VMEM(route_weight.shape[::-1], route_weight.dtype),
                pltpu.VMEM((2 * share, width), jnp.bfloat16),
                pltpu.VMEM((2 * share, width), jnp.bfloat16),
                pltpu.VMEM((2 * share, width), jnp.bfloat16),
                pltpu.VMEM((width, 2 * share), jnp.bfloat16),
                pltpu.VMEM((width, 2 * share), jnp.bfloat16),
                pltpu.VMEM((half, CAP, width), jnp.bfloat16),
                pltpu.VMEM((half, CAP, width), jnp.bfloat16),
                pltpu.VMEM((planes - 1, 2, rows, part), jnp.int16),
                pltpu.VMEM((planes - 1, 2, rows, part), jnp.int16),
                pltpu.VMEM((planes - 1, CAP, part), jnp.float32),
                pltpu.VMEM((planes - 1, CAP, part), jnp.float32),
                pltpu.VMEM((2, half, CAP, part), jnp.float32),
                pltpu.VMEM((groups, CAP, part), jnp.float32),
                pltpu.SemaphoreType.DMA((7,)),
                pltpu.SemaphoreType.DMA((3,)),
                pltpu.SemaphoreType.DMA((3,)),
                pltpu.SemaphoreType.DMA,
                pltpu.SemaphoreType.DMA((len(CHUNKS),)),
                pltpu.SemaphoreType.DMA((planes - 1, pieces)),
                pltpu.SemaphoreType.DMA((planes - 1, pieces)),
                pltpu.SemaphoreType.DMA((planes - 1,)),
                pltpu.SemaphoreType.DMA((planes - 1,)),
                pltpu.SemaphoreType.DMA,
                pltpu.SemaphoreType.DMA,
            ],
            compiler_params=pltpu.CompilerParams(collective_id=0, has_side_effects=True,
                                                 vmem_limit_bytes=67043328 - 16384),
            name="experts",
        )(tokens, norm_gain.reshape(1, width), routing.T, route_weight.T,
          jnp.swapaxes(w_gate, 1, 2), jnp.swapaxes(w_up, 1, 2), w_down)

    in_specs = (
        P("ep", None),
        P(),
        P("ep", None),
        P("ep", None),
        P("ep", None, "tp"),
        P("ep", None, "tp"),
        P("ep", "tp", None),
    )
    return jax.shard_map(local, mesh=mesh, in_specs=in_specs, out_specs=P("ep", "tp"), check_vma=False)
```

```python
import functools

import jax
import jax.numpy as jnp
from jax import lax
from jax.experimental import pallas as pl
from jax.experimental.pallas import tpu as pltpu
from jax.sharding import PartitionSpec as P

CAP = 8
XS = 4
CHUNKS = ((0, 16),)
PIECES = (((0, 8, 1), (8, 12, 1), (0, 8, 0), (12, 16, 1), (8, 12, 0), (12, 16, 0)),)
STEPS = ('c0', 'r0', 'r1', 'r2', 'r3', 'r4', 'r5')
MESH = pl.DeviceIdType.MESH

norm_eps = 1e-06


def kernel(groups, shares, tokens_hbm, gain_hbm, routing_hbm, route_weight_hbm, gate_hbm, up_hbm, down_hbm, mixed,
           tokens, gain, routing, route_weight, gate, up, down, gate_across, up_across,
           outgoing, incoming, partial, reduced, back, arrived,
           load_sem, swap_send, swap_recv, out_sem, in_sem, part_send, part_recv, back_send, back_recv):
    ep, tp = lax.axis_index("ep"), lax.axis_index("tp")
    width = tokens.shape[1]
    part = mixed.shape[1]
    half = groups // 2
    rows = half * CAP
    planes = shares // 2
    share = gate_hbm.shape[1]
    y, core = tp // 2, lax.rem(tp, 2)
    zs = groups // XS
    z, x = ep // XS, lax.rem(ep, XS)
    lower = 1 - z // (zs // 2)
    theirs, goal = half * (1 - core), half * core

    def near(q, dx):
        return XS * lax.rem(z + q, zs // 2) + lax.rem(x + dx, XS)

    rounds = [(q, dx) for dx in (2, 3, 1, 0) for q in (0, 3, 1, 2)]

    chunk_of = {p: k for k, (first, upto) in enumerate(CHUNKS) for p in range(first, upto)}
    tile = 2 * part

    barrier = pltpu.get_barrier_semaphore()
    for p in range(half):
        pl.semaphore_signal(barrier, inc=1, device_id=(theirs + p, 2 * y + 1 - lower), device_id_type=MESH)
    for d in range(1, planes):
        pl.semaphore_signal(barrier, inc=1, device_id=(ep, 2 * lax.rem(y + d, planes) + core), device_id_type=MESH)
    pl.semaphore_signal(barrier, inc=1, device_id=(ep, 2 * y + 1 - core), device_id_type=MESH)

    pairs = ((tokens_hbm, tokens), (gain_hbm, gain), (routing_hbm, routing), (route_weight_hbm, route_weight),
             (gate_hbm.at[0], gate.at[0:share]), (up_hbm.at[0], up.at[0:share]), (down_hbm.at[0], down.at[0:share]))
    loads = [pltpu.make_async_copy(source, target, load_sem.at[i]) for i, (source, target) in enumerate(pairs)]
    for i in (2, 3, 0, 1, 4, 5, 6):
        loads[i].start()

    count = tokens.shape[0]
    earlier = lax.broadcasted_iota(jnp.int32, (count, count), 0) < lax.broadcasted_iota(jnp.int32, (count, count), 1)
    earlier = jnp.where(earlier, 1.0, 0.0).astype(jnp.bfloat16)

    def slots_of(lines, expert_of):
        line = lax.broadcasted_iota(jnp.int32, (lines, count), 0)
        expert = expert_of(line // CAP)
        member = jnp.zeros((lines, count), jnp.float32)
        weight = jnp.zeros((lines, count), jnp.float32)
        for k in range(routing.shape[0]):
            named = routing[k:k + 1, :] == expert
            member = jnp.where(named, 1.0, member)
            weight = jnp.where(named, route_weight[k:k + 1, :], weight)
        before = jnp.dot(member.astype(jnp.bfloat16), earlier, preferred_element_type=jnp.float32)
        placed = jnp.where(before == lax.rem(line, CAP).astype(jnp.float32), member, 0.0)
        return placed, weight

    loads[2].wait()
    loads[3].wait()
    placed, _ = slots_of(rows, lambda p: goal + p)
    loads[0].wait()
    loads[1].wait()
    values = tokens[...].astype(jnp.float32)
    scale = lax.rsqrt(jnp.mean(values * values, axis=-1, keepdims=True) + norm_eps)
    normed = (values * scale * gain[...]).astype(jnp.bfloat16)
    sent = jnp.dot(placed.astype(jnp.bfloat16), normed, preferred_element_type=jnp.float32)
    outgoing[...] = sent.reshape(half, CAP, width).astype(jnp.bfloat16)

    pl.semaphore_wait(barrier, half + planes)

    def dispatch():
        for q, dx in rounds:
            p = near(q, dx)
            pltpu.make_async_remote_copy(
                src_ref=outgoing.at[p], dst_ref=incoming.at[lax.rem(ep, half)], send_sem=out_sem, recv_sem=in_sem.at[0],
                device_id=(goal + p, 2 * y + lower), device_id_type=MESH).start()

    pl.when(lower + 1 - core > 0)(dispatch)

    swaps = [pltpu.make_async_remote_copy(
        src_ref=ref.at[0:share], dst_ref=ref.at[share:2 * share], send_sem=swap_send.at[i], recv_sem=swap_recv.at[i],
        device_id=(ep, 2 * y + 1 - core), device_id_type=MESH) for i, ref in enumerate((gate, up, down))]
    for i in (4, 5, 6):
        loads[i].wait()
    for swap in swaps:
        swap.start()

    picked, weight = slots_of(groups * CAP, lambda q: q)
    weight = jnp.transpose(weight * picked)

    for swap in swaps:
        swap.wait_recv()
    pl.when(lower + 1 - core == 0)(dispatch)
    gate_across[...] = jnp.transpose(gate[...])
    up_across[...] = jnp.transpose(up[...])

    def wait_for(ref, sem, most):
        less, full = ref.at[pl.ds(0, most - 1)], ref.at[pl.ds(0, most)]
        pl.when(core == lower)(lambda: pltpu.make_async_copy(less, less, sem).wait())
        pl.when(core != lower)(lambda: pltpu.make_async_copy(full, full, sem).wait())

    def wait_all(ref, sem):
        pltpu.make_async_copy(ref, ref, sem).wait()

    pieces = [piece for some in PIECES for piece in some]
    totals = {}
    others = range(planes - 1)

    def plane(d):
        return d + (d + planes - y) // planes

    def seen_at(d):
        return y - (y + planes - 1 - plane(d)) // planes

    def columns(to):
        return pl.ds(pl.multiple_of(to * tile, tile), tile)

    def give(d, piece):
        some, side, k = pl.ds(piece[0] * CAP, (piece[1] - piece[0]) * CAP), piece[2], pieces.index(piece)
        return pltpu.make_async_remote_copy(
            src_ref=partial.at[d, side, some], dst_ref=reduced.at[seen_at(d), side, some],
            send_sem=part_send.at[d, k], recv_sem=part_recv.at[seen_at(d), k],
            device_id=(ep, 2 * plane(d) + core), device_id_type=MESH)

    def received(d, piece):
        some, side, k = pl.ds(piece[0] * CAP, (piece[1] - piece[0]) * CAP), piece[2], pieces.index(piece)
        return pltpu.make_async_copy(reduced.at[d, side, some], reduced.at[d, side, some], part_recv.at[d, k])

    def multiply(k):
        first, upto = CHUNKS[k]
        wait_all(incoming.at[pl.ds(first, upto - first)], in_sem.at[k])
        a = incoming[first:upto].astype(jnp.float32).reshape((upto - first) * CAP, width).astype(jnp.bfloat16)
        gate_act = jnp.dot(a, gate_across[...], preferred_element_type=jnp.float32)
        up_act = jnp.dot(a, up_across[...], preferred_element_type=jnp.float32)
        hidden = (gate_act / (1.0 + jnp.exp(-gate_act)) * up_act).astype(jnp.bfloat16)
        for d in others:
            block = jnp.dot(hidden, down[:, columns(plane(d))], preferred_element_type=jnp.float32)
            for side in range(2):
                partial[d, side, first * CAP:upto * CAP] = block[:, side * part:(side + 1) * part]
            give(d, PIECES[k][0]).start()
        for piece in PIECES[k][1:]:
            for d in others:
                give(d, piece).start()
        mine = jnp.dot(hidden, down[:, columns(y)], preferred_element_type=jnp.float32)
        for piece in PIECES[k]:
            totals[piece] = mine[(piece[0] - first) * CAP:(piece[1] - first) * CAP]

    def give_back(k):
        piece = pieces[k]
        first, upto, side = piece
        for d in others:
            received(d, piece).wait()
        total = totals[piece][:, side * part:(side + 1) * part].reshape(upto - first, CAP, part)
        for d in others:
            total = total + reduced[d, side, first * CAP:upto * CAP].reshape(upto - first, CAP, part)
        back[side, first:upto] = total
        for start in range(first, upto, XS):
            for dx in (2, 3, 1, 0):
                p = start + lax.rem(x + dx, XS)

                def send(p=p):
                    pltpu.make_async_remote_copy(
                        src_ref=back.at[side, p], dst_ref=arrived.at[ep], send_sem=back_send, recv_sem=back_recv,
                        device_id=(theirs + p, 2 * y + side), device_id_type=MESH).start()

                def hold(p=p):
                    arrived[ep] = back[side, p]
                if dx == 0:
                    here = jnp.logical_and(theirs + p == ep, core == side)
                    pl.when(here)(hold)
                    pl.when(jnp.logical_not(here))(send)
                else:
                    send()

    for step in STEPS:
        (multiply if step[0] == "c" else give_back)(int(step[1:]))

    wait_for(arrived, back_recv, groups)
    out = jnp.dot(weight, arrived[...].reshape(groups * CAP, part), precision=lax.Precision.HIGHEST,
                  preferred_element_type=jnp.float32)
    mixed[...] = out.astype(mixed.dtype)
    wait_all(outgoing, out_sem)
    for swap in swaps:
        swap.wait_send()
    for piece in pieces:
        for d in others:
            give(d, piece).wait_send()
    wait_for(arrived, back_send, groups)


def solution(mesh):
    groups, shares = mesh.shape["ep"], mesh.shape["tp"]

    def local(tokens, norm_gain, routing, route_weight, w_gate, w_up, w_down):
        count, width = tokens.shape
        part = width // shares
        half, planes = groups // 2, shares // 2
        rows = half * CAP
        share = w_down.shape[1]
        pieces = sum(map(len, PIECES))
        vmem = pl.BlockSpec(memory_space=pltpu.VMEM)
        hbm = pl.BlockSpec(memory_space=pltpu.HBM)
        return pl.pallas_call(
            functools.partial(kernel, groups, shares),
            out_shape=pltpu.VMEM((count, part), jnp.bfloat16),
            in_specs=[hbm] * 7,
            out_specs=vmem,
            scratch_shapes=[
                pltpu.VMEM((count, width), tokens.dtype),
                pltpu.VMEM((1, width), norm_gain.dtype),
                pltpu.VMEM(routing.shape[::-1], routing.dtype),
                pltpu.VMEM(route_weight.shape[::-1], route_weight.dtype),
                pltpu.VMEM((2 * share, width), jnp.bfloat16),
                pltpu.VMEM((2 * share, width), jnp.bfloat16),
                pltpu.VMEM((2 * share, width), jnp.bfloat16),
                pltpu.VMEM((width, 2 * share), jnp.bfloat16),
                pltpu.VMEM((width, 2 * share), jnp.bfloat16),
                pltpu.VMEM((half, CAP, width), jnp.bfloat16),
                pltpu.VMEM((half, CAP, width), jnp.bfloat16),
                pltpu.VMEM((planes - 1, 2, rows, part), jnp.float32),
                pltpu.VMEM((planes - 1, 2, rows, part), jnp.float32),
                pltpu.VMEM((2, half, CAP, part), jnp.float32),
                pltpu.VMEM((groups, CAP, part), jnp.float32),
                pltpu.SemaphoreType.DMA((7,)),
                pltpu.SemaphoreType.DMA((3,)),
                pltpu.SemaphoreType.DMA((3,)),
                pltpu.SemaphoreType.DMA,
                pltpu.SemaphoreType.DMA((len(CHUNKS),)),
                pltpu.SemaphoreType.DMA((planes - 1, pieces)),
                pltpu.SemaphoreType.DMA((planes - 1, pieces)),
                pltpu.SemaphoreType.DMA,
                pltpu.SemaphoreType.DMA,
            ],
            compiler_params=pltpu.CompilerParams(collective_id=0, has_side_effects=True,
                                                 vmem_limit_bytes=67043328 - 16384),
            name="experts",
        )(tokens, norm_gain.reshape(1, width), routing.T, route_weight.T,
          jnp.swapaxes(w_gate, 1, 2), jnp.swapaxes(w_up, 1, 2), w_down)

    in_specs = (
        P("ep", None),
        P(),
        P("ep", None),
        P("ep", None),
        P("ep", None, "tp"),
        P("ep", None, "tp"),
        P("ep", "tp", None),
    )
    return jax.shard_map(local, mesh=mesh, in_specs=in_specs, out_specs=P("ep", "tp"), check_vma=False)
```

```python
import functools

import jax
import jax.numpy as jnp
from jax import lax
from jax.experimental import pallas as pl
from jax.experimental.pallas import tpu as pltpu
from jax.sharding import PartitionSpec as P

CAP = 8
XS = 4
CHUNKS = ((0, 16),)
PIECES = (((0, 4, 1), (0, 8, 0), (4, 16, 1), (8, 16, 0)),)
STEPS = ('c0', 'r0', 'r1', 'r2', 'r3')
STEPS_16 = 32767.0
LEAST = 2e-34
MESH = pl.DeviceIdType.MESH

norm_eps = 1e-06


def kernel(groups, shares, tokens_hbm, gain_hbm, routing_hbm, route_weight_hbm, gate_hbm, up_hbm, down_hbm, mixed,
           tokens, gain, routing, route_weight, gate, up, down, gate_across, up_across,
           outgoing, helping, incoming, partial, reduced, peak, their_peak, back, arrived,
           load_sem, swap_send, swap_recv, out_sem, help_sem, in_sem, part_send, part_recv, peak_send, peak_recv, back_send, back_recv):
    ep, tp = lax.axis_index("ep"), lax.axis_index("tp")
    width = tokens.shape[1]
    part = mixed.shape[1]
    half = groups // 2
    rows = half * CAP
    planes = shares // 2
    share = gate_hbm.shape[1]
    y, core = tp // 2, lax.rem(tp, 2)
    zs = groups // XS
    z, x = ep // XS, lax.rem(ep, XS)
    lower = 1 - z // (zs // 2)
    theirs, goal = half * (1 - core), half * core

    def near(q, dx):
        return XS * lax.rem(z + q, zs // 2) + lax.rem(x + dx, XS)

    rounds = [(q, dx) for dx in (2, 3, 1, 0) for q in (0, 3, 1, 2)]

    chunk_of = {p: k for k, (first, upto) in enumerate(CHUNKS) for p in range(first, upto)}
    tile = 2 * part

    barrier = pltpu.get_barrier_semaphore()
    closer = [(q, dx) for q, dx in rounds if q == 2]
    cross = jnp.logical_and(lower == 0, core == 1).astype(jnp.int32)
    for q, dx in rounds:
        other = 1 - lower - cross if (q, dx) in closer else 1 - lower
        pl.semaphore_signal(barrier, inc=1, device_id=(theirs + near(q, dx), 2 * y + other), device_id_type=MESH)
    for d in range(1, planes):
        pl.semaphore_signal(barrier, inc=1, device_id=(ep, 2 * lax.rem(y + d, planes) + core), device_id_type=MESH)
    pl.semaphore_signal(barrier, inc=1, device_id=(ep, 2 * y + 1 - core), device_id_type=MESH)

    pairs = ((tokens_hbm, tokens), (gain_hbm, gain), (routing_hbm, routing), (route_weight_hbm, route_weight),
             (gate_hbm.at[0], gate.at[0:share]), (up_hbm.at[0], up.at[0:share]), (down_hbm.at[0], down.at[0:share]))
    loads = [pltpu.make_async_copy(source, target, load_sem.at[i]) for i, (source, target) in enumerate(pairs)]
    for i in (2, 3, 0, 1, 4, 5, 6):
        loads[i].start()

    count = tokens.shape[0]
    earlier = lax.broadcasted_iota(jnp.int32, (count, count), 0) < lax.broadcasted_iota(jnp.int32, (count, count), 1)
    earlier = jnp.where(earlier, 1.0, 0.0).astype(jnp.bfloat16)

    def slots_of(lines, expert_of):
        line = lax.broadcasted_iota(jnp.int32, (lines, count), 0)
        expert = expert_of(line // CAP)
        member = jnp.zeros((lines, count), jnp.float32)
        weight = jnp.zeros((lines, count), jnp.float32)
        for k in range(routing.shape[0]):
            named = routing[k:k + 1, :] == expert
            member = jnp.where(named, 1.0, member)
            weight = jnp.where(named, route_weight[k:k + 1, :], weight)
        before = jnp.dot(member.astype(jnp.bfloat16), earlier, preferred_element_type=jnp.float32)
        placed = jnp.where(before == lax.rem(line, CAP).astype(jnp.float32), member, 0.0)
        return placed, weight

    loads[2].wait()
    loads[3].wait()
    placed, _ = slots_of(rows, lambda p: goal + p)
    loads[0].wait()
    loads[1].wait()
    values = tokens[...].astype(jnp.float32)
    scale = lax.rsqrt(jnp.mean(values * values, axis=-1, keepdims=True) + norm_eps)
    normed = (values * scale * gain[...]).astype(jnp.bfloat16)
    sent = jnp.dot(placed.astype(jnp.bfloat16), normed, preferred_element_type=jnp.float32)
    outgoing[...] = sent.reshape(half, CAP, width).astype(jnp.bfloat16)
    helps = jnp.logical_and(lower == 1, core == 0)

    @pl.when(helps)
    def _():
        more, _ = slots_of(rows, lambda p: half + p)
        sent = jnp.dot(more.astype(jnp.bfloat16), normed, preferred_element_type=jnp.float32)
        helping[...] = sent.reshape(half, CAP, width).astype(jnp.bfloat16)

    pl.semaphore_wait(barrier, half + planes + len(closer) * lower * (1 - 2 * core))

    def send_block(block, sem, expert):
        pltpu.make_async_remote_copy(
            src_ref=block, dst_ref=incoming.at[lax.rem(ep, half)], send_sem=sem, recv_sem=in_sem.at[0],
            device_id=(expert, 2 * y + lower), device_id_type=MESH).start()

    def help_out():
        for q, dx in closer:
            p = near(q, dx)
            send_block(helping.at[p], help_sem, half + p)

    keeps = jnp.logical_or(lower == 0, core == 0)

    def dispatch():
        for q, dx in rounds:
            def send(p=near(q, dx)):
                send_block(outgoing.at[p], out_sem, goal + p)
            if (q, dx) in closer:
                pl.when(keeps)(send)
            else:
                send()

    pl.when(helps)(help_out)
    pl.when(lower + 1 - core > 0)(dispatch)

    swaps = [pltpu.make_async_remote_copy(
        src_ref=ref.at[0:share], dst_ref=ref.at[share:2 * share], send_sem=swap_send.at[i], recv_sem=swap_recv.at[i],
        device_id=(ep, 2 * y + 1 - core), device_id_type=MESH) for i, ref in enumerate((gate, up, down))]
    for i in (4, 5, 6):
        loads[i].wait()
    for swap in swaps:
        swap.start()

    picked, weight = slots_of(groups * CAP, lambda q: q)
    weight = jnp.transpose(weight * picked)

    for swap in swaps:
        swap.wait_recv()
    pl.when(lower + 1 - core == 0)(dispatch)
    gate_across[...] = jnp.transpose(gate[...])
    up_across[...] = jnp.transpose(up[...])

    def wait_for(ref, sem, most):
        less, full = ref.at[pl.ds(0, most - 1)], ref.at[pl.ds(0, most)]
        pl.when(core == lower)(lambda: pltpu.make_async_copy(less, less, sem).wait())
        pl.when(core != lower)(lambda: pltpu.make_async_copy(full, full, sem).wait())

    def wait_all(ref, sem):
        pltpu.make_async_copy(ref, ref, sem).wait()

    pieces = [piece for some in PIECES for piece in some]
    totals = {}
    others = range(planes - 1)

    def plane(d):
        return d + (d + planes - y) // planes

    def seen_at(d):
        return y - (y + planes - 1 - plane(d)) // planes

    def columns(to):
        return pl.ds(pl.multiple_of(to * tile, tile), tile)

    def give(d, piece):
        some, side, k = pl.ds(piece[0] * CAP, (piece[1] - piece[0]) * CAP), piece[2], pieces.index(piece)
        return pltpu.make_async_remote_copy(
            src_ref=partial.at[d, side, some], dst_ref=reduced.at[seen_at(d), side, some],
            send_sem=part_send.at[d, k], recv_sem=part_recv.at[seen_at(d), k],
            device_id=(ep, 2 * plane(d) + core), device_id_type=MESH)

    def received(d, piece):
        some, side, k = pl.ds(piece[0] * CAP, (piece[1] - piece[0]) * CAP), piece[2], pieces.index(piece)
        return pltpu.make_async_copy(reduced.at[d, side, some], reduced.at[d, side, some], part_recv.at[d, k])

    def give_peak(d):
        return pltpu.make_async_remote_copy(
            src_ref=peak.at[d], dst_ref=their_peak.at[seen_at(d)], send_sem=peak_send.at[d],
            recv_sem=peak_recv.at[seen_at(d)], device_id=(ep, 2 * plane(d) + core), device_id_type=MESH)

    def multiply(k):
        first, upto = CHUNKS[k]
        wait_all(incoming.at[pl.ds(first, upto - first)], in_sem.at[k])
        a = incoming[first:upto].astype(jnp.float32).reshape((upto - first) * CAP, width).astype(jnp.bfloat16)
        gate_act = jnp.dot(a, gate_across[...], preferred_element_type=jnp.float32)
        up_act = jnp.dot(a, up_across[...], preferred_element_type=jnp.float32)
        hidden = (gate_act / (1.0 + jnp.exp(-gate_act)) * up_act).astype(jnp.bfloat16)
        for d in others:
            block = jnp.dot(hidden, down[:, columns(plane(d))], preferred_element_type=jnp.float32)
            sides = [block[:, side * part:(side + 1) * part].reshape(upto - first, CAP, part) for side in range(2)]
            most = jnp.maximum(jnp.max(jnp.maximum(jnp.abs(sides[0]), jnp.abs(sides[1])), axis=0), LEAST)
            peak[d] = most
            give_peak(d).start()
            for side in range(2):
                coded = jnp.round(sides[side] * (STEPS_16 / most)).reshape((upto - first) * CAP, part)
                partial[d, side, first * CAP:upto * CAP] = (
                    coded.astype(jnp.int32).astype(jnp.int16))
            give(d, PIECES[k][0]).start()
        for piece in PIECES[k][1:]:
            for d in others:
                give(d, piece).start()
        mine = jnp.dot(hidden, down[:, columns(y)], preferred_element_type=jnp.float32)
        for piece in PIECES[k]:
            totals[piece] = mine[(piece[0] - first) * CAP:(piece[1] - first) * CAP]

    def give_back(k):
        piece = pieces[k]
        first, upto, side = piece
        for d in others:
            if k == 0:
                pltpu.make_async_copy(their_peak.at[d], their_peak.at[d], peak_recv.at[d]).wait()
            received(d, piece).wait()
        total = totals[piece][:, side * part:(side + 1) * part].reshape(upto - first, CAP, part)
        for d in others:
            coded = reduced[d, side, first * CAP:upto * CAP].astype(jnp.int32).astype(jnp.float32)
            total = total + coded.reshape(upto - first, CAP, part) * (their_peak[d] * (1.0 / STEPS_16))
        back[side, first:upto] = total
        for start in range(first, upto, XS):
            for dx in (2, 3, 1, 0):
                p = start + lax.rem(x + dx, XS)

                def send(p=p):
                    pltpu.make_async_remote_copy(
                        src_ref=back.at[side, p], dst_ref=arrived.at[ep], send_sem=back_send, recv_sem=back_recv,
                        device_id=(theirs + p, 2 * y + side), device_id_type=MESH).start()

                def hold(p=p):
                    arrived[ep] = back[side, p]
                if dx == 0:
                    here = jnp.logical_and(theirs + p == ep, core == side)
                    pl.when(here)(hold)
                    pl.when(jnp.logical_not(here))(send)
                else:
                    send()

    for step in STEPS:
        (multiply if step[0] == "c" else give_back)(int(step[1:]))

    wait_for(arrived, back_recv, groups)
    out = jnp.dot(weight, arrived[...].reshape(groups * CAP, part), precision=lax.Precision.HIGHEST,
                  preferred_element_type=jnp.float32)
    mixed[...] = out.astype(mixed.dtype)
    def wait_some(ref, blocks, sem):
        some = ref.at[pl.ds(0, blocks)]
        pltpu.make_async_copy(some, some, sem).wait()
    pl.when(keeps)(lambda: wait_some(outgoing, half, out_sem))
    pl.when(jnp.logical_not(keeps))(lambda: wait_some(outgoing, half - len(closer), out_sem))
    pl.when(helps)(lambda: wait_some(helping, len(closer), help_sem))
    for swap in swaps:
        swap.wait_send()
    for d in others:
        give_peak(d).wait_send()
    for piece in pieces:
        for d in others:
            give(d, piece).wait_send()
    wait_for(arrived, back_send, groups)


def solution(mesh):
    groups, shares = mesh.shape["ep"], mesh.shape["tp"]

    def local(tokens, norm_gain, routing, route_weight, w_gate, w_up, w_down):
        count, width = tokens.shape
        part = width // shares
        half, planes = groups // 2, shares // 2
        rows = half * CAP
        share = w_down.shape[1]
        pieces = sum(map(len, PIECES))
        vmem = pl.BlockSpec(memory_space=pltpu.VMEM)
        hbm = pl.BlockSpec(memory_space=pltpu.HBM)
        return pl.pallas_call(
            functools.partial(kernel, groups, shares),
            out_shape=pltpu.VMEM((count, part), jnp.bfloat16),
            in_specs=[hbm] * 7,
            out_specs=vmem,
            scratch_shapes=[
                pltpu.VMEM((count, width), tokens.dtype),
                pltpu.VMEM((1, width), norm_gain.dtype),
                pltpu.VMEM(routing.shape[::-1], routing.dtype),
                pltpu.VMEM(route_weight.shape[::-1], route_weight.dtype),
                pltpu.VMEM((2 * share, width), jnp.bfloat16),
                pltpu.VMEM((2 * share, width), jnp.bfloat16),
                pltpu.VMEM((2 * share, width), jnp.bfloat16),
                pltpu.VMEM((width, 2 * share), jnp.bfloat16),
                pltpu.VMEM((width, 2 * share), jnp.bfloat16),
                pltpu.VMEM((half, CAP, width), jnp.bfloat16),
                pltpu.VMEM((half, CAP, width), jnp.bfloat16),
                pltpu.VMEM((half, CAP, width), jnp.bfloat16),
                pltpu.VMEM((planes - 1, 2, rows, part), jnp.int16),
                pltpu.VMEM((planes - 1, 2, rows, part), jnp.int16),
                pltpu.VMEM((planes - 1, CAP, part), jnp.float32),
                pltpu.VMEM((planes - 1, CAP, part), jnp.float32),
                pltpu.VMEM((2, half, CAP, part), jnp.float32),
                pltpu.VMEM((groups, CAP, part), jnp.float32),
                pltpu.SemaphoreType.DMA((7,)),
                pltpu.SemaphoreType.DMA((3,)),
                pltpu.SemaphoreType.DMA((3,)),
                pltpu.SemaphoreType.DMA,
                pltpu.SemaphoreType.DMA,
                pltpu.SemaphoreType.DMA((len(CHUNKS),)),
                pltpu.SemaphoreType.DMA((planes - 1, pieces)),
                pltpu.SemaphoreType.DMA((planes - 1, pieces)),
                pltpu.SemaphoreType.DMA((planes - 1,)),
                pltpu.SemaphoreType.DMA((planes - 1,)),
                pltpu.SemaphoreType.DMA,
                pltpu.SemaphoreType.DMA,
            ],
            compiler_params=pltpu.CompilerParams(collective_id=0, has_side_effects=True,
                                                 vmem_limit_bytes=67043328 - 16384),
            name="experts",
        )(tokens, norm_gain.reshape(1, width), routing.T, route_weight.T,
          jnp.swapaxes(w_gate, 1, 2), jnp.swapaxes(w_up, 1, 2), w_down)

    in_specs = (
        P("ep", None),
        P(),
        P("ep", None),
        P("ep", None),
        P("ep", None, "tp"),
        P("ep", None, "tp"),
        P("ep", "tp", None),
    )
    return jax.shard_map(local, mesh=mesh, in_specs=in_specs, out_specs=P("ep", "tp"), check_vma=False)
```

```python
import functools

import jax
import jax.numpy as jnp
from jax import lax
from jax.experimental import pallas as pl
from jax.experimental.pallas import tpu as pltpu
from jax.sharding import PartitionSpec as P

CAP = 8
XS = 4
CHUNKS = ((0, 16),)
PIECES = (((0, 4, 1), (0, 8, 0), (4, 16, 1), (8, 16, 0)),)
STEPS = ('c0', 'r0', 'r1', 'r2', 'r3')
STEPS_16 = 32767.0
LEAST = 2e-34
MESH = pl.DeviceIdType.MESH

norm_eps = 1e-06


def kernel(groups, shares, tokens_hbm, gain_hbm, routing_hbm, route_weight_hbm, gate_hbm, up_hbm, down_hbm, mixed,
           tokens, gain, routing, route_weight, gate, up, down, gate_across, up_across,
           outgoing, helping, incoming, partial, reduced, peak, their_peak, back, arrived,
           load_sem, swap_send, swap_recv, out_sem, help_sem, in_sem, part_send, part_recv, peak_send, peak_recv, back_send, back_recv):
    ep, tp = lax.axis_index("ep"), lax.axis_index("tp")
    width = tokens.shape[1]
    part = mixed.shape[1]
    half = groups // 2
    rows = half * CAP
    planes = shares // 2
    share = gate_hbm.shape[1]
    y, core = tp // 2, lax.rem(tp, 2)
    zs = groups // XS
    z, x = ep // XS, lax.rem(ep, XS)
    lower = 1 - z // (zs // 2)
    theirs, goal = half * (1 - core), half * core

    def near(q, dx):
        return XS * lax.rem(z + q, zs // 2) + lax.rem(x + dx, XS)

    rounds = [(q, dx) for dx in (2, 3, 1, 0) for q in (0, 1, 3, 2)]

    chunk_of = {p: k for k, (first, upto) in enumerate(CHUNKS) for p in range(first, upto)}
    tile = 2 * part

    barrier = pltpu.get_barrier_semaphore()
    closer = [(q, dx) for q, dx in rounds if q == 2]
    cross = jnp.logical_and(lower == 0, core == 1).astype(jnp.int32)
    for q, dx in rounds:
        other = 1 - lower - cross if (q, dx) in closer else 1 - lower
        pl.semaphore_signal(barrier, inc=1, device_id=(theirs + near(q, dx), 2 * y + other), device_id_type=MESH)
    for d in range(1, planes):
        pl.semaphore_signal(barrier, inc=1, device_id=(ep, 2 * lax.rem(y + d, planes) + core), device_id_type=MESH)
    pl.semaphore_signal(barrier, inc=1, device_id=(ep, 2 * y + 1 - core), device_id_type=MESH)

    pairs = ((tokens_hbm, tokens), (gain_hbm, gain), (routing_hbm, routing), (route_weight_hbm, route_weight),
             (gate_hbm.at[0], gate.at[0:share]), (up_hbm.at[0], up.at[0:share]), (down_hbm.at[0], down.at[0:share]))
    loads = [pltpu.make_async_copy(source, target, load_sem.at[i]) for i, (source, target) in enumerate(pairs)]
    for i in (2, 3, 0, 1, 4, 5, 6):
        loads[i].start()

    count = tokens.shape[0]
    earlier = lax.broadcasted_iota(jnp.int32, (count, count), 0) < lax.broadcasted_iota(jnp.int32, (count, count), 1)
    earlier = jnp.where(earlier, 1.0, 0.0).astype(jnp.bfloat16)

    def slots_of(lines, expert_of):
        line = lax.broadcasted_iota(jnp.int32, (lines, count), 0)
        expert = expert_of(line // CAP)
        member = jnp.zeros((lines, count), jnp.float32)
        weight = jnp.zeros((lines, count), jnp.float32)
        for k in range(routing.shape[0]):
            named = routing[k:k + 1, :] == expert
            member = jnp.where(named, 1.0, member)
            weight = jnp.where(named, route_weight[k:k + 1, :], weight)
        before = jnp.dot(member.astype(jnp.bfloat16), earlier, preferred_element_type=jnp.float32)
        placed = jnp.where(before == lax.rem(line, CAP).astype(jnp.float32), member, 0.0)
        return placed, weight

    loads[2].wait()
    loads[3].wait()
    placed, _ = slots_of(rows, lambda p: goal + p)
    loads[0].wait()
    loads[1].wait()
    values = tokens[...].astype(jnp.float32)
    scale = lax.rsqrt(jnp.mean(values * values, axis=-1, keepdims=True) + norm_eps)
    normed = (values * scale * gain[...]).astype(jnp.bfloat16)
    sent = jnp.dot(placed.astype(jnp.bfloat16), normed, preferred_element_type=jnp.float32)
    outgoing[...] = sent.reshape(half, CAP, width).astype(jnp.bfloat16)
    helps = jnp.logical_and(lower == 1, core == 0)

    @pl.when(helps)
    def _():
        more, _ = slots_of(rows, lambda p: half + p)
        sent = jnp.dot(more.astype(jnp.bfloat16), normed, preferred_element_type=jnp.float32)
        helping[...] = sent.reshape(half, CAP, width).astype(jnp.bfloat16)

    pl.semaphore_wait(barrier, half + planes + len(closer) * lower * (1 - 2 * core))

    def send_block(block, sem, expert):
        pltpu.make_async_remote_copy(
            src_ref=block, dst_ref=incoming.at[lax.rem(ep, half)], send_sem=sem, recv_sem=in_sem.at[0],
            device_id=(expert, 2 * y + lower), device_id_type=MESH).start()

    def help_out():
        for q, dx in closer:
            p = near(q, dx)
            send_block(helping.at[p], help_sem, half + p)

    keeps = jnp.logical_or(lower == 0, core == 0)

    def dispatch():
        for q, dx in rounds:
            def send(p=near(q, dx)):
                send_block(outgoing.at[p], out_sem, goal + p)
            if (q, dx) in closer:
                pl.when(keeps)(send)
            else:
                send()

    pl.when(helps)(help_out)
    pl.when(lower + 1 - core > 0)(dispatch)

    swaps = [pltpu.make_async_remote_copy(
        src_ref=ref.at[0:share], dst_ref=ref.at[share:2 * share], send_sem=swap_send.at[i], recv_sem=swap_recv.at[i],
        device_id=(ep, 2 * y + 1 - core), device_id_type=MESH) for i, ref in enumerate((gate, up, down))]
    for i in (4, 5, 6):
        loads[i].wait()
    for swap in swaps:
        swap.start()

    picked, weight = slots_of(groups * CAP, lambda q: q)
    weight = jnp.transpose(weight * picked)

    for swap in swaps:
        swap.wait_recv()
    pl.when(lower + 1 - core == 0)(dispatch)
    gate_across[...] = jnp.transpose(gate[...])
    up_across[...] = jnp.transpose(up[...])

    def wait_for(ref, sem, most):
        less, full = ref.at[pl.ds(0, most - 1)], ref.at[pl.ds(0, most)]
        pl.when(core == lower)(lambda: pltpu.make_async_copy(less, less, sem).wait())
        pl.when(core != lower)(lambda: pltpu.make_async_copy(full, full, sem).wait())

    def wait_all(ref, sem):
        pltpu.make_async_copy(ref, ref, sem).wait()

    pieces = [piece for some in PIECES for piece in some]
    totals = {}
    others = range(planes - 1)

    def plane(d):
        return d + (d + planes - y) // planes

    def seen_at(d):
        return y - (y + planes - 1 - plane(d)) // planes

    def columns(to):
        return pl.ds(pl.multiple_of(to * tile, tile), tile)

    def give(d, piece):
        some, side, k = pl.ds(piece[0] * CAP, (piece[1] - piece[0]) * CAP), piece[2], pieces.index(piece)
        return pltpu.make_async_remote_copy(
            src_ref=partial.at[d, side, some], dst_ref=reduced.at[seen_at(d), side, some],
            send_sem=part_send.at[d, k], recv_sem=part_recv.at[seen_at(d), k],
            device_id=(ep, 2 * plane(d) + core), device_id_type=MESH)

    def received(d, piece):
        some, side, k = pl.ds(piece[0] * CAP, (piece[1] - piece[0]) * CAP), piece[2], pieces.index(piece)
        return pltpu.make_async_copy(reduced.at[d, side, some], reduced.at[d, side, some], part_recv.at[d, k])

    def give_peak(d):
        return pltpu.make_async_remote_copy(
            src_ref=peak.at[d], dst_ref=their_peak.at[seen_at(d)], send_sem=peak_send.at[d],
            recv_sem=peak_recv.at[seen_at(d)], device_id=(ep, 2 * plane(d) + core), device_id_type=MESH)

    def multiply(k):
        first, upto = CHUNKS[k]
        wait_all(incoming.at[pl.ds(first, upto - first)], in_sem.at[k])
        a = incoming[first:upto].astype(jnp.float32).reshape((upto - first) * CAP, width).astype(jnp.bfloat16)
        gate_act = jnp.dot(a, gate_across[...], preferred_element_type=jnp.float32)
        up_act = jnp.dot(a, up_across[...], preferred_element_type=jnp.float32)
        hidden = (gate_act / (1.0 + jnp.exp(-gate_act)) * up_act).astype(jnp.bfloat16)
        for d in others:
            block = jnp.dot(hidden, down[:, columns(plane(d))], preferred_element_type=jnp.float32)
            sides = [block[:, side * part:(side + 1) * part].reshape(upto - first, CAP, part) for side in range(2)]
            most = jnp.maximum(jnp.max(jnp.maximum(jnp.abs(sides[0]), jnp.abs(sides[1])), axis=0), LEAST)
            peak[d] = most
            give_peak(d).start()
            for side in range(2):
                coded = jnp.round(sides[side] * (STEPS_16 / most)).reshape((upto - first) * CAP, part)
                partial[d, side, first * CAP:upto * CAP] = (
                    coded.astype(jnp.int32).astype(jnp.int16))
            give(d, PIECES[k][0]).start()
        for piece in PIECES[k][1:]:
            for d in others:
                give(d, piece).start()
        mine = jnp.dot(hidden, down[:, columns(y)], preferred_element_type=jnp.float32)
        for piece in PIECES[k]:
            totals[piece] = mine[(piece[0] - first) * CAP:(piece[1] - first) * CAP]

    def give_back(k):
        piece = pieces[k]
        first, upto, side = piece
        for d in others:
            if k == 0:
                pltpu.make_async_copy(their_peak.at[d], their_peak.at[d], peak_recv.at[d]).wait()
            received(d, piece).wait()
        total = totals[piece][:, side * part:(side + 1) * part].reshape(upto - first, CAP, part)
        for d in others:
            coded = reduced[d, side, first * CAP:upto * CAP].astype(jnp.int32).astype(jnp.float32)
            total = total + coded.reshape(upto - first, CAP, part) * (their_peak[d] * (1.0 / STEPS_16))
        back[side, first:upto] = total
        for start in range(first, upto, XS):
            for dx in (2, 1, 3, 0):
                p = start + lax.rem(x + dx, XS)

                def send(p=p):
                    pltpu.make_async_remote_copy(
                        src_ref=back.at[side, p], dst_ref=arrived.at[ep], send_sem=back_send, recv_sem=back_recv,
                        device_id=(theirs + p, 2 * y + side), device_id_type=MESH).start()

                def hold(p=p):
                    arrived[ep] = back[side, p]
                if dx == 0:
                    here = jnp.logical_and(theirs + p == ep, core == side)
                    pl.when(here)(hold)
                    pl.when(jnp.logical_not(here))(send)
                else:
                    send()

    for step in STEPS:
        (multiply if step[0] == "c" else give_back)(int(step[1:]))

    wait_for(arrived, back_recv, groups)
    out = jnp.dot(weight, arrived[...].reshape(groups * CAP, part), precision=lax.Precision.HIGHEST,
                  preferred_element_type=jnp.float32)
    mixed[...] = out.astype(mixed.dtype)
    def wait_some(ref, blocks, sem):
        some = ref.at[pl.ds(0, blocks)]
        pltpu.make_async_copy(some, some, sem).wait()
    pl.when(keeps)(lambda: wait_some(outgoing, half, out_sem))
    pl.when(jnp.logical_not(keeps))(lambda: wait_some(outgoing, half - len(closer), out_sem))
    pl.when(helps)(lambda: wait_some(helping, len(closer), help_sem))
    for swap in swaps:
        swap.wait_send()
    for d in others:
        give_peak(d).wait_send()
    for piece in pieces:
        for d in others:
            give(d, piece).wait_send()
    wait_for(arrived, back_send, groups)


def solution(mesh):
    groups, shares = mesh.shape["ep"], mesh.shape["tp"]

    def local(tokens, norm_gain, routing, route_weight, w_gate, w_up, w_down):
        count, width = tokens.shape
        part = width // shares
        half, planes = groups // 2, shares // 2
        rows = half * CAP
        share = w_down.shape[1]
        pieces = sum(map(len, PIECES))
        vmem = pl.BlockSpec(memory_space=pltpu.VMEM)
        hbm = pl.BlockSpec(memory_space=pltpu.HBM)
        return pl.pallas_call(
            functools.partial(kernel, groups, shares),
            out_shape=pltpu.VMEM((count, part), jnp.bfloat16),
            in_specs=[hbm] * 7,
            out_specs=vmem,
            scratch_shapes=[
                pltpu.VMEM((count, width), tokens.dtype),
                pltpu.VMEM((1, width), norm_gain.dtype),
                pltpu.VMEM(routing.shape[::-1], routing.dtype),
                pltpu.VMEM(route_weight.shape[::-1], route_weight.dtype),
                pltpu.VMEM((2 * share, width), jnp.bfloat16),
                pltpu.VMEM((2 * share, width), jnp.bfloat16),
                pltpu.VMEM((2 * share, width), jnp.bfloat16),
                pltpu.VMEM((width, 2 * share), jnp.bfloat16),
                pltpu.VMEM((width, 2 * share), jnp.bfloat16),
                pltpu.VMEM((half, CAP, width), jnp.bfloat16),
                pltpu.VMEM((half, CAP, width), jnp.bfloat16),
                pltpu.VMEM((half, CAP, width), jnp.bfloat16),
                pltpu.VMEM((planes - 1, 2, rows, part), jnp.int16),
                pltpu.VMEM((planes - 1, 2, rows, part), jnp.int16),
                pltpu.VMEM((planes - 1, CAP, part), jnp.float32),
                pltpu.VMEM((planes - 1, CAP, part), jnp.float32),
                pltpu.VMEM((2, half, CAP, part), jnp.float32),
                pltpu.VMEM((groups, CAP, part), jnp.float32),
                pltpu.SemaphoreType.DMA((7,)),
                pltpu.SemaphoreType.DMA((3,)),
                pltpu.SemaphoreType.DMA((3,)),
                pltpu.SemaphoreType.DMA,
                pltpu.SemaphoreType.DMA,
                pltpu.SemaphoreType.DMA((len(CHUNKS),)),
                pltpu.SemaphoreType.DMA((planes - 1, pieces)),
                pltpu.SemaphoreType.DMA((planes - 1, pieces)),
                pltpu.SemaphoreType.DMA((planes - 1,)),
                pltpu.SemaphoreType.DMA((planes - 1,)),
                pltpu.SemaphoreType.DMA,
                pltpu.SemaphoreType.DMA,
            ],
            compiler_params=pltpu.CompilerParams(collective_id=0, has_side_effects=True,
                                                 vmem_limit_bytes=67043328 - 16384),
            name="experts",
        )(tokens, norm_gain.reshape(1, width), routing.T, route_weight.T,
          jnp.swapaxes(w_gate, 1, 2), jnp.swapaxes(w_up, 1, 2), w_down)

    in_specs = (
        P("ep", None),
        P(),
        P("ep", None),
        P("ep", None),
        P("ep", None, "tp"),
        P("ep", None, "tp"),
        P("ep", "tp", None),
    )
    return jax.shard_map(local, mesh=mesh, in_specs=in_specs, out_specs=P("ep", "tp"), check_vma=False)
```

```python
import functools

import jax
import jax.numpy as jnp
from jax import lax
from jax.experimental import pallas as pl
from jax.experimental.pallas import tpu as pltpu
from jax.sharding import PartitionSpec as P

CAP = 8
XS = 4
CHUNKS = ((0, 16),)
PIECES = (((0, 8, 1), (8, 12, 1), (0, 8, 0), (8, 12, 0), (12, 16, 1), (12, 16, 0)),)
STEPS = ('c0', 'r0', 'r1', 'r2', 'r3', 'r4', 'r5')
MESH = pl.DeviceIdType.MESH

norm_eps = 1e-06


def kernel(groups, shares, tokens_hbm, gain_hbm, routing_hbm, route_weight_hbm, gate_hbm, up_hbm, down_hbm, mixed,
           tokens, gain, routing, route_weight, gate, up, down, gate_across, up_across,
           outgoing, helping, incoming, partial, reduced, back, arrived,
           load_sem, swap_send, swap_recv, out_sem, help_sem, in_sem, part_send, part_recv, back_send, back_recv):
    ep, tp = lax.axis_index("ep"), lax.axis_index("tp")
    width = tokens.shape[1]
    part = mixed.shape[1]
    half = groups // 2
    rows = half * CAP
    planes = shares // 2
    share = gate_hbm.shape[1]
    y, core = tp // 2, lax.rem(tp, 2)
    zs = groups // XS
    z, x = ep // XS, lax.rem(ep, XS)
    lower = 1 - z // (zs // 2)
    theirs, goal = half * (1 - core), half * core

    def near(q, dx):
        return XS * lax.rem(z + q, zs // 2) + lax.rem(x + dx, XS)

    rounds = [(q, dx) for dx in (2, 3, 1, 0) for q in (0, 1, 3, 2)]

    chunk_of = {p: k for k, (first, upto) in enumerate(CHUNKS) for p in range(first, upto)}
    tile = 2 * part

    barrier = pltpu.get_barrier_semaphore()
    closer = [(q, dx) for q, dx in rounds if q == 2]
    cross = jnp.logical_and(lower == 0, core == 1).astype(jnp.int32)
    for q, dx in rounds:
        other = 1 - lower - cross if (q, dx) in closer else 1 - lower
        pl.semaphore_signal(barrier, inc=1, device_id=(theirs + near(q, dx), 2 * y + other), device_id_type=MESH)
    for d in range(1, planes):
        pl.semaphore_signal(barrier, inc=1, device_id=(ep, 2 * lax.rem(y + d, planes) + core), device_id_type=MESH)
    pl.semaphore_signal(barrier, inc=1, device_id=(ep, 2 * y + 1 - core), device_id_type=MESH)

    pairs = ((tokens_hbm, tokens), (gain_hbm, gain), (routing_hbm, routing), (route_weight_hbm, route_weight),
             (gate_hbm.at[0], gate.at[0:share]), (up_hbm.at[0], up.at[0:share]), (down_hbm.at[0], down.at[0:share]))
    loads = [pltpu.make_async_copy(source, target, load_sem.at[i]) for i, (source, target) in enumerate(pairs)]
    for i in (2, 3, 0, 1, 4, 5, 6):
        loads[i].start()

    count = tokens.shape[0]
    earlier = lax.broadcasted_iota(jnp.int32, (count, count), 0) < lax.broadcasted_iota(jnp.int32, (count, count), 1)
    earlier = jnp.where(earlier, 1.0, 0.0).astype(jnp.bfloat16)

    def slots_of(lines, expert_of):
        line = lax.broadcasted_iota(jnp.int32, (lines, count), 0)
        expert = expert_of(line // CAP)
        member = jnp.zeros((lines, count), jnp.float32)
        weight = jnp.zeros((lines, count), jnp.float32)
        for k in range(routing.shape[0]):
            named = routing[k:k + 1, :] == expert
            member = jnp.where(named, 1.0, member)
            weight = jnp.where(named, route_weight[k:k + 1, :], weight)
        before = jnp.dot(member.astype(jnp.bfloat16), earlier, preferred_element_type=jnp.float32)
        placed = jnp.where(before == lax.rem(line, CAP).astype(jnp.float32), member, 0.0)
        return placed, weight

    loads[2].wait()
    loads[3].wait()
    placed, _ = slots_of(rows, lambda p: goal + p)
    loads[0].wait()
    loads[1].wait()
    values = tokens[...].astype(jnp.float32)
    scale = lax.rsqrt(jnp.mean(values * values, axis=-1, keepdims=True) + norm_eps)
    normed = (values * scale * gain[...]).astype(jnp.bfloat16)
    sent = jnp.dot(placed.astype(jnp.bfloat16), normed, preferred_element_type=jnp.float32)
    outgoing[...] = sent.reshape(half, CAP, width).astype(jnp.bfloat16)
    helps = jnp.logical_and(lower == 1, core == 0)

    @pl.when(helps)
    def _():
        more, _ = slots_of(rows, lambda p: half + p)
        sent = jnp.dot(more.astype(jnp.bfloat16), normed, preferred_element_type=jnp.float32)
        helping[...] = sent.reshape(half, CAP, width).astype(jnp.bfloat16)

    pl.semaphore_wait(barrier, half + planes + len(closer) * lower * (1 - 2 * core))

    def send_block(block, sem, expert):
        pltpu.make_async_remote_copy(
            src_ref=block, dst_ref=incoming.at[lax.rem(ep, half)], send_sem=sem, recv_sem=in_sem.at[0],
            device_id=(expert, 2 * y + lower), device_id_type=MESH).start()

    def help_out():
        for q, dx in closer:
            p = near(q, dx)
            send_block(helping.at[p], help_sem, half + p)

    keeps = jnp.logical_or(lower == 0, core == 0)

    def dispatch():
        for q, dx in rounds:
            def send(p=near(q, dx)):
                send_block(outgoing.at[p], out_sem, goal + p)
            if (q, dx) in closer:
                pl.when(keeps)(send)
            else:
                send()

    pl.when(helps)(help_out)
    pl.when(lower + 1 - core > 0)(dispatch)

    swaps = [pltpu.make_async_remote_copy(
        src_ref=ref.at[0:share], dst_ref=ref.at[share:2 * share], send_sem=swap_send.at[i], recv_sem=swap_recv.at[i],
        device_id=(ep, 2 * y + 1 - core), device_id_type=MESH) for i, ref in enumerate((gate, up, down))]
    for i in (4, 5, 6):
        loads[i].wait()
    for swap in swaps:
        swap.start()

    picked, weight = slots_of(groups * CAP, lambda q: q)
    weight = jnp.transpose(weight * picked)

    for swap in swaps:
        swap.wait_recv()
    pl.when(lower + 1 - core == 0)(dispatch)
    gate_across[...] = jnp.transpose(gate[...])
    up_across[...] = jnp.transpose(up[...])

    def wait_for(ref, sem, most):
        less, full = ref.at[pl.ds(0, most - 1)], ref.at[pl.ds(0, most)]
        pl.when(core == lower)(lambda: pltpu.make_async_copy(less, less, sem).wait())
        pl.when(core != lower)(lambda: pltpu.make_async_copy(full, full, sem).wait())

    def wait_all(ref, sem):
        pltpu.make_async_copy(ref, ref, sem).wait()

    pieces = [piece for some in PIECES for piece in some]
    totals = {}
    others = range(planes - 1)

    def plane(d):
        return d + (d + planes - y) // planes

    def seen_at(d):
        return y - (y + planes - 1 - plane(d)) // planes

    def columns(to):
        return pl.ds(pl.multiple_of(to * tile, tile), tile)

    def give(d, piece):
        some, side, k = pl.ds(piece[0] * CAP, (piece[1] - piece[0]) * CAP), piece[2], pieces.index(piece)
        return pltpu.make_async_remote_copy(
            src_ref=partial.at[d, side, some], dst_ref=reduced.at[seen_at(d), side, some],
            send_sem=part_send.at[d, k], recv_sem=part_recv.at[seen_at(d), k],
            device_id=(ep, 2 * plane(d) + core), device_id_type=MESH)

    def received(d, piece):
        some, side, k = pl.ds(piece[0] * CAP, (piece[1] - piece[0]) * CAP), piece[2], pieces.index(piece)
        return pltpu.make_async_copy(reduced.at[d, side, some], reduced.at[d, side, some], part_recv.at[d, k])

    def multiply(k):
        first, upto = CHUNKS[k]
        wait_all(incoming.at[pl.ds(first, upto - first)], in_sem.at[k])
        a = incoming[first:upto].astype(jnp.float32).reshape((upto - first) * CAP, width).astype(jnp.bfloat16)
        gate_act = jnp.dot(a, gate_across[...], preferred_element_type=jnp.float32)
        up_act = jnp.dot(a, up_across[...], preferred_element_type=jnp.float32)
        hidden = (gate_act / (1.0 + jnp.exp(-gate_act)) * up_act).astype(jnp.bfloat16)
        for d in others:
            block = jnp.dot(hidden, down[:, columns(plane(d))], preferred_element_type=jnp.float32)
            for side in range(2):
                partial[d, side, first * CAP:upto * CAP] = block[:, side * part:(side + 1) * part]
            give(d, PIECES[k][0]).start()
        for piece in PIECES[k][1:]:
            for d in others:
                give(d, piece).start()
        mine = jnp.dot(hidden, down[:, columns(y)], preferred_element_type=jnp.float32)
        for piece in PIECES[k]:
            totals[piece] = mine[(piece[0] - first) * CAP:(piece[1] - first) * CAP]

    def give_back(k):
        piece = pieces[k]
        first, upto, side = piece
        for d in others:
            received(d, piece).wait()
        total = totals[piece][:, side * part:(side + 1) * part].reshape(upto - first, CAP, part)
        for d in others:
            total = total + reduced[d, side, first * CAP:upto * CAP].reshape(upto - first, CAP, part)
        back[side, first:upto] = total
        for start in range(first, upto, XS):
            for dx in (2, 1, 3, 0):
                p = start + lax.rem(x + dx, XS)

                def send(p=p):
                    pltpu.make_async_remote_copy(
                        src_ref=back.at[side, p], dst_ref=arrived.at[ep], send_sem=back_send, recv_sem=back_recv,
                        device_id=(theirs + p, 2 * y + side), device_id_type=MESH).start()

                def hold(p=p):
                    arrived[ep] = back[side, p]
                if dx == 0:
                    here = jnp.logical_and(theirs + p == ep, core == side)
                    pl.when(here)(hold)
                    pl.when(jnp.logical_not(here))(send)
                else:
                    send()

    for step in STEPS:
        (multiply if step[0] == "c" else give_back)(int(step[1:]))

    wait_for(arrived, back_recv, groups)
    out = jnp.dot(weight, arrived[...].reshape(groups * CAP, part), precision=lax.Precision.HIGHEST,
                  preferred_element_type=jnp.float32)
    mixed[...] = out.astype(mixed.dtype)
    def wait_some(ref, blocks, sem):
        some = ref.at[pl.ds(0, blocks)]
        pltpu.make_async_copy(some, some, sem).wait()
    pl.when(keeps)(lambda: wait_some(outgoing, half, out_sem))
    pl.when(jnp.logical_not(keeps))(lambda: wait_some(outgoing, half - len(closer), out_sem))
    pl.when(helps)(lambda: wait_some(helping, len(closer), help_sem))
    for swap in swaps:
        swap.wait_send()
    for piece in pieces:
        for d in others:
            give(d, piece).wait_send()
    wait_for(arrived, back_send, groups)


def solution(mesh):
    groups, shares = mesh.shape["ep"], mesh.shape["tp"]

    def local(tokens, norm_gain, routing, route_weight, w_gate, w_up, w_down):
        count, width = tokens.shape
        part = width // shares
        half, planes = groups // 2, shares // 2
        rows = half * CAP
        share = w_down.shape[1]
        pieces = sum(map(len, PIECES))
        vmem = pl.BlockSpec(memory_space=pltpu.VMEM)
        hbm = pl.BlockSpec(memory_space=pltpu.HBM)
        return pl.pallas_call(
            functools.partial(kernel, groups, shares),
            out_shape=pltpu.VMEM((count, part), jnp.bfloat16),
            in_specs=[hbm] * 7,
            out_specs=vmem,
            scratch_shapes=[
                pltpu.VMEM((count, width), tokens.dtype),
                pltpu.VMEM((1, width), norm_gain.dtype),
                pltpu.VMEM(routing.shape[::-1], routing.dtype),
                pltpu.VMEM(route_weight.shape[::-1], route_weight.dtype),
                pltpu.VMEM((2 * share, width), jnp.bfloat16),
                pltpu.VMEM((2 * share, width), jnp.bfloat16),
                pltpu.VMEM((2 * share, width), jnp.bfloat16),
                pltpu.VMEM((width, 2 * share), jnp.bfloat16),
                pltpu.VMEM((width, 2 * share), jnp.bfloat16),
                pltpu.VMEM((half, CAP, width), jnp.bfloat16),
                pltpu.VMEM((half, CAP, width), jnp.bfloat16),
                pltpu.VMEM((half, CAP, width), jnp.bfloat16),
                pltpu.VMEM((planes - 1, 2, rows, part), jnp.float32),
                pltpu.VMEM((planes - 1, 2, rows, part), jnp.float32),
                pltpu.VMEM((2, half, CAP, part), jnp.float32),
                pltpu.VMEM((groups, CAP, part), jnp.float32),
                pltpu.SemaphoreType.DMA((7,)),
                pltpu.SemaphoreType.DMA((3,)),
                pltpu.SemaphoreType.DMA((3,)),
                pltpu.SemaphoreType.DMA,
                pltpu.SemaphoreType.DMA,
                pltpu.SemaphoreType.DMA((len(CHUNKS),)),
                pltpu.SemaphoreType.DMA((planes - 1, pieces)),
                pltpu.SemaphoreType.DMA((planes - 1, pieces)),
                pltpu.SemaphoreType.DMA,
                pltpu.SemaphoreType.DMA,
            ],
            compiler_params=pltpu.CompilerParams(collective_id=0, has_side_effects=True,
                                                 vmem_limit_bytes=67043328 - 16384),
            name="experts",
        )(tokens, norm_gain.reshape(1, width), routing.T, route_weight.T,
          jnp.swapaxes(w_gate, 1, 2), jnp.swapaxes(w_up, 1, 2), w_down)

    in_specs = (
        P("ep", None),
        P(),
        P("ep", None),
        P("ep", None),
        P("ep", None, "tp"),
        P("ep", None, "tp"),
        P("ep", "tp", None),
    )
    return jax.shard_map(local, mesh=mesh, in_specs=in_specs, out_specs=P("ep", "tp"), check_vma=False)
```

```python
import functools

import jax
import jax.numpy as jnp
from jax import lax
from jax.experimental import pallas as pl
from jax.experimental.pallas import tpu as pltpu
from jax.sharding import PartitionSpec as P

CAP = 8
XS = 4
CHUNKS = ((0, 16),)
PIECES = (((0, 4, 1), (0, 8, 0), (4, 16, 1), (8, 16, 0)),)
STEPS = ('c0', 'r0', 'r1', 'r2', 'r3')
STEPS_16 = 32767.0
LEAST = 2e-34
MESH = pl.DeviceIdType.MESH

norm_eps = 1e-06


def kernel(groups, shares, tokens_hbm, gain_hbm, routing_hbm, route_weight_hbm, gate_hbm, up_hbm, down_hbm, mixed,
           tokens, gain, routing, route_weight, gate, up, down, gate_across, up_across,
           outgoing, helping, incoming, partial, reduced, peak, their_peak, back, arrived,
           load_sem, swap_send, swap_recv, out_sem, help_sem, in_sem, part_send, part_recv, peak_send, peak_recv, back_send, back_recv):
    ep, tp = lax.axis_index("ep"), lax.axis_index("tp")
    width = tokens.shape[1]
    part = mixed.shape[1]
    half = groups // 2
    rows = half * CAP
    planes = shares // 2
    share = gate_hbm.shape[1]
    y, core = tp // 2, lax.rem(tp, 2)
    zs = groups // XS
    z, x = ep // XS, lax.rem(ep, XS)
    lower = 1 - z // (zs // 2)
    theirs, goal = half * (1 - core), half * core

    def near(q, dx):
        return XS * lax.rem(z + q, zs // 2) + lax.rem(x + dx, XS)

    rounds = [(q, dx) for dx in (2, 3, 1, 0) for q in (0, 1, 3, 2)]

    chunk_of = {p: k for k, (first, upto) in enumerate(CHUNKS) for p in range(first, upto)}
    tile = 2 * part

    barrier = pltpu.get_barrier_semaphore()
    closer = [(q, dx) for q, dx in rounds if q == 2 and dx in (2, 1, 3)]
    cross = jnp.logical_and(lower == 0, core == 1).astype(jnp.int32)
    for q, dx in rounds:
        other = 1 - lower - cross if (q, dx) in closer else 1 - lower
        pl.semaphore_signal(barrier, inc=1, device_id=(theirs + near(q, dx), 2 * y + other), device_id_type=MESH)
    for d in range(1, planes):
        pl.semaphore_signal(barrier, inc=1, device_id=(ep, 2 * lax.rem(y + d, planes) + core), device_id_type=MESH)
    pl.semaphore_signal(barrier, inc=1, device_id=(ep, 2 * y + 1 - core), device_id_type=MESH)

    pairs = ((tokens_hbm, tokens), (gain_hbm, gain), (routing_hbm, routing), (route_weight_hbm, route_weight),
             (gate_hbm.at[0], gate.at[0:share]), (up_hbm.at[0], up.at[0:share]), (down_hbm.at[0], down.at[0:share]))
    loads = [pltpu.make_async_copy(source, target, load_sem.at[i]) for i, (source, target) in enumerate(pairs)]
    for i in (2, 3, 0, 1, 4, 5, 6):
        loads[i].start()

    count = tokens.shape[0]
    earlier = lax.broadcasted_iota(jnp.int32, (count, count), 0) < lax.broadcasted_iota(jnp.int32, (count, count), 1)
    earlier = jnp.where(earlier, 1.0, 0.0).astype(jnp.bfloat16)

    def slots_of(lines, expert_of):
        line = lax.broadcasted_iota(jnp.int32, (lines, count), 0)
        expert = expert_of(line // CAP)
        member = jnp.zeros((lines, count), jnp.float32)
        weight = jnp.zeros((lines, count), jnp.float32)
        for k in range(routing.shape[0]):
            named = routing[k:k + 1, :] == expert
            member = jnp.where(named, 1.0, member)
            weight = jnp.where(named, route_weight[k:k + 1, :], weight)
        before = jnp.dot(member.astype(jnp.bfloat16), earlier, preferred_element_type=jnp.float32)
        placed = jnp.where(before == lax.rem(line, CAP).astype(jnp.float32), member, 0.0)
        return placed, weight

    loads[2].wait()
    loads[3].wait()
    placed, _ = slots_of(rows, lambda p: goal + p)
    loads[0].wait()
    loads[1].wait()
    values = tokens[...].astype(jnp.float32)
    scale = lax.rsqrt(jnp.mean(values * values, axis=-1, keepdims=True) + norm_eps)
    normed = (values * scale * gain[...]).astype(jnp.bfloat16)
    sent = jnp.dot(placed.astype(jnp.bfloat16), normed, preferred_element_type=jnp.float32)
    outgoing[...] = sent.reshape(half, CAP, width).astype(jnp.bfloat16)
    helps = jnp.logical_and(lower == 1, core == 0)

    @pl.when(helps)
    def _():
        more, _ = slots_of(rows, lambda p: half + p)
        sent = jnp.dot(more.astype(jnp.bfloat16), normed, preferred_element_type=jnp.float32)
        helping[...] = sent.reshape(half, CAP, width).astype(jnp.bfloat16)

    pl.semaphore_wait(barrier, half + planes + len(closer) * lower * (1 - 2 * core))

    def send_block(block, sem, expert):
        pltpu.make_async_remote_copy(
            src_ref=block, dst_ref=incoming.at[lax.rem(ep, half)], send_sem=sem, recv_sem=in_sem.at[0],
            device_id=(expert, 2 * y + lower), device_id_type=MESH).start()

    def help_out():
        for q, dx in closer:
            p = near(q, dx)
            send_block(helping.at[p], help_sem, half + p)

    keeps = jnp.logical_or(lower == 0, core == 0)

    def dispatch():
        for q, dx in rounds:
            def send(p=near(q, dx)):
                send_block(outgoing.at[p], out_sem, goal + p)
            if (q, dx) in closer:
                pl.when(keeps)(send)
            else:
                send()

    pl.when(helps)(help_out)
    pl.when(lower + 1 - core > 0)(dispatch)

    swaps = [pltpu.make_async_remote_copy(
        src_ref=ref.at[0:share], dst_ref=ref.at[share:2 * share], send_sem=swap_send.at[i], recv_sem=swap_recv.at[i],
        device_id=(ep, 2 * y + 1 - core), device_id_type=MESH) for i, ref in enumerate((gate, up, down))]
    for i in (4, 5, 6):
        loads[i].wait()
    for swap in swaps:
        swap.start()

    picked, weight = slots_of(groups * CAP, lambda q: q)
    weight = jnp.transpose(weight * picked)

    for swap in swaps:
        swap.wait_recv()
    pl.when(lower + 1 - core == 0)(dispatch)
    gate_across[...] = jnp.transpose(gate[...])
    up_across[...] = jnp.transpose(up[...])

    def wait_for(ref, sem, most):
        less, full = ref.at[pl.ds(0, most - 1)], ref.at[pl.ds(0, most)]
        pl.when(core == lower)(lambda: pltpu.make_async_copy(less, less, sem).wait())
        pl.when(core != lower)(lambda: pltpu.make_async_copy(full, full, sem).wait())

    def wait_all(ref, sem):
        pltpu.make_async_copy(ref, ref, sem).wait()

    pieces = [piece for some in PIECES for piece in some]
    totals = {}
    others = range(planes - 1)

    def plane(d):
        return d + (d + planes - y) // planes

    def seen_at(d):
        return y - (y + planes - 1 - plane(d)) // planes

    def columns(to):
        return pl.ds(pl.multiple_of(to * tile, tile), tile)

    def give(d, piece):
        some, side, k = pl.ds(piece[0] * CAP, (piece[1] - piece[0]) * CAP), piece[2], pieces.index(piece)
        return pltpu.make_async_remote_copy(
            src_ref=partial.at[d, side, some], dst_ref=reduced.at[seen_at(d), side, some],
            send_sem=part_send.at[d, k], recv_sem=part_recv.at[seen_at(d), k],
            device_id=(ep, 2 * plane(d) + core), device_id_type=MESH)

    def received(d, piece):
        some, side, k = pl.ds(piece[0] * CAP, (piece[1] - piece[0]) * CAP), piece[2], pieces.index(piece)
        return pltpu.make_async_copy(reduced.at[d, side, some], reduced.at[d, side, some], part_recv.at[d, k])

    def give_peak(d):
        return pltpu.make_async_remote_copy(
            src_ref=peak.at[d], dst_ref=their_peak.at[seen_at(d)], send_sem=peak_send.at[d],
            recv_sem=peak_recv.at[seen_at(d)], device_id=(ep, 2 * plane(d) + core), device_id_type=MESH)

    def multiply(k):
        first, upto = CHUNKS[k]
        wait_all(incoming.at[pl.ds(first, upto - first)], in_sem.at[k])
        a = incoming[first:upto].astype(jnp.float32).reshape((upto - first) * CAP, width).astype(jnp.bfloat16)
        gate_act = jnp.dot(a, gate_across[...], preferred_element_type=jnp.float32)
        up_act = jnp.dot(a, up_across[...], preferred_element_type=jnp.float32)
        hidden = (gate_act / (1.0 + jnp.exp(-gate_act)) * up_act).astype(jnp.bfloat16)
        for d in others:
            block = jnp.dot(hidden, down[:, columns(plane(d))], preferred_element_type=jnp.float32)
            sides = [block[:, side * part:(side + 1) * part].reshape(upto - first, CAP, part) for side in range(2)]
            most = jnp.maximum(jnp.max(jnp.maximum(jnp.abs(sides[0]), jnp.abs(sides[1])), axis=0), LEAST)
            peak[d] = most
            give_peak(d).start()
            for side in range(2):
                coded = jnp.round(sides[side] * (STEPS_16 / most)).reshape((upto - first) * CAP, part)
                partial[d, side, first * CAP:upto * CAP] = (
                    coded.astype(jnp.int32).astype(jnp.int16))
            give(d, PIECES[k][0]).start()
        for piece in PIECES[k][1:]:
            for d in others:
                give(d, piece).start()
        mine = jnp.dot(hidden, down[:, columns(y)], preferred_element_type=jnp.float32)
        for piece in PIECES[k]:
            totals[piece] = mine[(piece[0] - first) * CAP:(piece[1] - first) * CAP]

    def give_back(k):
        piece = pieces[k]
        first, upto, side = piece
        for d in others:
            if k == 0:
                pltpu.make_async_copy(their_peak.at[d], their_peak.at[d], peak_recv.at[d]).wait()
            received(d, piece).wait()
        total = totals[piece][:, side * part:(side + 1) * part].reshape(upto - first, CAP, part)
        for d in others:
            coded = reduced[d, side, first * CAP:upto * CAP].astype(jnp.int32).astype(jnp.float32)
            total = total + coded.reshape(upto - first, CAP, part) * (their_peak[d] * (1.0 / STEPS_16))
        back[side, first:upto] = total
        for start in range(first, upto, XS):
            for dx in (2, 1, 3, 0):
                p = start + lax.rem(x + dx, XS)

                def send(p=p):
                    pltpu.make_async_remote_copy(
                        src_ref=back.at[side, p], dst_ref=arrived.at[ep], send_sem=back_send, recv_sem=back_recv,
                        device_id=(theirs + p, 2 * y + side), device_id_type=MESH).start()

                def hold(p=p):
                    arrived[ep] = back[side, p]
                if dx == 0:
                    here = jnp.logical_and(theirs + p == ep, core == side)
                    pl.when(here)(hold)
                    pl.when(jnp.logical_not(here))(send)
                else:
                    send()

    for step in STEPS:
        (multiply if step[0] == "c" else give_back)(int(step[1:]))

    wait_for(arrived, back_recv, groups)
    out = jnp.dot(weight, arrived[...].reshape(groups * CAP, part), precision=lax.Precision.HIGHEST,
                  preferred_element_type=jnp.float32)
    mixed[...] = out.astype(mixed.dtype)
    def wait_some(ref, blocks, sem):
        some = ref.at[pl.ds(0, blocks)]
        pltpu.make_async_copy(some, some, sem).wait()
    pl.when(keeps)(lambda: wait_some(outgoing, half, out_sem))
    pl.when(jnp.logical_not(keeps))(lambda: wait_some(outgoing, half - len(closer), out_sem))
    pl.when(helps)(lambda: wait_some(helping, len(closer), help_sem))
    for swap in swaps:
        swap.wait_send()
    for d in others:
        give_peak(d).wait_send()
    for piece in pieces:
        for d in others:
            give(d, piece).wait_send()
    wait_for(arrived, back_send, groups)


def solution(mesh):
    groups, shares = mesh.shape["ep"], mesh.shape["tp"]

    def local(tokens, norm_gain, routing, route_weight, w_gate, w_up, w_down):
        count, width = tokens.shape
        part = width // shares
        half, planes = groups // 2, shares // 2
        rows = half * CAP
        share = w_down.shape[1]
        pieces = sum(map(len, PIECES))
        vmem = pl.BlockSpec(memory_space=pltpu.VMEM)
        hbm = pl.BlockSpec(memory_space=pltpu.HBM)
        return pl.pallas_call(
            functools.partial(kernel, groups, shares),
            out_shape=pltpu.VMEM((count, part), jnp.bfloat16),
            in_specs=[hbm] * 7,
            out_specs=vmem,
            scratch_shapes=[
                pltpu.VMEM((count, width), tokens.dtype),
                pltpu.VMEM((1, width), norm_gain.dtype),
                pltpu.VMEM(routing.shape[::-1], routing.dtype),
                pltpu.VMEM(route_weight.shape[::-1], route_weight.dtype),
                pltpu.VMEM((2 * share, width), jnp.bfloat16),
                pltpu.VMEM((2 * share, width), jnp.bfloat16),
                pltpu.VMEM((2 * share, width), jnp.bfloat16),
                pltpu.VMEM((width, 2 * share), jnp.bfloat16),
                pltpu.VMEM((width, 2 * share), jnp.bfloat16),
                pltpu.VMEM((half, CAP, width), jnp.bfloat16),
                pltpu.VMEM((half, CAP, width), jnp.bfloat16),
                pltpu.VMEM((half, CAP, width), jnp.bfloat16),
                pltpu.VMEM((planes - 1, 2, rows, part), jnp.int16),
                pltpu.VMEM((planes - 1, 2, rows, part), jnp.int16),
                pltpu.VMEM((planes - 1, CAP, part), jnp.float32),
                pltpu.VMEM((planes - 1, CAP, part), jnp.float32),
                pltpu.VMEM((2, half, CAP, part), jnp.float32),
                pltpu.VMEM((groups, CAP, part), jnp.float32),
                pltpu.SemaphoreType.DMA((7,)),
                pltpu.SemaphoreType.DMA((3,)),
                pltpu.SemaphoreType.DMA((3,)),
                pltpu.SemaphoreType.DMA,
                pltpu.SemaphoreType.DMA,
                pltpu.SemaphoreType.DMA((len(CHUNKS),)),
                pltpu.SemaphoreType.DMA((planes - 1, pieces)),
                pltpu.SemaphoreType.DMA((planes - 1, pieces)),
                pltpu.SemaphoreType.DMA((planes - 1,)),
                pltpu.SemaphoreType.DMA((planes - 1,)),
                pltpu.SemaphoreType.DMA,
                pltpu.SemaphoreType.DMA,
            ],
            compiler_params=pltpu.CompilerParams(collective_id=0, has_side_effects=True,
                                                 vmem_limit_bytes=67043328 - 16384),
            name="experts",
        )(tokens, norm_gain.reshape(1, width), routing.T, route_weight.T,
          jnp.swapaxes(w_gate, 1, 2), jnp.swapaxes(w_up, 1, 2), w_down)

    in_specs = (
        P("ep", None),
        P(),
        P("ep", None),
        P("ep", None),
        P("ep", None, "tp"),
        P("ep", None, "tp"),
        P("ep", "tp", None),
    )
    return jax.shard_map(local, mesh=mesh, in_specs=in_specs, out_specs=P("ep", "tp"), check_vma=False)
```

```python
import functools

import jax
import jax.numpy as jnp
from jax import lax
from jax.experimental import pallas as pl
from jax.experimental.pallas import tpu as pltpu
from jax.sharding import PartitionSpec as P

CAP = 8
XS = 4
CHUNKS = ((0, 16),)
PIECES = (((0, 8, 1), (0, 8, 0), (8, 16, 1), (8, 16, 0)),)
STEPS = ('c0', 'r0', 'r1', 'r2', 'r3')
STEPS_16 = 32767.0
LEAST = 2e-34
MESH = pl.DeviceIdType.MESH

norm_eps = 1e-06


def kernel(groups, shares, tokens_hbm, gain_hbm, routing_hbm, route_weight_hbm, gate_hbm, up_hbm, down_hbm, mixed,
           tokens, gain, routing, route_weight, gate, up, down, gate_across, up_across,
           outgoing, helping, incoming, partial, reduced, peak, their_peak, back, arrived,
           load_sem, swap_send, swap_recv, out_sem, help_sem, in_sem, part_send, part_recv, peak_send, peak_recv, back_send, back_recv):
    ep, tp = lax.axis_index("ep"), lax.axis_index("tp")
    width = tokens.shape[1]
    part = mixed.shape[1]
    half = groups // 2
    rows = half * CAP
    planes = shares // 2
    share = gate_hbm.shape[1]
    y, core = tp // 2, lax.rem(tp, 2)
    zs = groups // XS
    z, x = ep // XS, lax.rem(ep, XS)
    lower = 1 - z // (zs // 2)
    theirs, goal = half * (1 - core), half * core

    def near(q, dx):
        return XS * lax.rem(z + q, zs // 2) + lax.rem(x + dx, XS)

    rounds = [(q, dx) for dx in (2, 3, 1, 0) for q in (0, 1, 3, 2)]

    chunk_of = {p: k for k, (first, upto) in enumerate(CHUNKS) for p in range(first, upto)}
    tile = 2 * part

    barrier = pltpu.get_barrier_semaphore()
    closer = [(q, dx) for q, dx in rounds if q == 2 and dx in (2, 1, 3)]
    cross = jnp.logical_and(lower == 0, core == 1).astype(jnp.int32)
    for q, dx in rounds:
        other = 1 - lower - cross if (q, dx) in closer else 1 - lower
        pl.semaphore_signal(barrier, inc=1, device_id=(theirs + near(q, dx), 2 * y + other), device_id_type=MESH)
    for d in range(1, planes):
        pl.semaphore_signal(barrier, inc=1, device_id=(ep, 2 * lax.rem(y + d, planes) + core), device_id_type=MESH)
    pl.semaphore_signal(barrier, inc=1, device_id=(ep, 2 * y + 1 - core), device_id_type=MESH)

    pairs = ((tokens_hbm, tokens), (gain_hbm, gain), (routing_hbm, routing), (route_weight_hbm, route_weight),
             (gate_hbm.at[0], gate.at[0:share]), (up_hbm.at[0], up.at[0:share]), (down_hbm.at[0], down.at[0:share]))
    loads = [pltpu.make_async_copy(source, target, load_sem.at[i]) for i, (source, target) in enumerate(pairs)]
    for i in (2, 3, 0, 1, 4, 5, 6):
        loads[i].start()

    count = tokens.shape[0]
    earlier = lax.broadcasted_iota(jnp.int32, (count, count), 0) < lax.broadcasted_iota(jnp.int32, (count, count), 1)
    earlier = jnp.where(earlier, 1.0, 0.0).astype(jnp.bfloat16)

    def slots_of(lines, expert_of):
        line = lax.broadcasted_iota(jnp.int32, (lines, count), 0)
        expert = expert_of(line // CAP)
        member = jnp.zeros((lines, count), jnp.float32)
        weight = jnp.zeros((lines, count), jnp.float32)
        for k in range(routing.shape[0]):
            named = routing[k:k + 1, :] == expert
            member = jnp.where(named, 1.0, member)
            weight = jnp.where(named, route_weight[k:k + 1, :], weight)
        before = jnp.dot(member.astype(jnp.bfloat16), earlier, preferred_element_type=jnp.float32)
        placed = jnp.where(before == lax.rem(line, CAP).astype(jnp.float32), member, 0.0)
        return placed, weight

    loads[2].wait()
    loads[3].wait()
    placed, _ = slots_of(rows, lambda p: goal + p)
    loads[0].wait()
    loads[1].wait()
    values = tokens[...].astype(jnp.float32)
    scale = lax.rsqrt(jnp.mean(values * values, axis=-1, keepdims=True) + norm_eps)
    normed = (values * scale * gain[...]).astype(jnp.bfloat16)
    sent = jnp.dot(placed.astype(jnp.bfloat16), normed, preferred_element_type=jnp.float32)
    outgoing[...] = sent.reshape(half, CAP, width).astype(jnp.bfloat16)
    helps = jnp.logical_and(lower == 1, core == 0)

    @pl.when(helps)
    def _():
        more, _ = slots_of(rows, lambda p: half + p)
        sent = jnp.dot(more.astype(jnp.bfloat16), normed, preferred_element_type=jnp.float32)
        helping[...] = sent.reshape(half, CAP, width).astype(jnp.bfloat16)

    pl.semaphore_wait(barrier, half + planes + len(closer) * lower * (1 - 2 * core))

    def send_block(block, sem, expert):
        pltpu.make_async_remote_copy(
            src_ref=block, dst_ref=incoming.at[lax.rem(ep, half)], send_sem=sem, recv_sem=in_sem.at[0],
            device_id=(expert, 2 * y + lower), device_id_type=MESH).start()

    def help_out():
        for q, dx in closer:
            p = near(q, dx)
            send_block(helping.at[p], help_sem, half + p)

    keeps = jnp.logical_or(lower == 0, core == 0)

    def dispatch():
        for q, dx in rounds:
            def send(p=near(q, dx)):
                send_block(outgoing.at[p], out_sem, goal + p)
            if (q, dx) in closer:
                pl.when(keeps)(send)
            else:
                send()

    pl.when(helps)(help_out)
    pl.when(lower + 1 - core > 0)(dispatch)

    swaps = [pltpu.make_async_remote_copy(
        src_ref=ref.at[0:share], dst_ref=ref.at[share:2 * share], send_sem=swap_send.at[i], recv_sem=swap_recv.at[i],
        device_id=(ep, 2 * y + 1 - core), device_id_type=MESH) for i, ref in enumerate((gate, up, down))]
    for i in (4, 5, 6):
        loads[i].wait()
    for swap in swaps:
        swap.start()

    picked, weight = slots_of(groups * CAP, lambda q: q)
    weight = jnp.transpose(weight * picked)

    for swap in swaps:
        swap.wait_recv()
    pl.when(lower + 1 - core == 0)(dispatch)
    gate_across[...] = jnp.transpose(gate[...])
    up_across[...] = jnp.transpose(up[...])

    def wait_for(ref, sem, most):
        less, full = ref.at[pl.ds(0, most - 1)], ref.at[pl.ds(0, most)]
        pl.when(core == lower)(lambda: pltpu.make_async_copy(less, less, sem).wait())
        pl.when(core != lower)(lambda: pltpu.make_async_copy(full, full, sem).wait())

    def wait_all(ref, sem):
        pltpu.make_async_copy(ref, ref, sem).wait()

    pieces = [piece for some in PIECES for piece in some]
    totals = {}
    others = range(planes - 1)

    def plane(d):
        return d + (d + planes - y) // planes

    def seen_at(d):
        return y - (y + planes - 1 - plane(d)) // planes

    def columns(to):
        return pl.ds(pl.multiple_of(to * tile, tile), tile)

    def give(d, piece):
        some, side, k = pl.ds(piece[0] * CAP, (piece[1] - piece[0]) * CAP), piece[2], pieces.index(piece)
        return pltpu.make_async_remote_copy(
            src_ref=partial.at[d, side, some], dst_ref=reduced.at[seen_at(d), side, some],
            send_sem=part_send.at[d, k], recv_sem=part_recv.at[seen_at(d), k],
            device_id=(ep, 2 * plane(d) + core), device_id_type=MESH)

    def received(d, piece):
        some, side, k = pl.ds(piece[0] * CAP, (piece[1] - piece[0]) * CAP), piece[2], pieces.index(piece)
        return pltpu.make_async_copy(reduced.at[d, side, some], reduced.at[d, side, some], part_recv.at[d, k])

    def give_peak(d):
        return pltpu.make_async_remote_copy(
            src_ref=peak.at[d], dst_ref=their_peak.at[seen_at(d)], send_sem=peak_send.at[d],
            recv_sem=peak_recv.at[seen_at(d)], device_id=(ep, 2 * plane(d) + core), device_id_type=MESH)

    def multiply(k):
        first, upto = CHUNKS[k]
        wait_all(incoming.at[pl.ds(first, upto - first)], in_sem.at[k])
        a = incoming[first:upto].astype(jnp.float32).reshape((upto - first) * CAP, width).astype(jnp.bfloat16)
        gate_act = jnp.dot(a, gate_across[...], preferred_element_type=jnp.float32)
        up_act = jnp.dot(a, up_across[...], preferred_element_type=jnp.float32)
        hidden = (gate_act / (1.0 + jnp.exp(-gate_act)) * up_act).astype(jnp.bfloat16)
        for d in others:
            block = jnp.dot(hidden, down[:, columns(plane(d))], preferred_element_type=jnp.float32)
            sides = [block[:, side * part:(side + 1) * part].reshape(upto - first, CAP, part) for side in range(2)]
            most = jnp.maximum(jnp.max(jnp.maximum(jnp.abs(sides[0]), jnp.abs(sides[1])), axis=0), LEAST)
            peak[d] = most
            give_peak(d).start()
            for side in range(2):
                coded = jnp.round(sides[side] * (STEPS_16 / most)).reshape((upto - first) * CAP, part)
                partial[d, side, first * CAP:upto * CAP] = (
                    coded.astype(jnp.int32).astype(jnp.int16))
            give(d, PIECES[k][0]).start()
        for piece in PIECES[k][1:]:
            for d in others:
                give(d, piece).start()
        mine = jnp.dot(hidden, down[:, columns(y)], preferred_element_type=jnp.float32)
        for piece in PIECES[k]:
            totals[piece] = mine[(piece[0] - first) * CAP:(piece[1] - first) * CAP]

    def give_back(k):
        piece = pieces[k]
        first, upto, side = piece
        for d in others:
            if k == 0:
                pltpu.make_async_copy(their_peak.at[d], their_peak.at[d], peak_recv.at[d]).wait()
            received(d, piece).wait()
        total = totals[piece][:, side * part:(side + 1) * part].reshape(upto - first, CAP, part)
        for d in others:
            coded = reduced[d, side, first * CAP:upto * CAP].astype(jnp.int32).astype(jnp.float32)
            total = total + coded.reshape(upto - first, CAP, part) * (their_peak[d] * (1.0 / STEPS_16))
        back[side, first:upto] = total
        for start in range(first, upto, XS):
            for dx in (2, 1, 3, 0):
                p = start + lax.rem(x + dx, XS)

                def send(p=p):
                    pltpu.make_async_remote_copy(
                        src_ref=back.at[side, p], dst_ref=arrived.at[ep], send_sem=back_send, recv_sem=back_recv,
                        device_id=(theirs + p, 2 * y + side), device_id_type=MESH).start()

                def hold(p=p):
                    arrived[ep] = back[side, p]
                if dx == 0:
                    here = jnp.logical_and(theirs + p == ep, core == side)
                    pl.when(here)(hold)
                    pl.when(jnp.logical_not(here))(send)
                else:
                    send()

    for step in STEPS:
        (multiply if step[0] == "c" else give_back)(int(step[1:]))

    wait_for(arrived, back_recv, groups)
    out = jnp.dot(weight, arrived[...].reshape(groups * CAP, part), precision=lax.Precision.HIGHEST,
                  preferred_element_type=jnp.float32)
    mixed[...] = out.astype(mixed.dtype)
    def wait_some(ref, blocks, sem):
        some = ref.at[pl.ds(0, blocks)]
        pltpu.make_async_copy(some, some, sem).wait()
    pl.when(keeps)(lambda: wait_some(outgoing, half, out_sem))
    pl.when(jnp.logical_not(keeps))(lambda: wait_some(outgoing, half - len(closer), out_sem))
    pl.when(helps)(lambda: wait_some(helping, len(closer), help_sem))
    for swap in swaps:
        swap.wait_send()
    for d in others:
        give_peak(d).wait_send()
    for piece in pieces:
        for d in others:
            give(d, piece).wait_send()
    wait_for(arrived, back_send, groups)


def solution(mesh):
    groups, shares = mesh.shape["ep"], mesh.shape["tp"]

    def local(tokens, norm_gain, routing, route_weight, w_gate, w_up, w_down):
        count, width = tokens.shape
        part = width // shares
        half, planes = groups // 2, shares // 2
        rows = half * CAP
        share = w_down.shape[1]
        pieces = sum(map(len, PIECES))
        vmem = pl.BlockSpec(memory_space=pltpu.VMEM)
        hbm = pl.BlockSpec(memory_space=pltpu.HBM)
        return pl.pallas_call(
            functools.partial(kernel, groups, shares),
            out_shape=pltpu.VMEM((count, part), jnp.bfloat16),
            in_specs=[hbm] * 7,
            out_specs=vmem,
            scratch_shapes=[
                pltpu.VMEM((count, width), tokens.dtype),
                pltpu.VMEM((1, width), norm_gain.dtype),
                pltpu.VMEM(routing.shape[::-1], routing.dtype),
                pltpu.VMEM(route_weight.shape[::-1], route_weight.dtype),
                pltpu.VMEM((2 * share, width), jnp.bfloat16),
                pltpu.VMEM((2 * share, width), jnp.bfloat16),
                pltpu.VMEM((2 * share, width), jnp.bfloat16),
                pltpu.VMEM((width, 2 * share), jnp.bfloat16),
                pltpu.VMEM((width, 2 * share), jnp.bfloat16),
                pltpu.VMEM((half, CAP, width), jnp.bfloat16),
                pltpu.VMEM((half, CAP, width), jnp.bfloat16),
                pltpu.VMEM((half, CAP, width), jnp.bfloat16),
                pltpu.VMEM((planes - 1, 2, rows, part), jnp.int16),
                pltpu.VMEM((planes - 1, 2, rows, part), jnp.int16),
                pltpu.VMEM((planes - 1, CAP, part), jnp.float32),
                pltpu.VMEM((planes - 1, CAP, part), jnp.float32),
                pltpu.VMEM((2, half, CAP, part), jnp.float32),
                pltpu.VMEM((groups, CAP, part), jnp.float32),
                pltpu.SemaphoreType.DMA((7,)),
                pltpu.SemaphoreType.DMA((3,)),
                pltpu.SemaphoreType.DMA((3,)),
                pltpu.SemaphoreType.DMA,
                pltpu.SemaphoreType.DMA,
                pltpu.SemaphoreType.DMA((len(CHUNKS),)),
                pltpu.SemaphoreType.DMA((planes - 1, pieces)),
                pltpu.SemaphoreType.DMA((planes - 1, pieces)),
                pltpu.SemaphoreType.DMA((planes - 1,)),
                pltpu.SemaphoreType.DMA((planes - 1,)),
                pltpu.SemaphoreType.DMA,
                pltpu.SemaphoreType.DMA,
            ],
            compiler_params=pltpu.CompilerParams(collective_id=0, has_side_effects=True,
                                                 vmem_limit_bytes=67043328 - 16384),
            name="experts",
        )(tokens, norm_gain.reshape(1, width), routing.T, route_weight.T,
          jnp.swapaxes(w_gate, 1, 2), jnp.swapaxes(w_up, 1, 2), w_down)

    in_specs = (
        P("ep", None),
        P(),
        P("ep", None),
        P("ep", None),
        P("ep", None, "tp"),
        P("ep", None, "tp"),
        P("ep", "tp", None),
    )
    return jax.shard_map(local, mesh=mesh, in_specs=in_specs, out_specs=P("ep", "tp"), check_vma=False)
```

```python
import functools

import jax
import jax.numpy as jnp
from jax import lax
from jax.experimental import pallas as pl
from jax.experimental.pallas import tpu as pltpu
from jax.sharding import PartitionSpec as P

CAP = 8
XS = 4
CHUNKS = ((0, 16),)
PIECES = (((0, 4, 1), (0, 8, 0), (4, 16, 1), (8, 16, 0)),)
STEPS = ('c0', 'r0', 'r1', 'r2', 'r3')
STEPS_16 = 32767.0
LEAST = 2e-34
MESH = pl.DeviceIdType.MESH

norm_eps = 1e-06


def kernel(groups, shares, tokens_hbm, gain_hbm, routing_hbm, route_weight_hbm, gate_hbm, up_hbm, down_hbm, mixed,
           tokens, gain, routing, route_weight, gate, up, down, gate_across, up_across,
           outgoing, helping, incoming, partial, reduced, peak, their_peak, back, arrived,
           load_sem, swap_send, swap_recv, out_sem, help_sem, in_sem, part_send, part_recv, peak_send, peak_recv, back_send, back_recv):
    ep, tp = lax.axis_index("ep"), lax.axis_index("tp")
    width = tokens.shape[1]
    part = mixed.shape[1]
    half = groups // 2
    rows = half * CAP
    planes = shares // 2
    share = gate_hbm.shape[1]
    y, core = tp // 2, lax.rem(tp, 2)
    zs = groups // XS
    z, x = ep // XS, lax.rem(ep, XS)
    lower = 1 - z // (zs // 2)
    theirs, goal = half * (1 - core), half * core

    def near(q, dx):
        return XS * lax.rem(z + q, zs // 2) + lax.rem(x + dx, XS)

    rounds = [(q, dx) for dx in (2, 3, 1, 0) for q in (0, 1, 3, 2)]

    chunk_of = {p: k for k, (first, upto) in enumerate(CHUNKS) for p in range(first, upto)}
    tile = 2 * part

    barrier = pltpu.get_barrier_semaphore()
    for d in range(1, planes):
        pl.semaphore_signal(barrier, inc=1, device_id=(ep, 2 * lax.rem(y + d, planes) + core), device_id_type=MESH)
    pl.semaphore_signal(barrier, inc=1, device_id=(ep, 2 * y + 1 - core), device_id_type=MESH)

    closer = [(q, dx) for q, dx in rounds if q == 2 and dx in (2, 1, 3)]
    cross = jnp.logical_and(lower == 0, core == 1).astype(jnp.int32)
    for q, dx in rounds:
        other = 1 - lower - cross if (q, dx) in closer else 1 - lower
        pl.semaphore_signal(barrier, inc=1, device_id=(theirs + near(q, dx), 2 * y + other), device_id_type=MESH)
    pairs = ((tokens_hbm, tokens), (gain_hbm, gain), (routing_hbm, routing), (route_weight_hbm, route_weight),
             (gate_hbm.at[0], gate.at[0:share]), (up_hbm.at[0], up.at[0:share]), (down_hbm.at[0], down.at[0:share]))
    loads = [pltpu.make_async_copy(source, target, load_sem.at[i]) for i, (source, target) in enumerate(pairs)]
    for i in (2, 3, 0, 1, 4, 5, 6):
        loads[i].start()

    count = tokens.shape[0]
    earlier = lax.broadcasted_iota(jnp.int32, (count, count), 0) < lax.broadcasted_iota(jnp.int32, (count, count), 1)
    earlier = jnp.where(earlier, 1.0, 0.0).astype(jnp.bfloat16)

    def slots_of(lines, expert_of):
        line = lax.broadcasted_iota(jnp.int32, (lines, count), 0)
        expert = expert_of(line // CAP)
        member = jnp.zeros((lines, count), jnp.float32)
        weight = jnp.zeros((lines, count), jnp.float32)
        for k in range(routing.shape[0]):
            named = routing[k:k + 1, :] == expert
            member = jnp.where(named, 1.0, member)
            weight = jnp.where(named, route_weight[k:k + 1, :], weight)
        before = jnp.dot(member.astype(jnp.bfloat16), earlier, preferred_element_type=jnp.float32)
        placed = jnp.where(before == lax.rem(line, CAP).astype(jnp.float32), member, 0.0)
        return placed, weight

    loads[2].wait()
    loads[3].wait()
    placed, _ = slots_of(rows, lambda p: goal + p)
    loads[0].wait()
    loads[1].wait()
    values = tokens[...].astype(jnp.float32)
    scale = lax.rsqrt(jnp.mean(values * values, axis=-1, keepdims=True) + norm_eps)
    normed = (values * scale * gain[...]).astype(jnp.bfloat16)
    sent = jnp.dot(placed.astype(jnp.bfloat16), normed, preferred_element_type=jnp.float32)
    outgoing[...] = sent.reshape(half, CAP, width).astype(jnp.bfloat16)
    helps = jnp.logical_and(lower == 1, core == 0)

    @pl.when(helps)
    def _():
        more, _ = slots_of(rows, lambda p: half + p)
        sent = jnp.dot(more.astype(jnp.bfloat16), normed, preferred_element_type=jnp.float32)
        helping[...] = sent.reshape(half, CAP, width).astype(jnp.bfloat16)

    pl.semaphore_wait(barrier, half + planes + len(closer) * lower * (1 - 2 * core))

    def send_block(block, sem, expert):
        pltpu.make_async_remote_copy(
            src_ref=block, dst_ref=incoming.at[lax.rem(ep, half)], send_sem=sem, recv_sem=in_sem.at[0],
            device_id=(expert, 2 * y + lower), device_id_type=MESH).start()

    def help_out():
        for q, dx in closer:
            p = near(q, dx)
            send_block(helping.at[p], help_sem, half + p)

    keeps = jnp.logical_or(lower == 0, core == 0)

    def dispatch():
        for q, dx in rounds:
            def send(p=near(q, dx)):
                send_block(outgoing.at[p], out_sem, goal + p)
            if (q, dx) in closer:
                pl.when(keeps)(send)
            else:
                send()

    pl.when(helps)(help_out)
    pl.when(lower + 1 - core > 0)(dispatch)

    swaps = [pltpu.make_async_remote_copy(
        src_ref=ref.at[0:share], dst_ref=ref.at[share:2 * share], send_sem=swap_send.at[i], recv_sem=swap_recv.at[i],
        device_id=(ep, 2 * y + 1 - core), device_id_type=MESH) for i, ref in enumerate((gate, up, down))]
    for i in (4, 5, 6):
        loads[i].wait()
    for swap in swaps:
        swap.start()

    picked, weight = slots_of(groups * CAP, lambda q: q)
    weight = jnp.transpose(weight * picked)

    for swap in swaps:
        swap.wait_recv()
    pl.when(lower + 1 - core == 0)(dispatch)
    gate_across[...] = jnp.transpose(gate[...])
    up_across[...] = jnp.transpose(up[...])

    def wait_for(ref, sem, most):
        less, full = ref.at[pl.ds(0, most - 1)], ref.at[pl.ds(0, most)]
        pl.when(core == lower)(lambda: pltpu.make_async_copy(less, less, sem).wait())
        pl.when(core != lower)(lambda: pltpu.make_async_copy(full, full, sem).wait())

    def wait_all(ref, sem):
        pltpu.make_async_copy(ref, ref, sem).wait()

    pieces = [piece for some in PIECES for piece in some]
    totals = {}
    others = range(planes - 1)

    def plane(d):
        return d + (d + planes - y) // planes

    def seen_at(d):
        return y - (y + planes - 1 - plane(d)) // planes

    def columns(to):
        return pl.ds(pl.multiple_of(to * tile, tile), tile)

    def give(d, piece):
        some, side, k = pl.ds(piece[0] * CAP, (piece[1] - piece[0]) * CAP), piece[2], pieces.index(piece)
        return pltpu.make_async_remote_copy(
            src_ref=partial.at[d, side, some], dst_ref=reduced.at[seen_at(d), side, some],
            send_sem=part_send.at[d, k], recv_sem=part_recv.at[seen_at(d), k],
            device_id=(ep, 2 * plane(d) + core), device_id_type=MESH)

    def received(d, piece):
        some, side, k = pl.ds(piece[0] * CAP, (piece[1] - piece[0]) * CAP), piece[2], pieces.index(piece)
        return pltpu.make_async_copy(reduced.at[d, side, some], reduced.at[d, side, some], part_recv.at[d, k])

    def give_peak(d):
        return pltpu.make_async_remote_copy(
            src_ref=peak.at[d], dst_ref=their_peak.at[seen_at(d)], send_sem=peak_send.at[d],
            recv_sem=peak_recv.at[seen_at(d)], device_id=(ep, 2 * plane(d) + core), device_id_type=MESH)

    def multiply(k):
        first, upto = CHUNKS[k]
        wait_all(incoming.at[pl.ds(first, upto - first)], in_sem.at[k])
        a = incoming[first:upto].astype(jnp.float32).reshape((upto - first) * CAP, width).astype(jnp.bfloat16)
        gate_act = jnp.dot(a, gate_across[...], preferred_element_type=jnp.float32)
        up_act = jnp.dot(a, up_across[...], preferred_element_type=jnp.float32)
        hidden = (gate_act / (1.0 + jnp.exp(-gate_act)) * up_act).astype(jnp.bfloat16)
        for d in others:
            block = jnp.dot(hidden, down[:, columns(plane(d))], preferred_element_type=jnp.float32)
            sides = [block[:, side * part:(side + 1) * part].reshape(upto - first, CAP, part) for side in range(2)]
            most = jnp.maximum(jnp.max(jnp.maximum(jnp.abs(sides[0]), jnp.abs(sides[1])), axis=0), LEAST)
            peak[d] = most
            give_peak(d).start()
            for side in range(2):
                coded = jnp.round(sides[side] * (STEPS_16 / most)).reshape((upto - first) * CAP, part)
                partial[d, side, first * CAP:upto * CAP] = (
                    coded.astype(jnp.int32).astype(jnp.int16))
            give(d, PIECES[k][0]).start()
        for piece in PIECES[k][1:]:
            for d in others:
                give(d, piece).start()
        mine = jnp.dot(hidden, down[:, columns(y)], preferred_element_type=jnp.float32)
        for piece in PIECES[k]:
            totals[piece] = mine[(piece[0] - first) * CAP:(piece[1] - first) * CAP]

    def give_back(k):
        piece = pieces[k]
        first, upto, side = piece
        for d in others:
            if k == 0:
                pltpu.make_async_copy(their_peak.at[d], their_peak.at[d], peak_recv.at[d]).wait()
            received(d, piece).wait()
        total = totals[piece][:, side * part:(side + 1) * part].reshape(upto - first, CAP, part)
        for d in others:
            coded = reduced[d, side, first * CAP:upto * CAP].astype(jnp.int32).astype(jnp.float32)
            total = total + coded.reshape(upto - first, CAP, part) * (their_peak[d] * (1.0 / STEPS_16))
        back[side, first:upto] = total
        for start in range(first, upto, XS):
            for dx in (2, 1, 3, 0):
                p = start + lax.rem(x + dx, XS)

                def send(p=p):
                    pltpu.make_async_remote_copy(
                        src_ref=back.at[side, p], dst_ref=arrived.at[ep], send_sem=back_send, recv_sem=back_recv,
                        device_id=(theirs + p, 2 * y + side), device_id_type=MESH).start()

                def hold(p=p):
                    arrived[ep] = back[side, p]
                if dx == 0:
                    here = jnp.logical_and(theirs + p == ep, core == side)
                    pl.when(here)(hold)
                    pl.when(jnp.logical_not(here))(send)
                else:
                    send()

    for step in STEPS:
        (multiply if step[0] == "c" else give_back)(int(step[1:]))

    wait_for(arrived, back_recv, groups)
    out = jnp.dot(weight, arrived[...].reshape(groups * CAP, part), precision=lax.Precision.HIGHEST,
                  preferred_element_type=jnp.float32)
    mixed[...] = out.astype(mixed.dtype)
    def wait_some(ref, blocks, sem):
        some = ref.at[pl.ds(0, blocks)]
        pltpu.make_async_copy(some, some, sem).wait()
    pl.when(keeps)(lambda: wait_some(outgoing, half, out_sem))
    pl.when(jnp.logical_not(keeps))(lambda: wait_some(outgoing, half - len(closer), out_sem))
    pl.when(helps)(lambda: wait_some(helping, len(closer), help_sem))
    for swap in swaps:
        swap.wait_send()
    for d in others:
        give_peak(d).wait_send()
    for piece in pieces:
        for d in others:
            give(d, piece).wait_send()
    wait_for(arrived, back_send, groups)


def solution(mesh):
    groups, shares = mesh.shape["ep"], mesh.shape["tp"]

    def local(tokens, norm_gain, routing, route_weight, w_gate, w_up, w_down):
        count, width = tokens.shape
        part = width // shares
        half, planes = groups // 2, shares // 2
        rows = half * CAP
        share = w_down.shape[1]
        pieces = sum(map(len, PIECES))
        vmem = pl.BlockSpec(memory_space=pltpu.VMEM)
        hbm = pl.BlockSpec(memory_space=pltpu.HBM)
        return pl.pallas_call(
            functools.partial(kernel, groups, shares),
            out_shape=pltpu.VMEM((count, part), jnp.bfloat16),
            in_specs=[hbm] * 7,
            out_specs=vmem,
            scratch_shapes=[
                pltpu.VMEM((count, width), tokens.dtype),
                pltpu.VMEM((1, width), norm_gain.dtype),
                pltpu.VMEM(routing.shape[::-1], routing.dtype),
                pltpu.VMEM(route_weight.shape[::-1], route_weight.dtype),
                pltpu.VMEM((2 * share, width), jnp.bfloat16),
                pltpu.VMEM((2 * share, width), jnp.bfloat16),
                pltpu.VMEM((2 * share, width), jnp.bfloat16),
                pltpu.VMEM((width, 2 * share), jnp.bfloat16),
                pltpu.VMEM((width, 2 * share), jnp.bfloat16),
                pltpu.VMEM((half, CAP, width), jnp.bfloat16),
                pltpu.VMEM((half, CAP, width), jnp.bfloat16),
                pltpu.VMEM((half, CAP, width), jnp.bfloat16),
                pltpu.VMEM((planes - 1, 2, rows, part), jnp.int16),
                pltpu.VMEM((planes - 1, 2, rows, part), jnp.int16),
                pltpu.VMEM((planes - 1, CAP, part), jnp.float32),
                pltpu.VMEM((planes - 1, CAP, part), jnp.float32),
                pltpu.VMEM((2, half, CAP, part), jnp.float32),
                pltpu.VMEM((groups, CAP, part), jnp.float32),
                pltpu.SemaphoreType.DMA((7,)),
                pltpu.SemaphoreType.DMA((3,)),
                pltpu.SemaphoreType.DMA((3,)),
                pltpu.SemaphoreType.DMA,
                pltpu.SemaphoreType.DMA,
                pltpu.SemaphoreType.DMA((len(CHUNKS),)),
                pltpu.SemaphoreType.DMA((planes - 1, pieces)),
                pltpu.SemaphoreType.DMA((planes - 1, pieces)),
                pltpu.SemaphoreType.DMA((planes - 1,)),
                pltpu.SemaphoreType.DMA((planes - 1,)),
                pltpu.SemaphoreType.DMA,
                pltpu.SemaphoreType.DMA,
            ],
            compiler_params=pltpu.CompilerParams(collective_id=0, has_side_effects=True,
                                                 vmem_limit_bytes=67043328 - 16384),
            name="experts",
        )(tokens, norm_gain.reshape(1, width), routing.T, route_weight.T,
          jnp.swapaxes(w_gate, 1, 2), jnp.swapaxes(w_up, 1, 2), w_down)

    in_specs = (
        P("ep", None),
        P(),
        P("ep", None),
        P("ep", None),
        P("ep", None, "tp"),
        P("ep", None, "tp"),
        P("ep", "tp", None),
    )
    return jax.shard_map(local, mesh=mesh, in_specs=in_specs, out_specs=P("ep", "tp"), check_vma=False)
```
